32 devices in a mesh: grp: 2 (over y), sp: 4 (over z), tp: 4 (over x, core).
Axes of the slice: x: 2, y: 2, z: 4, core: 2. Of those that a mesh axis runs over, the one named last changes fastest.
Arguments:
- tokens: bfloat16 [1024, 2048], P(('grp', 'sp'), 'tp'), parts along dimension 0
- mix_gain: bfloat16 [2048], replicated, may hold values from 0.099609375 to 1.8984375
- w_conv_value: bfloat16 [2048, 1024], P('sp', 'tp'), may hold values from -0.125 to 0.125
- w_conv_outer: bfloat16 [2048, 1024], P('sp', 'tp'), may hold values from -0.125 to 0.125
- w_conv_inner: bfloat16 [2048, 1024], P('sp', 'tp'), may hold values from -0.125 to 0.125
- conv_kernel: bfloat16 [3, 1024], P(None, 'tp'), may hold values from -3.5 to 3.5
- w_q_down: bfloat16 [2048, 512], P(None, 'tp'), may hold values from -0.125 to 0.125
- w_kv_down: bfloat16 [2048, 256], P(None, 'tp'), may hold values from -0.125 to 0.125
- w_rope_key: bfloat16 [2048, 32], replicated, may hold values from -0.125 to 0.125
- q_gain: bfloat16 [512], replicated
- kv_gain: bfloat16 [256], replicated, may hold values from 0.099609375 to 1.8984375
- w_q_nope: bfloat16 [512, 1024], P(None, 'tp'), may hold values from -0.25 to 0.25
- w_q_rope: bfloat16 [512, 512], P(None, 'tp'), may hold values from -0.25 to 0.25
- w_k_nope: bfloat16 [256, 1024], P(None, 'tp'), may hold values from -0.375 to 0.375
- w_value: bfloat16 [256, 1024], P(None, 'tp'), may hold values from -0.375 to 0.375
- w_out_conv: bfloat16 [1024, 2048], P('tp'), may hold values from -0.1875 to 0.1875
- w_out_attn: bfloat16 [1024, 2048], P('tp'), may hold values from -1.5 to 1.5
Outputs:
- mixed: bfloat16 [1024, 2048], P(('grp', 'sp'), 'tp'), parts along dimension 0
The draws below stay inside these ranges and needn't reach their ends.
There are 2 independent parts, one for each index of `grp`. The reference program is written for one: setup_inputs(seed, part) draws one part's arguments, and reference() takes and returns one part's arrays. A program takes and returns all parts, laid end to end along the dimension named above; an argument that names none is the same for every part. Nothing has to cross between parts.
All inputs are finite; a program needn't handle non-finite values.
Results may differ from the reference program's by a relative error of at most 0.028.
Values may be sent and summed in bfloat16 or wider, within the bound.
A program may use at most 64 MiB of HBM per device.

```python
import jax
import jax.numpy as jnp
from jax import lax

D = 2048
MLA_HEADS = 16
Q_LATENT = 512
KV_LATENT = 256
NOPE = 64
ROPE = 32
VALUE = 64
TAPS = 3
TOKENS = 512
CONV_WIDTH = 1024
N_TP = 4


def draw_tokens(key, part):
    first = jax.random.fold_in(key, 11)
    second = jax.random.fold_in(key, 12)
    column = jnp.arange(D, dtype=jnp.float32) / max(D - 1, 1)
    column_scale = jnp.exp(jnp.log(3.0) * column) * jnp.exp(jax.random.uniform(second, (D,), jnp.float32, -0.35, 0.35))
    base = jax.random.normal(first, (TOKENS, D), jnp.float32)
    return (base * column_scale[None, :]).astype(jnp.bfloat16)


def draw_q_gain(key, part):
    spread = jax.random.uniform(jax.random.fold_in(key, 21), (Q_LATENT,), jnp.float32, -1.0, 1.0)
    return (2.0 * (1.0 + 0.18 * spread)).astype(jnp.bfloat16)


def shard_levels(rng, extent, shards, low, high):
    def one(axis_at, parts):
        draws = jax.random.uniform(jax.random.fold_in(jax.random.fold_in(rng, 6), axis_at), (parts,), jnp.float32, low / len(shards), high / len(shards))
        return jnp.repeat(jnp.exp(draws), extent[axis_at] // parts).reshape((-1,) + (1,) * (len(extent) - axis_at - 1))

    loudness = one(*shards[0])
    for cut in shards[1:]:
        loudness = loudness * one(*cut)
    return loudness


def normal_values(own_key, shape, scale, bound, shards=(), held_as=jnp.bfloat16):
    drawn = jax.random.normal(own_key, shape, jnp.float32) * scale
    if len(shards) > 0:
        drawn = shard_levels(own_key, shape, shards, -0.22, 0.18) * drawn
    return jnp.clip(drawn, min=-bound, max=bound).astype(held_as)


def setup_inputs(seed: int = 0, part: int = 0) -> dict:
    keys = jax.random.split(jax.random.key(seed), 18)
    own_keys = jax.random.split(jax.random.fold_in(keys[17], part), 18)
    tokens = draw_tokens(jax.random.fold_in(jax.random.fold_in(keys[17], part), 71), part)
    mix_gain = jnp.clip(1.0 + 0.18 * jax.random.normal(keys[1], (D,), jnp.float32), 0.099609375, 1.8984375).astype(jnp.bfloat16)
    w_conv_value = normal_values(keys[2], (D, CONV_WIDTH), D ** -0.5, 0.125, ((0, 4), (1, 4)))
    w_conv_outer = normal_values(keys[3], (D, CONV_WIDTH), D ** -0.5, 0.125, ((0, 4), (1, 4)))
    w_conv_inner = normal_values(keys[4], (D, CONV_WIDTH), D ** -0.5, 0.125, ((0, 4), (1, 4)))
    conv_kernel = normal_values(keys[5], (TAPS, CONV_WIDTH), TAPS ** -0.5, 3.5, ((1, 4),))
    w_q_down = normal_values(keys[6], (D, Q_LATENT), D ** -0.5, 0.125, ((1, 4),))
    w_kv_down = normal_values(keys[7], (D, KV_LATENT), D ** -0.5, 0.125, ((1, 4),))
    w_rope_key = normal_values(keys[8], (D, ROPE), D ** -0.5, 0.125)
    q_gain = draw_q_gain(jax.random.fold_in(keys[17], 71), part)
    kv_gain = jnp.clip(1.0 + 0.18 * jax.random.normal(keys[10], (KV_LATENT,), jnp.float32), 0.099609375, 1.8984375).astype(jnp.bfloat16)
    w_q_nope = normal_values(keys[11], (Q_LATENT, MLA_HEADS * NOPE), Q_LATENT ** -0.5, 0.25, ((1, 4),))
    w_q_rope = normal_values(keys[12], (Q_LATENT, MLA_HEADS * ROPE), Q_LATENT ** -0.5, 0.25, ((1, 4),))
    w_k_nope = normal_values(keys[13], (KV_LATENT, MLA_HEADS * NOPE), KV_LATENT ** -0.5, 0.375, ((1, 4),))
    w_value = normal_values(keys[14], (KV_LATENT, MLA_HEADS * VALUE), KV_LATENT ** -0.5, 0.375, ((1, 4),))
    w_out_conv = normal_values(keys[15], (CONV_WIDTH, D), CONV_WIDTH ** -0.5, 0.1875, ((0, 4),))
    w_out_attn = normal_values(keys[16], (MLA_HEADS * VALUE, D), (max(1, MLA_HEADS * VALUE // 64)) ** -0.5, 1.5, ((0, 4),))
    return dict(tokens=tokens, mix_gain=mix_gain, w_conv_value=w_conv_value, w_conv_outer=w_conv_outer, w_conv_inner=w_conv_inner, conv_kernel=conv_kernel, w_q_down=w_q_down, w_kv_down=w_kv_down, w_rope_key=w_rope_key, q_gain=q_gain, kv_gain=kv_gain, w_q_nope=w_q_nope, w_q_rope=w_q_rope, w_k_nope=w_k_nope, w_value=w_value, w_out_conv=w_out_conv, w_out_attn=w_out_attn)


EPS = 1e-06
THETA = 10000.0

def rms_scale(values):
    return lax.rsqrt(lax.optimization_barrier(jnp.mean(values * values, axis=-1, keepdims=True)) + EPS)

def angles(positions, width):
    inverse = THETA ** (-jnp.arange(0, width, 2, dtype=jnp.float32) / width)
    phase = positions[:, None] * inverse[None, :]
    phase = jnp.concatenate([phase, phase], axis=-1)
    return (jnp.cos(phase), jnp.sin(phase))

def turned(values, cosine, sine):
    half = values.shape[-1] // 2
    first = values[..., :half]
    second = values[..., half:]
    return values * cosine + jnp.concatenate([-second, first], axis=-1) * sine

def reference(tokens, mix_gain, w_conv_value, w_conv_outer, w_conv_inner, conv_kernel, w_q_down, w_kv_down, w_rope_key, q_gain, kv_gain, w_q_nope, w_q_rope, w_k_nope, w_value, w_out_conv, w_out_attn):
    f32 = jnp.float32
    bf16 = jnp.bfloat16
    inputs = tokens.astype(f32)
    row_scale = rms_scale(inputs)
    scaled = (inputs * mix_gain.astype(f32)).astype(bf16)

    def project(weight):
        return (row_scale * jnp.dot(scaled, weight, preferred_element_type=f32)).astype(bf16)
    conv_value = project(w_conv_value)
    conv_outer = project(w_conv_outer)
    conv_inner = project(w_conv_inner)
    q_latent = project(w_q_down)
    kv_latent = project(w_kv_down)
    rope_raw = project(w_rope_key)
    gated = (conv_inner.astype(f32) * conv_value.astype(f32)).astype(bf16)
    padded = jnp.pad(gated.astype(f32), ((1, 1), (0, 0)))
    kernel = conv_kernel.astype(f32)
    conv_out = padded[:-2] * kernel[0] + padded[1:-1] * kernel[1] + padded[2:] * kernel[2]
    y_conv = (conv_outer.astype(f32) * conv_out).astype(bf16)
    q_float = q_latent.astype(f32)
    q_normed = (q_float * rms_scale(q_float) * q_gain.astype(f32)).astype(bf16)
    kv_float = kv_latent.astype(f32)
    kv_normed = (kv_float * rms_scale(kv_float) * kv_gain.astype(f32)).astype(bf16)
    count = tokens.shape[0]
    heads = w_q_nope.shape[1] // NOPE
    positions = jnp.arange(count, dtype=f32)
    cosine, sine = angles(positions, ROPE)
    q_nope = jnp.dot(q_normed, w_q_nope, preferred_element_type=f32).astype(bf16).reshape(count, heads, NOPE)
    q_rope_raw = jnp.dot(q_normed, w_q_rope, preferred_element_type=f32).reshape(count, heads, ROPE)
    q_rope = turned(q_rope_raw, cosine[:, None, :], sine[:, None, :]).astype(bf16)
    k_nope = jnp.dot(kv_normed, w_k_nope, preferred_element_type=f32).astype(bf16).reshape(count, heads, NOPE)
    values = jnp.dot(kv_normed, w_value, preferred_element_type=f32).astype(bf16).reshape(count, heads, VALUE)
    k_rope = turned(rope_raw.astype(f32), cosine, sine).astype(bf16)
    factor = (NOPE + ROPE) ** (-0.5)
    block = 128 if count % 128 == 0 else count
    keys_f = k_nope.astype(f32)
    rope_f = k_rope.astype(f32)
    values_f = values.astype(f32)

    def attend(pieces):
        query_nope, query_rope = pieces
        scores = jnp.einsum('qhd,khd->qhk', query_nope.astype(f32), keys_f)
        scores = scores + jnp.einsum('qhr,kr->qhk', query_rope.astype(f32), rope_f)
        scores = scores * factor
        peak = lax.optimization_barrier(jnp.max(scores, axis=-1, keepdims=True))
        weights = jnp.exp(scores - peak)
        total = lax.optimization_barrier(jnp.sum(weights, axis=-1))
        summed = jnp.einsum('qhk,khd->qhd', weights.astype(bf16).astype(f32), values_f)
        return (summed / total[..., None]).astype(bf16)
    blocks = count // block
    result = lax.map(attend, (q_nope.reshape(blocks, block, heads, NOPE), q_rope.reshape(blocks, block, heads, ROPE)))
    y_attn = result.reshape(count, heads * VALUE)
    conv_share = y_conv.shape[1] // N_TP
    attn_share = y_attn.shape[1] // N_TP
    summed = jnp.zeros((count, w_out_conv.shape[1]), f32)
    for index in range(N_TP):
        conv_rows = slice(index * conv_share, (index + 1) * conv_share)
        attn_rows = slice(index * attn_share, (index + 1) * attn_share)
        partial_sum = jnp.dot(y_conv[:, conv_rows], w_out_conv[conv_rows], preferred_element_type=f32)
        partial_sum = partial_sum + jnp.dot(y_attn[:, attn_rows], w_out_attn[attn_rows], preferred_element_type=f32)
        summed = summed + lax.optimization_barrier(partial_sum.astype(bf16)).astype(f32)
    return summed.astype(bf16)
```

```python
import functools

import jax
import jax.numpy as jnp
import numpy as np
from jax import lax
from jax.experimental import pallas as pl
from jax.experimental.pallas import tpu as pltpu
from jax.sharding import PartitionSpec as P

MESH = pl.DeviceIdType.MESH

D = 2048
NOPE = 64
ROPE = 32
VALUE = 64


EPS = 1e-06
THETA = 10000.0


def with_halo(x, sides, width):
    for axis, dim in sides:
        size, length = (lax.axis_size(axis), x.shape[dim])
        up = [(i, (i + 1) % size) for i in range(size - 1)]
        down = [(j, i) for i, j in up]
        last = lax.slice_in_dim(x, length - width, length, axis=dim)
        first = lax.slice_in_dim(x, 0, width, axis=dim)
        before = lax.ppermute(last, axis, up)
        after = lax.ppermute(first, axis, down)
        x = jnp.concatenate([before, x, after], axis=dim)
    return x


def rms_scale(values):
    return lax.rsqrt(jnp.mean(values * values, axis=-1, keepdims=True) + EPS)


def angles(positions, width):
    inverse = THETA ** (-jnp.arange(0, width, 2, dtype=jnp.float32) / width)
    phase = positions[:, None] * inverse[None, :]
    phase = jnp.concatenate([phase, phase], axis=-1)
    return (jnp.cos(phase), jnp.sin(phase))


def turned(values, cosine, sine):
    half = values.shape[-1] // 2
    first = values[..., :half]
    second = values[..., half:]
    return values * cosine + jnp.concatenate([-second, first], axis=-1) * sine


def block_rows(count):
    for candidate in range(min(count, 1024), 0, -1):
        if count % candidate == 0 and candidate % 128 == 0:
            return candidate
    for candidate in range(min(count, 1024), 0, -1):
        if count % candidate == 0:
            return candidate
    return count


def gathered_weights(
    tokens,
    mix_gain,
    w_conv_value,
    w_conv_outer,
    w_conv_inner,
    conv_kernel,
    w_q_down,
    w_kv_down,
    w_rope_key,
    q_gain,
    kv_gain,
    w_q_nope,
    w_q_rope,
    w_k_nope,
    w_value,
    w_out_conv,
    w_out_attn,
):
    f32 = jnp.float32
    bf16 = jnp.bfloat16
    rows = tokens.shape[0]
    conv_value_w, conv_outer_w, conv_inner_w = (
        lax.all_gather(w_conv_value, "sp", axis=0, tiled=True),
        lax.all_gather(w_conv_outer, "sp", axis=0, tiled=True),
        lax.all_gather(w_conv_inner, "sp", axis=0, tiled=True),
    )
    matrices = (conv_value_w, conv_outer_w, conv_inner_w, w_q_down, w_kv_down, w_rope_key)
    gain = mix_gain.astype(f32)
    piece_f = lax.all_gather(tokens, "tp", axis=1, tiled=True).astype(f32)
    scaled = (piece_f * gain).astype(bf16)
    updated = tuple((jnp.dot(scaled, matrix, preferred_element_type=f32) for matrix in matrices))
    squares = jnp.sum(piece_f * piece_f, axis=1)
    row_scale = lax.rsqrt(squares / D + EPS)[:, None]
    conv_value, conv_outer, conv_inner, q_part, kv_part, rope_raw = [
        (row_scale * total).astype(bf16) for total in updated
    ]
    gated = (conv_inner.astype(f32) * conv_value.astype(f32)).astype(bf16)
    padded = with_halo(gated, (("sp", 0),), 1).astype(f32)
    kernel = conv_kernel.astype(f32)
    conv_out = padded[:-2] * kernel[0] + padded[1:-1] * kernel[1] + padded[2:] * kernel[2]
    y_conv = (conv_outer.astype(f32) * conv_out).astype(bf16)
    q_latent, kv_latent = (
        lax.all_gather(q_part, "tp", axis=1, tiled=True),
        lax.all_gather(kv_part, "tp", axis=1, tiled=True),
    )
    q_float = q_latent.astype(f32)
    q_normed = (q_float * rms_scale(q_float) * q_gain.astype(f32)).astype(bf16)
    kv_float = kv_latent.astype(f32)
    kv_normed = (kv_float * rms_scale(kv_float) * kv_gain.astype(f32)).astype(bf16)
    heads = w_q_nope.shape[1] // NOPE
    positions = (lax.axis_index("sp") * rows + jnp.arange(rows, dtype=jnp.int32)).astype(f32)
    cosine, sine = angles(positions, ROPE)
    q_nope = (
        jnp.dot(q_normed, w_q_nope, preferred_element_type=f32)
        .astype(bf16)
        .reshape(rows, heads, NOPE)
    )
    q_rope_raw = jnp.dot(q_normed, w_q_rope, preferred_element_type=f32).reshape(rows, heads, ROPE)
    q_rope = turned(q_rope_raw, cosine[:, None, :], sine[:, None, :]).astype(bf16)
    k_rope = turned(rope_raw.astype(f32), cosine, sine).astype(bf16)
    factor = (NOPE + ROPE) ** (-0.5)

    def attend(state, key_block, value_block, rope_block):
        peak, total, summed = state
        count = key_block.shape[0]
        keys3 = key_block.reshape(count, heads, NOPE)
        values3 = value_block.reshape(count, heads, VALUE)
        scores = jnp.einsum("qhd,khd->qhk", q_nope, keys3, preferred_element_type=f32)
        scores = scores + jnp.einsum("qhr,kr->qhk", q_rope, rope_block, preferred_element_type=f32)
        scores = scores * factor
        new_peak = jnp.maximum(peak, jnp.max(scores, axis=-1))
        fade = jnp.exp(peak - new_peak)
        weights = jnp.exp(scores - new_peak[..., None])
        total = total * fade + jnp.sum(weights, axis=-1)
        summed = summed * fade[..., None] + jnp.einsum(
            "qhk,khd->qhd", weights.astype(bf16), values3, preferred_element_type=f32
        )
        return (new_peak, total, summed)

    start_state = (
        jnp.full((rows, heads), -jnp.inf, f32),
        jnp.zeros((rows, heads), f32),
        jnp.zeros((rows, heads, VALUE), f32),
    )
    latent = lax.all_gather(kv_normed, "sp", axis=0, tiled=True)
    rope_keys = lax.all_gather(k_rope, "sp", axis=0, tiled=True)
    size = block_rows(latent.shape[0])
    count = latent.shape[0] // size

    def one_block(carry, blocks):
        latent_block, rope_block = blocks
        key_block = jnp.dot(latent_block, w_k_nope, preferred_element_type=f32).astype(bf16)
        value_block = jnp.dot(latent_block, w_value, preferred_element_type=f32).astype(bf16)
        return (attend(carry, key_block, value_block, rope_block), None)

    carry, ignored = lax.scan(
        one_block,
        start_state,
        (
            latent.reshape(count, size, latent.shape[1]),
            rope_keys.reshape(count, size, rope_keys.shape[1]),
        ),
    )
    peak, total, summed = carry
    y_attn = (summed / total[..., None]).astype(bf16).reshape(rows, heads * VALUE)
    partial_sum = jnp.dot(y_conv, w_out_conv, preferred_element_type=f32) + jnp.dot(
        y_attn, w_out_attn, preferred_element_type=f32
    )
    return (
        lax.psum_scatter(partial_sum.astype(jnp.bfloat16), "tp", scatter_dimension=1, tiled=True)
        .astype(jnp.float32)
        .astype(bf16)
    )


def copy_to(src, dst, send, recv, sp, tp):
    return pltpu.make_async_remote_copy(
        src_ref=src,
        dst_ref=dst,
        send_sem=send,
        recv_sem=recv,
        device_id={"sp": sp, "tp": tp},
        device_id_type=MESH,
    )


def dot(a, b):
    return jnp.dot(a, b, preferred_element_type=jnp.float32)


def dot_t(a, b):
    return lax.dot_general(a, b, (((1,), (1,)), ((), ())), preferred_element_type=jnp.float32)


def mixer_kernel(
    n,
    tokens_h,
    gain_h,
    wcv_h,
    wco_h,
    wci_h,
    taps_h,
    wq_h,
    wkv_h,
    wr_h,
    qg_h,
    kvg_h,
    wqn_h,
    wqr_h,
    wkn_h,
    wva_h,
    woc_h,
    woa_h,
    cos_h,
    sin_h,
    out_ref,
    tok,
    gain,
    wcv,
    wco,
    wci,
    taps,
    wq,
    wkv,
    wr,
    qg,
    kvg,
    wqn,
    wqr,
    wkn,
    wva,
    woc,
    woa,
    cosine,
    sine,
    xt,
    part,
    got,
    own,
    qp,
    kvp,
    kvr,
    gate,
    before,
    after,
    acc,
    put_near,
    got_near,
    put_far,
    got_far,
    load_sem,
    s_tok,
    r_tok,
    s_z,
    r_z,
    s_xf,
    r_xf,
    s_q,
    r_q,
    s_kv,
    r_kv,
    s_kz,
    r_kz,
    s_kf,
    r_kf,
    s_p,
    r_p,
    s_h,
    r_h,
    s_o,
    r_o,
):
    f32, bf16 = jnp.float32, jnp.bfloat16
    s, t = lax.axis_index("sp"), lax.axis_index("tp")
    core = lax.rem(t, 2)
    near = t + 1 - 2 * core
    far = lax.rem(t + 2, n)
    diag = lax.rem(near + 2, n)
    rows, width = tok.shape[1], tok.shape[2]
    cw = wcv.shape[1]
    tp_peers = (near, far, diag)

    loads = [
        (tokens_h, tok.at[t]),
        (gain_h, gain),
        (wq_h, wq),
        (wkv_h, wkv),
        (wr_h, wr),
        (wcv_h, wcv),
        (wco_h, wco),
        (wci_h, wci),
        (taps_h, taps),
        (qg_h, qg),
        (kvg_h, kvg),
        (wqn_h, wqn),
        (wqr_h, wqr),
        (wkn_h, wkn),
        (wva_h, wva),
        (cos_h.at[s], cosine),
        (sin_h.at[s], sine),
    ]
    for j in range(n):
        columns = pl.ds(j * width, width)
        loads.append((woa_h.at[:, columns], woa.at[j]))
        loads.append((woc_h.at[:, columns], woc.at[j]))
    loads = [pltpu.make_async_copy(a, b, load_sem.at[i]) for i, (a, b) in enumerate(loads)]
    for load in loads:
        load.start()

    barrier = pltpu.get_barrier_semaphore()
    for peer in tp_peers:
        pl.semaphore_signal(barrier, inc=1, device_id={"sp": s, "tp": peer}, device_id_type=MESH)
    for k in range(1, n):
        pl.semaphore_signal(
            barrier, inc=1, device_id={"sp": lax.rem(s + k, n), "tp": t}, device_id_type=MESH
        )
    loads[0].wait()
    pl.semaphore_wait(barrier, 2 * (n - 1))

    tok_far = copy_to(tok.at[t], tok.at[t], s_tok.at[0], r_tok.at[0], s, far)
    tok_near = copy_to(tok.at[t], tok.at[t], s_tok.at[1], r_tok.at[1], s, near)
    tok_fwd = copy_to(tok.at[far], tok.at[far], s_tok.at[2], r_tok.at[2], s, near)
    z_own = copy_to(tok.at[t], xt.at[s], s_z.at[0], r_z.at[s], t, t)
    z_far = copy_to(tok.at[far], xt.at[s], s_z.at[1], r_z.at[s], far, t)
    tok_far.start()

    @pl.when(t != s)
    def _():
        z_own.start()

    tok_near.start()
    for load in loads[1:]:
        load.wait()
    copy_to(tok.at[far], tok.at[far], s_tok.at[0], r_tok.at[0], s, far).wait_recv()
    tok_fwd.start()

    @pl.when(far != s)
    def _():
        z_far.start()

    copy_to(tok.at[near], tok.at[near], s_tok.at[1], r_tok.at[1], s, near).wait_recv()
    copy_to(tok.at[diag], tok.at[diag], s_tok.at[2], r_tok.at[2], s, near).wait_recv()

    squares = jnp.zeros((rows, 1), f32)
    q_sum = jnp.zeros((rows, wq.shape[2]), f32)
    kv_sum = jnp.zeros((rows, wkv.shape[0]), f32)
    r_sum = jnp.zeros((rows, wr.shape[0]), f32)
    for j in range(n):
        piece = tok[j].astype(f32)
        squares = squares + jnp.sum(piece * piece, axis=1, keepdims=True)
        scaled = (piece * gain[j * width : (j + 1) * width][None, :].astype(f32)).astype(bf16)
        kv_sum = kv_sum + dot_t(scaled, wkv[:, j * width : (j + 1) * width])
        r_sum = r_sum + dot_t(scaled, wr[:, j * width : (j + 1) * width])
        q_sum = q_sum + dot(scaled, wq[j])
    row_scale = lax.rsqrt(squares / (n * width) + EPS)
    kw = wkv.shape[0]
    place = (
        lax.broadcasted_iota(jnp.int32, (kw, 2 * kw), 1)
        == lax.broadcasted_iota(jnp.int32, (kw, 2 * kw), 0) + kw * core
    )
    place = jnp.where(place, 1.0, 0.0).astype(bf16)
    kvp[t] = dot((row_scale * kv_sum).astype(bf16), place).astype(bf16)
    kv_sends = [
        copy_to(kvp.at[t], kvp.at[t], s_kv.at[i], r_kv.at[i], s, p) for i, p in enumerate(tp_peers)
    ]
    for copy in (kv_sends[1], kv_sends[2], kv_sends[0]):
        copy.start()
    qp[t] = (row_scale * q_sum).astype(bf16)
    q_sends = [
        copy_to(qp.at[t], qp.at[t], s_q.at[i], r_q.at[i], s, p) for i, p in enumerate(tp_peers)
    ]
    for copy in (q_sends[1], q_sends[2], q_sends[0]):
        copy.start()

    meets = lax.rem(s, 2) == core
    my_gain = gain[pl.ds(pl.multiple_of(s * width, width), width)][None, :].astype(f32)
    p_sends = []

    def conv_part(block):
        scaled = (block.astype(f32) * my_gain).astype(bf16)
        return dot(scaled, wcv[...]), dot(scaled, wco[...]), dot(scaled, wci[...])

    upper = lax.div(s, n // 2)
    step = 1 - 2 * upper
    inner = s + upper * (n - 1 - 2 * s)

    def conv_block(i, mirrored, way, onward):
        z = mirrored + upper * (n - 1 - 2 * mirrored)
        fwd = copy_to(xt.at[z], xt.at[z], s_xf.at[i], r_xf.at[z], s, near)

        @pl.when(meets)
        def _():
            copy_to(xt.at[z], xt.at[z], s_z.at[0], r_z.at[z], z, t).wait_recv()
            fwd.start()

        @pl.when(jnp.logical_not(meets))
        def _():
            fwd.wait_recv()

        products = conv_part(xt[z])
        for m in (0, 2, 1):
            product = products[m]
            copy = copy_to(
                part.at[i, m], got.at[way, z, m], s_p.at[i, m], r_p.at[way, z, m], onward, t
            )

            @pl.when(inner > 0)
            def _():
                copy.wait_recv()
                part[i, m] = (product + got[way, z, m].astype(f32)).astype(bf16)

            @pl.when(inner == 0)
            def _():
                part[i, m] = product.astype(bf16)

            copy.start()
            p_sends.append(copy)
        p_sends.append(fwd)

    for i, product in enumerate(conv_part(tok[s])):
        own[i] = product

    cos_v, sin_v = cosine[...], sine[...]
    lanes = cos_v.shape[1]
    turn_r = lax.broadcasted_iota(jnp.int32, (lanes, lanes), 0)
    turn_c = lax.broadcasted_iota(jnp.int32, (lanes, lanes), 1)
    half = ROPE // 2
    low = lax.rem(turn_c, ROPE) < half
    turn = jnp.where(
        low & (turn_r == turn_c + half), -1.0, jnp.where((~low) & (turn_r == turn_c - half), 1.0, 0.0)
    ).astype(bf16)
    spread_r = lax.broadcasted_iota(jnp.int32, (ROPE, lanes), 0)
    spread_c = lax.broadcasted_iota(jnp.int32, (ROPE, lanes), 1)
    spread = jnp.where(lax.rem(spread_c, ROPE) == spread_r, 1.0, 0.0).astype(bf16)
    rope_raw = dot((row_scale * r_sum).astype(bf16), spread).astype(bf16)
    k_rope = (rope_raw.astype(f32) * cos_v + dot(rope_raw, turn) * sin_v).astype(bf16)
    for i, p in enumerate(tp_peers):
        copy_to(kvp.at[p], kvp.at[p], s_kv.at[i], r_kv.at[i], s, p).wait_recv()
    kv_float = jnp.concatenate(
        [kvp[j].astype(f32) + kvp[j + 1].astype(f32) for j in range(0, n, 2)], axis=1
    )
    kv_scale = lax.rsqrt(jnp.mean(kv_float * kv_float, axis=1, keepdims=True) + EPS)
    lat = kv_float.shape[1]
    kvr[s, :, :lat] = (kv_float * kv_scale * kvg[...][None, :].astype(f32)).astype(bf16)
    kvr[s, :, lat:] = k_rope
    def quarter(index):
        return pl.ds(pl.multiple_of(index * (rows // n), rows // n), rows // n)

    mine = quarter(t)
    kz_sends = []
    for k in (2, 1, 3):
        z = lax.rem(s + k, n)
        copy = copy_to(
            kvr.at[s, mine], kvr.at[s, mine], s_kz.at[k - 1], r_kz.at[k - 1], z, t
        )
        copy.start()
        kz_sends.append(copy)

    conv_block(0, n - 1, upper, s + step)

    for i, p in enumerate(tp_peers):
        copy_to(qp.at[p], qp.at[p], s_q.at[i], r_q.at[i], s, p).wait_recv()
    q_float = [qp[j].astype(f32) for j in range(n)]
    qw = q_float[0].shape[1]
    q_square = sum(jnp.sum(q * q, axis=1, keepdims=True) for q in q_float)
    q_scale = lax.rsqrt(q_square / (n * qw) + EPS)
    q_normed = jnp.concatenate(
        [(q * q_scale * qg[j * qw : (j + 1) * qw][None, :].astype(f32)).astype(bf16) for j, q in enumerate(q_float)], axis=1
    )
    q_nope = dot(q_normed, wqn[...]).astype(bf16)
    q_raw = dot(q_normed, wqr[...])
    w_turned = dot(wqr[...], turn).astype(bf16)
    q_rope = (q_raw * cos_v + dot(q_normed, w_turned) * sin_v).astype(bf16)

    conv_block(1, n - 2, upper, s + step)
    kf_sends = []
    for k in (2, 1, 3):
        z = lax.rem(s + n - k, n)
        copy_to(
            kvr.at[z, mine], kvr.at[z, mine], s_kz.at[k - 1], r_kz.at[k - 1], z, t
        ).wait_recv()
        for i, p in enumerate(tp_peers):
            copy = copy_to(
                kvr.at[z, mine], kvr.at[z, mine], s_kf.at[k - 1, i], r_kf.at[k - 1, i], s, p
            )
            copy.start()
            kf_sends.append(copy)
    conv_block(2, 1 - inner, upper + inner * step, s + step * (1 - 2 * inner))
    for k in (2, 1, 3):
        z = lax.rem(s + n - k, n)
        for i, p in enumerate(tp_peers):
            rest = kvr.at[z, quarter(p)]
            copy_to(rest, rest, s_kf.at[k - 1, i], r_kf.at[k - 1, i], s, p).wait_recv()

    latent = jnp.concatenate([kvr[j, :, :lat] for j in range(n)], axis=0)
    ropes = jnp.concatenate([kvr[j, :, lat:] for j in range(n)], axis=0)
    keys = dot(latent, wkn[...]).astype(bf16)
    values = dot(latent, wva[...]).astype(bf16)
    heads = wqn.shape[1] // NOPE
    factor = (NOPE + ROPE) ** (-0.5)
    pair = 2 * NOPE
    lane = lax.broadcasted_iota(jnp.int32, (rows, pair), 1)
    lane_r = lax.broadcasted_iota(jnp.int32, (rows, lanes), 1)
    pieces = []
    for p in range(heads // 2):
        cut = slice(p * pair, (p + 1) * pair)
        key_pair = jnp.concatenate([keys[:, cut], ropes], axis=1)
        value_pair = values[:, cut]
        outs = []
        for i in range(2):
            h = 2 * p + i
            in_head = (lane >= i * NOPE) & (lane < (i + 1) * NOPE)
            in_rope = (lane_r >= h * ROPE) & (lane_r < (h + 1) * ROPE)
            query = jnp.concatenate(
                [
                    jnp.where(in_head, q_nope[:, cut].astype(f32), 0.0).astype(bf16),
                    jnp.where(in_rope, q_rope.astype(f32), 0.0).astype(bf16),
                ],
                axis=1,
            )
            scores = dot_t(query, key_pair) * factor
            peak = jnp.max(scores, axis=1, keepdims=True)
            weights = jnp.exp(scores - peak)
            total = jnp.sum(weights, axis=1, keepdims=True)
            outs.append(dot(weights.astype(bf16), value_pair) / total)
        pieces.append(jnp.where(lane < NOPE, outs[0], outs[1]).astype(bf16))
    y_attn = jnp.concatenate(pieces, axis=1)
    for j in range(n):
        acc[j] = dot(y_attn, woa[j])

    def take(m):
        for way in (1 - upper, upper):

            @pl.when((way == 1 - upper) | (inner > 0))
            def _():
                copy_to(
                    part.at[0, m], got.at[way, s, m], s_p.at[0, m], r_p.at[way, s, m], s, near
                ).wait_recv()
                own[m] = own[m] + got[way, s, m].astype(f32)

    take(0)
    take(2)

    def summed(i):
        return (row_scale * own[i]).astype(bf16).astype(f32)

    gated = (summed(2) * summed(0)).astype(bf16)
    gate[...] = gated
    edge = before.shape[0]
    up = copy_to(gate.at[pl.ds(rows - edge, edge)], before, s_h.at[0], r_h.at[0], s + 1, t)
    down = copy_to(gate.at[pl.ds(0, edge)], after, s_h.at[1], r_h.at[1], s - 1, t)

    @pl.when(s < n - 1)
    def _():
        up.start()

    @pl.when(s > 0)
    def _():
        down.start()

    take(1)
    conv_outer = summed(1)
    middle = gated.astype(f32)
    kernel = [taps[i : i + 1, :].astype(f32) for i in range(3)]
    row = lax.broadcasted_iota(jnp.int32, middle.shape, 0)
    previous = pltpu.roll(middle, 1, 0)
    following = pltpu.roll(middle, rows - 1, 0)

    @pl.when(s > 0)
    def _():
        up.wait_recv()

    @pl.when(s == 0)
    def _():
        before[...] = jnp.zeros_like(before)

    @pl.when(s < n - 1)
    def _():
        down.wait_recv()

    @pl.when(s == n - 1)
    def _():
        after[...] = jnp.zeros_like(after)

    first = before[...].astype(f32)[edge - 1 : edge, :]
    last = after[...].astype(f32)[0:1, :]
    previous = jnp.where(row == 0, first, previous)
    following = jnp.where(row == rows - 1, last, following)
    conv_out = previous * kernel[0] + middle * kernel[1] + following * kernel[2]
    y_conv = (conv_outer * conv_out).astype(bf16)

    def share(j):
        return acc[j] + dot(y_conv, woc[j])

    put_near[0] = share(diag).astype(bf16)
    o_diag = copy_to(put_near.at[0], got_near.at[0], s_o.at[0], r_o.at[0], s, near)
    o_diag.start()
    far_share = share(far).astype(bf16).astype(f32)
    o_diag.wait_recv()
    put_far[...] = (far_share + got_near[0].astype(f32)).astype(bf16)
    o_far = copy_to(put_far, got_far, s_o.at[1], r_o.at[1], s, far)
    o_far.start()
    put_near[1] = share(near).astype(bf16)
    o_near = copy_to(put_near.at[1], got_near.at[1], s_o.at[2], r_o.at[2], s, near)
    o_near.start()
    my_share = share(t).astype(bf16).astype(f32)
    o_near.wait_recv()
    my_share = my_share + got_near[1].astype(f32)

    tok_far.wait_send()
    tok_near.wait_send()
    tok_fwd.wait_send()

    @pl.when(t != s)
    def _():
        z_own.wait_send()

    @pl.when(far != s)
    def _():
        z_far.wait_send()

    for copy in kv_sends + q_sends + kz_sends + kf_sends:
        copy.wait_send()
    for i, copy in enumerate(p_sends):
        if i % 4 < 3:
            copy.wait_send()
        else:

            @pl.when(meets)
            def _():
                copy.wait_send()

    @pl.when(s < n - 1)
    def _():
        up.wait_send()

    @pl.when(s > 0)
    def _():
        down.wait_send()

    o_diag.wait_send()
    o_near.wait_send()
    o_far.wait()
    out_ref[...] = (my_share + got_far[...].astype(f32)).astype(bf16)


def fits(sp, tp, tokens, mix_gain, w_conv_value, *others):
    rows, width = tokens.shape
    return sp == tp == 4 and rows * sp <= width * tp and width % 128 == 0 and rows % 64 == 0


def fused(
    sp,
    tp,
    tokens,
    mix_gain,
    w_conv_value,
    w_conv_outer,
    w_conv_inner,
    conv_kernel,
    w_q_down,
    w_kv_down,
    w_rope_key,
    q_gain,
    kv_gain,
    w_q_nope,
    w_q_rope,
    w_k_nope,
    w_value,
    w_out_conv,
    w_out_attn,
):
    f32, bf16 = jnp.float32, jnp.bfloat16
    n = tp
    rows, width = tokens.shape
    heads = w_q_nope.shape[1] // NOPE
    inverse = np.float32(THETA) ** (-np.arange(0, ROPE, 2, dtype=np.float32) / np.float32(ROPE))
    phase = np.arange(sp * rows, dtype=np.float32)[:, None] * inverse[None, :].astype(np.float32)
    phase = np.tile(phase, (1, 2 * heads)).reshape(sp, rows, heads * ROPE)
    cosine, sine = np.cos(phase).astype(np.float32), np.sin(phase).astype(np.float32)
    operands = (
        tokens,
        mix_gain,
        w_conv_value,
        w_conv_outer,
        w_conv_inner,
        conv_kernel,
        w_q_down.reshape(n, width, -1),
        w_kv_down.T,
        w_rope_key.T,
        q_gain,
        kv_gain,
        w_q_nope,
        w_q_rope,
        w_k_nope,
        w_value,
        w_out_conv,
        w_out_attn,
        jnp.asarray(cosine),
        jnp.asarray(sine),
    )
    vm = pltpu.VMEM
    cw = w_conv_value.shape[1]
    lat = kv_gain.shape[0]
    lanes = heads * ROPE
    scratch = [vm((n, rows, width), bf16)]
    scratch += [vm(x.shape, x.dtype) for x in operands[1:15]]
    scratch += [vm((n, w_out_conv.shape[0], width), bf16)] * 2
    scratch += [vm((rows, lanes), f32)] * 2
    scratch += [
        vm((n, rows, width), bf16),
        vm((n - 1, 3, rows, cw), bf16),
        vm((2, n, 3, rows, cw), bf16),
        vm((3, rows, cw), f32),
        vm((n, rows, w_q_down.shape[1]), bf16),
        vm((n, rows, 2 * w_kv_down.shape[1]), bf16),
        vm((n, rows, lat + lanes), bf16),
        vm((rows, cw), bf16),
        vm((16, cw), bf16),
        vm((16, cw), bf16),
        vm((n, rows, width), f32),
        vm((2, rows, width), bf16),
        vm((2, rows, width), bf16),
        vm((rows, width), bf16),
        vm((rows, width), bf16),
    ]
    dma = pltpu.SemaphoreType.DMA
    scratch += [dma((17 + 2 * n,)), dma((3,)), dma((3,)), dma((2,)), dma((n,))]
    scratch += [dma((n - 1,)), dma((n,))]
    scratch += [dma((n - 1,))] * 6
    scratch += [dma((n - 1, n - 1))] * 2
    scratch += [dma((n - 1, 3)), dma((2, n, 3))]
    scratch += [dma((2,)), dma((2,)), dma((3,)), dma((3,))]
    return pl.pallas_call(
        functools.partial(mixer_kernel, n),
        out_shape=jax.ShapeDtypeStruct((rows, width), bf16),
        in_specs=[pl.BlockSpec(memory_space=pl.ANY)] * len(operands),
        out_specs=pl.BlockSpec(memory_space=pltpu.VMEM),
        scratch_shapes=scratch,
        compiler_params=pltpu.CompilerParams(collective_id=0, has_side_effects=True),
    )(*operands)


def solution(mesh):
    placed = (
        P(("grp", "sp"), "tp"),
        P(),
        P("sp", "tp"),
        P("sp", "tp"),
        P("sp", "tp"),
        P(None, "tp"),
        P(None, "tp"),
        P(None, "tp"),
        P(),
        P(),
        P(),
        P(None, "tp"),
        P(None, "tp"),
        P(None, "tp"),
        P(None, "tp"),
        P("tp", None),
        P("tp", None),
    )
    sp, tp = mesh.shape["sp"], mesh.shape["tp"]

    def per_device(*args):
        if fits(sp, tp, *args):
            return fused(sp, tp, *args)
        return gathered_weights(*args)

    return jax.shard_map(
        per_device, mesh=mesh, in_specs=placed, out_specs=P(("grp", "sp"), "tp"), check_vma=False
    )
```

```python
import functools

import jax
import jax.numpy as jnp
import numpy as np
from jax import lax
from jax.experimental import pallas as pl
from jax.experimental.pallas import tpu as pltpu
from jax.sharding import PartitionSpec as P

MESH = pl.DeviceIdType.MESH

D = 2048
NOPE = 64
ROPE = 32
VALUE = 64


EPS = 1e-06
THETA = 10000.0


def with_halo(x, sides, width):
    for axis, dim in sides:
        size, length = (lax.axis_size(axis), x.shape[dim])
        up = [(i, (i + 1) % size) for i in range(size - 1)]
        down = [(j, i) for i, j in up]
        last = lax.slice_in_dim(x, length - width, length, axis=dim)
        first = lax.slice_in_dim(x, 0, width, axis=dim)
        before = lax.ppermute(last, axis, up)
        after = lax.ppermute(first, axis, down)
        x = jnp.concatenate([before, x, after], axis=dim)
    return x


def rms_scale(values):
    return lax.rsqrt(jnp.mean(values * values, axis=-1, keepdims=True) + EPS)


def angles(positions, width):
    inverse = THETA ** (-jnp.arange(0, width, 2, dtype=jnp.float32) / width)
    phase = positions[:, None] * inverse[None, :]
    phase = jnp.concatenate([phase, phase], axis=-1)
    return (jnp.cos(phase), jnp.sin(phase))


def turned(values, cosine, sine):
    half = values.shape[-1] // 2
    first = values[..., :half]
    second = values[..., half:]
    return values * cosine + jnp.concatenate([-second, first], axis=-1) * sine


def block_rows(count):
    for candidate in range(min(count, 1024), 0, -1):
        if count % candidate == 0 and candidate % 128 == 0:
            return candidate
    for candidate in range(min(count, 1024), 0, -1):
        if count % candidate == 0:
            return candidate
    return count


def gathered_weights(
    tokens,
    mix_gain,
    w_conv_value,
    w_conv_outer,
    w_conv_inner,
    conv_kernel,
    w_q_down,
    w_kv_down,
    w_rope_key,
    q_gain,
    kv_gain,
    w_q_nope,
    w_q_rope,
    w_k_nope,
    w_value,
    w_out_conv,
    w_out_attn,
):
    f32 = jnp.float32
    bf16 = jnp.bfloat16
    rows = tokens.shape[0]
    conv_value_w, conv_outer_w, conv_inner_w = (
        lax.all_gather(w_conv_value, "sp", axis=0, tiled=True),
        lax.all_gather(w_conv_outer, "sp", axis=0, tiled=True),
        lax.all_gather(w_conv_inner, "sp", axis=0, tiled=True),
    )
    matrices = (conv_value_w, conv_outer_w, conv_inner_w, w_q_down, w_kv_down, w_rope_key)
    gain = mix_gain.astype(f32)
    piece_f = lax.all_gather(tokens, "tp", axis=1, tiled=True).astype(f32)
    scaled = (piece_f * gain).astype(bf16)
    updated = tuple((jnp.dot(scaled, matrix, preferred_element_type=f32) for matrix in matrices))
    squares = jnp.sum(piece_f * piece_f, axis=1)
    row_scale = lax.rsqrt(squares / D + EPS)[:, None]
    conv_value, conv_outer, conv_inner, q_part, kv_part, rope_raw = [
        (row_scale * total).astype(bf16) for total in updated
    ]
    gated = (conv_inner.astype(f32) * conv_value.astype(f32)).astype(bf16)
    padded = with_halo(gated, (("sp", 0),), 1).astype(f32)
    kernel = conv_kernel.astype(f32)
    conv_out = padded[:-2] * kernel[0] + padded[1:-1] * kernel[1] + padded[2:] * kernel[2]
    y_conv = (conv_outer.astype(f32) * conv_out).astype(bf16)
    q_latent, kv_latent = (
        lax.all_gather(q_part, "tp", axis=1, tiled=True),
        lax.all_gather(kv_part, "tp", axis=1, tiled=True),
    )
    q_float = q_latent.astype(f32)
    q_normed = (q_float * rms_scale(q_float) * q_gain.astype(f32)).astype(bf16)
    kv_float = kv_latent.astype(f32)
    kv_normed = (kv_float * rms_scale(kv_float) * kv_gain.astype(f32)).astype(bf16)
    heads = w_q_nope.shape[1] // NOPE
    positions = (lax.axis_index("sp") * rows + jnp.arange(rows, dtype=jnp.int32)).astype(f32)
    cosine, sine = angles(positions, ROPE)
    q_nope = (
        jnp.dot(q_normed, w_q_nope, preferred_element_type=f32)
        .astype(bf16)
        .reshape(rows, heads, NOPE)
    )
    q_rope_raw = jnp.dot(q_normed, w_q_rope, preferred_element_type=f32).reshape(rows, heads, ROPE)
    q_rope = turned(q_rope_raw, cosine[:, None, :], sine[:, None, :]).astype(bf16)
    k_rope = turned(rope_raw.astype(f32), cosine, sine).astype(bf16)
    factor = (NOPE + ROPE) ** (-0.5)

    def attend(state, key_block, value_block, rope_block):
        peak, total, summed = state
        count = key_block.shape[0]
        keys3 = key_block.reshape(count, heads, NOPE)
        values3 = value_block.reshape(count, heads, VALUE)
        scores = jnp.einsum("qhd,khd->qhk", q_nope, keys3, preferred_element_type=f32)
        scores = scores + jnp.einsum("qhr,kr->qhk", q_rope, rope_block, preferred_element_type=f32)
        scores = scores * factor
        new_peak = jnp.maximum(peak, jnp.max(scores, axis=-1))
        fade = jnp.exp(peak - new_peak)
        weights = jnp.exp(scores - new_peak[..., None])
        total = total * fade + jnp.sum(weights, axis=-1)
        summed = summed * fade[..., None] + jnp.einsum(
            "qhk,khd->qhd", weights.astype(bf16), values3, preferred_element_type=f32
        )
        return (new_peak, total, summed)

    start_state = (
        jnp.full((rows, heads), -jnp.inf, f32),
        jnp.zeros((rows, heads), f32),
        jnp.zeros((rows, heads, VALUE), f32),
    )
    latent = lax.all_gather(kv_normed, "sp", axis=0, tiled=True)
    rope_keys = lax.all_gather(k_rope, "sp", axis=0, tiled=True)
    size = block_rows(latent.shape[0])
    count = latent.shape[0] // size

    def one_block(carry, blocks):
        latent_block, rope_block = blocks
        key_block = jnp.dot(latent_block, w_k_nope, preferred_element_type=f32).astype(bf16)
        value_block = jnp.dot(latent_block, w_value, preferred_element_type=f32).astype(bf16)
        return (attend(carry, key_block, value_block, rope_block), None)

    carry, ignored = lax.scan(
        one_block,
        start_state,
        (
            latent.reshape(count, size, latent.shape[1]),
            rope_keys.reshape(count, size, rope_keys.shape[1]),
        ),
    )
    peak, total, summed = carry
    y_attn = (summed / total[..., None]).astype(bf16).reshape(rows, heads * VALUE)
    partial_sum = jnp.dot(y_conv, w_out_conv, preferred_element_type=f32) + jnp.dot(
        y_attn, w_out_attn, preferred_element_type=f32
    )
    return (
        lax.psum_scatter(partial_sum.astype(jnp.bfloat16), "tp", scatter_dimension=1, tiled=True)
        .astype(jnp.float32)
        .astype(bf16)
    )


def copy_to(src, dst, send, recv, sp, tp, **group):
    return pltpu.make_async_remote_copy(
        src_ref=src,
        dst_ref=dst,
        send_sem=send,
        recv_sem=recv,
        device_id={"sp": sp, "tp": tp, **group},
        device_id_type=MESH,
    )


def dot(a, b):
    return jnp.dot(a, b, preferred_element_type=jnp.float32)


def dot_t(a, b):
    return lax.dot_general(a, b, (((1,), (1,)), ((), ())), preferred_element_type=jnp.float32)


def mixer_kernel(
    n,
    tokens_h,
    gain_h,
    wcv_h,
    wco_h,
    wci_h,
    taps_h,
    wq_h,
    wkv_h,
    wr_h,
    qg_h,
    kvg_h,
    wqn_h,
    wqr_h,
    wkn_h,
    wva_h,
    woc_h,
    woa_h,
    cos_h,
    sin_h,
    out_ref,
    tok,
    gain,
    wcv,
    wco,
    wci,
    taps,
    wq,
    wkv,
    wr,
    qg,
    kvg,
    wqn,
    wqr,
    wkn,
    wva,
    woc,
    woa,
    cosine,
    sine,
    wx,
    xt,
    part,
    got,
    own,
    qp,
    kvp,
    kvr,
    gate,
    before,
    after,
    acc,
    put_near,
    got_near,
    put_far,
    got_far,
    load_sem,
    s_tok,
    r_tok,
    s_z,
    r_z,
    s_xf,
    r_xf,
    s_w,
    r_w,
    s_y,
    r_y,
    s_q,
    r_q,
    s_kv,
    r_kv,
    s_kz,
    r_kz,
    s_kf,
    r_kf,
    s_p,
    r_p,
    s_h,
    r_h,
    s_o,
    r_o,
):
    f32, bf16 = jnp.float32, jnp.bfloat16
    g, s, t = lax.axis_index("grp"), lax.axis_index("sp"), lax.axis_index("tp")
    core = lax.rem(t, 2)
    near = t + 1 - 2 * core
    far = lax.rem(t + 2, n)
    diag = lax.rem(near + 2, n)
    rows, width = tok.shape[1], tok.shape[2]
    cw = wcv.shape[1]
    tp_peers = (near, far, diag)
    upper = lax.div(s, n // 2)
    side = lax.div(t, 2)
    is_hub = (s == 1) | (s == n - 2)
    mate = s + 1 - 2 * lax.rem(s, 2)
    hub_over = n // 2 - upper
    end_over = (n - 1) * (1 - upper)

    loads = [
        (tokens_h, tok.at[t]),
        (gain_h, gain),
        (wq_h, wq),
        (wkv_h, wkv),
        (wr_h, wr),
        (wcv_h, wcv),
        (wco_h, wco),
        (wci_h, wci),
        (taps_h, taps),
        (qg_h, qg),
        (kvg_h, kvg),
        (wqn_h, wqn),
        (wqr_h, wqr),
        (wkn_h, wkn),
        (wva_h, wva),
        (cos_h.at[s], cosine),
        (sin_h.at[s], sine),
    ]
    for j in range(n):
        columns = pl.ds(j * width, width)
        loads.append((woa_h.at[:, columns], woa.at[j]))
        loads.append((woc_h.at[:, columns], woc.at[j]))
    loads = [pltpu.make_async_copy(a, b, load_sem.at[i]) for i, (a, b) in enumerate(loads)]
    for load in loads:
        load.start()

    barrier = pltpu.get_barrier_semaphore()
    for peer in tp_peers:
        pl.semaphore_signal(barrier, inc=1, device_id={"sp": s, "tp": peer}, device_id_type=MESH)
    for k in range(1, n):
        pl.semaphore_signal(
            barrier, inc=1, device_id={"sp": lax.rem(s + k, n), "tp": t}, device_id_type=MESH
        )
    pl.semaphore_signal(
        barrier, inc=1, device_id={"grp": 1 - g, "sp": s, "tp": t}, device_id_type=MESH
    )
    loads[0].wait()
    pl.semaphore_wait(barrier, 2 * (n - 1) + 1)

    tok_far = copy_to(tok.at[t], tok.at[t], s_tok.at[0], r_tok.at[0], s, far)
    tok_near = copy_to(tok.at[t], tok.at[t], s_tok.at[1], r_tok.at[1], s, near)
    tok_fwd = copy_to(tok.at[far], tok.at[far], s_tok.at[2], r_tok.at[2], s, near)
    z_slot = xt.at[jnp.where(is_hub, 1, 0), core]
    z_recv = r_z.at[jnp.where(is_hub, 1, 0)]
    z_own = copy_to(tok.at[t], z_slot, s_z, z_recv, hub_over, t)
    z_far = copy_to(tok.at[far], z_slot, s_z, z_recv, hub_over, t)
    own_first = side != upper
    tok_far.start()

    @pl.when(own_first)
    def _():
        z_own.start()

    tok_near.start()
    weights = (wcv, wco, wci)
    order = (2, 0, 1)
    chunk = wcv.shape[0] // 4
    chunks = [(m, c) for m in order for c in range(2)]

    def chunk_rows(half, c):
        return pl.ds(pl.multiple_of((2 * half + c) * chunk, chunk), chunk)

    w_sends, y_sends = [], []
    for k, (m, c) in enumerate(chunks):
        w_sends.append(
            copy_to(
                weights[m].at[chunk_rows(g, c)],
                wx.at[m, chunk_rows(g, c)],
                s_w.at[k],
                r_w.at[k],
                mate,
                t,
            )
        )
        block = wx.at[m, chunk_rows(g, c)]
        y_sends.append(copy_to(block, block, s_y.at[k], r_y.at[k], s, t, grp=1 - g))

    def relay(k):
        w_sends[k].wait_recv()
        y_sends[k].start()

    for load in loads[5:8]:
        load.wait()
    for copy in w_sends[:3]:
        copy.start()
    for load in loads[1:5] + loads[8:]:
        load.wait()
    copy_to(tok.at[far], tok.at[far], s_tok.at[0], r_tok.at[0], s, far).wait_recv()
    tok_fwd.start()

    @pl.when(jnp.logical_not(own_first))
    def _():
        z_far.start()

    for copy in w_sends[3:]:
        copy.start()
    copy_to(tok.at[near], tok.at[near], s_tok.at[1], r_tok.at[1], s, near).wait_recv()
    copy_to(tok.at[diag], tok.at[diag], s_tok.at[2], r_tok.at[2], s, near).wait_recv()

    squares = jnp.zeros((rows, 1), f32)
    q_sum = jnp.zeros((rows, wq.shape[2]), f32)
    kv_sum = jnp.zeros((rows, wkv.shape[0]), f32)
    r_sum = jnp.zeros((rows, wr.shape[0]), f32)
    for j in range(n):
        piece = tok[j].astype(f32)
        squares = squares + jnp.sum(piece * piece, axis=1, keepdims=True)
        scaled = (piece * gain[j * width : (j + 1) * width][None, :].astype(f32)).astype(bf16)
        kv_sum = kv_sum + dot_t(scaled, wkv[:, j * width : (j + 1) * width])
        r_sum = r_sum + dot_t(scaled, wr[:, j * width : (j + 1) * width])
        q_sum = q_sum + dot(scaled, wq[j])
    row_scale = lax.rsqrt(squares / (n * width) + EPS)
    kw = wkv.shape[0]
    place = (
        lax.broadcasted_iota(jnp.int32, (kw, 2 * kw), 1)
        == lax.broadcasted_iota(jnp.int32, (kw, 2 * kw), 0) + kw * core
    )
    place = jnp.where(place, 1.0, 0.0).astype(bf16)
    kvp[t] = dot((row_scale * kv_sum).astype(bf16), place).astype(bf16)
    kv_sends = [
        copy_to(kvp.at[t], kvp.at[t], s_kv.at[i], r_kv.at[i], s, p) for i, p in enumerate(tp_peers)
    ]
    for copy in (kv_sends[1], kv_sends[2], kv_sends[0]):
        copy.start()
    qp[t] = (row_scale * q_sum).astype(bf16)
    q_sends = [
        copy_to(qp.at[t], qp.at[t], s_q.at[i], r_q.at[i], s, p) for i, p in enumerate(tp_peers)
    ]
    for copy in (q_sends[1], q_sends[2], q_sends[0]):
        copy.start()

    def scaled_slice(block, f):
        gain_f = gain[pl.ds(pl.multiple_of(f * width, width), width)][None, :].astype(f32)
        return (block.astype(f32) * gain_f).astype(bf16)

    mine_scaled = scaled_slice(tok[s], s)
    for m in order:
        own[m] = dot(mine_scaled, weights[m][...])
    for k in range(3):
        relay(k)

    p_sends = []
    for i in range(2):
        for m in range(3):
            target = hub_over if i else end_over
            p_sends.append(
                copy_to(part.at[i, m], got.at[m], s_p.at[i, m], r_p.at[m], target, t)
            )
    x_sends = []
    for i in range(2):
        slot = xt.at[i, core]
        x_sends.append(copy_to(slot, slot, s_xf.at[i], r_xf.at[i], s, near))

    def conv_block(j):
        m = order[j]
        for k in (2 * j, 2 * j + 1):
            y_sends[k].wait_recv()

        @pl.when(is_hub)
        def _():
            first = jnp.concatenate([xt[i, lax.rem(s, 2)] for i in range(2)], axis=0)
            second = jnp.concatenate([xt[i, lax.rem(mate, 2)] for i in range(2)], axis=0)
            total = dot(scaled_slice(first, s), weights[m][...]) + dot(
                scaled_slice(second, mate), wx[m]
            )
            for i in range(2):
                part[i, m] = total[i * rows : (i + 1) * rows].astype(bf16)
                p_sends[3 * i + m].start()

        own[m] = own[m] + dot(scaled_slice(tok[mate], mate), wx[m])

    cos_v, sin_v = cosine[...], sine[...]
    lanes = cos_v.shape[1]
    turn_r = lax.broadcasted_iota(jnp.int32, (lanes, lanes), 0)
    turn_c = lax.broadcasted_iota(jnp.int32, (lanes, lanes), 1)
    half = ROPE // 2
    low = lax.rem(turn_c, ROPE) < half
    turn = jnp.where(
        low & (turn_r == turn_c + half), -1.0, jnp.where((~low) & (turn_r == turn_c - half), 1.0, 0.0)
    ).astype(bf16)
    spread_r = lax.broadcasted_iota(jnp.int32, (ROPE, lanes), 0)
    spread_c = lax.broadcasted_iota(jnp.int32, (ROPE, lanes), 1)
    spread = jnp.where(lax.rem(spread_c, ROPE) == spread_r, 1.0, 0.0).astype(bf16)
    rope_raw = dot((row_scale * r_sum).astype(bf16), spread).astype(bf16)
    k_rope = (rope_raw.astype(f32) * cos_v + dot(rope_raw, turn) * sin_v).astype(bf16)
    for i, p in enumerate(tp_peers):
        copy_to(kvp.at[p], kvp.at[p], s_kv.at[i], r_kv.at[i], s, p).wait_recv()
    kv_float = jnp.concatenate(
        [kvp[j].astype(f32) + kvp[j + 1].astype(f32) for j in range(0, n, 2)], axis=1
    )
    kv_scale = lax.rsqrt(jnp.mean(kv_float * kv_float, axis=1, keepdims=True) + EPS)
    lat = kv_float.shape[1]
    kvr[s, :, :lat] = (kv_float * kv_scale * kvg[...][None, :].astype(f32)).astype(bf16)
    kvr[s, :, lat:] = k_rope
    def quarter(index):
        return pl.ds(pl.multiple_of(index * (rows // n), rows // n), rows // n)

    mine = quarter(t)
    kz_sends = []
    for k in (2, 1, 3):
        z = lax.rem(s + k, n)
        copy = copy_to(
            kvr.at[s, mine], kvr.at[s, mine], s_kz.at[k - 1], r_kz.at[k - 1], z, t
        )
        copy.start()
        kz_sends.append(copy)

    for k in range(3, 6):
        relay(k)

    @pl.when(is_hub)
    def _():
        for i in range(2):
            slot = xt.at[i, core]
            copy_to(slot, slot, s_z, r_z.at[i], s, near).wait_recv()
            x_sends[i].start()
        for copy in x_sends:
            copy.wait_recv()

    conv_block(0)

    for i, p in enumerate(tp_peers):
        copy_to(qp.at[p], qp.at[p], s_q.at[i], r_q.at[i], s, p).wait_recv()
    q_float = [qp[j].astype(f32) for j in range(n)]
    qw = q_float[0].shape[1]
    q_square = sum(jnp.sum(q * q, axis=1, keepdims=True) for q in q_float)
    q_scale = lax.rsqrt(q_square / (n * qw) + EPS)
    q_normed = jnp.concatenate(
        [(q * q_scale * qg[j * qw : (j + 1) * qw][None, :].astype(f32)).astype(bf16) for j, q in enumerate(q_float)], axis=1
    )
    q_nope = dot(q_normed, wqn[...]).astype(bf16)
    q_raw = dot(q_normed, wqr[...])
    w_turned = dot(wqr[...], turn).astype(bf16)
    q_rope = (q_raw * cos_v + dot(q_normed, w_turned) * sin_v).astype(bf16)

    kf_sends = []
    for k in (2, 1, 3):
        z = lax.rem(s + n - k, n)
        copy_to(
            kvr.at[z, mine], kvr.at[z, mine], s_kz.at[k - 1], r_kz.at[k - 1], z, t
        ).wait_recv()
        for i, p in enumerate(tp_peers):
            copy = copy_to(
                kvr.at[z, mine], kvr.at[z, mine], s_kf.at[k - 1, i], r_kf.at[k - 1, i], s, p
            )
            copy.start()
            kf_sends.append(copy)
    conv_block(1)
    conv_block(2)
    for k in (2, 1, 3):
        z = lax.rem(s + n - k, n)
        for i, p in enumerate(tp_peers):
            rest = kvr.at[z, quarter(p)]
            copy_to(rest, rest, s_kf.at[k - 1, i], r_kf.at[k - 1, i], s, p).wait_recv()

    latent = jnp.concatenate([kvr[j, :, :lat] for j in range(n)], axis=0)
    ropes = jnp.concatenate([kvr[j, :, lat:] for j in range(n)], axis=0)
    keys = dot(latent, wkn[...]).astype(bf16)
    values = dot(latent, wva[...]).astype(bf16)
    heads = wqn.shape[1] // NOPE
    factor = (NOPE + ROPE) ** (-0.5)
    pair = 2 * NOPE
    lane = lax.broadcasted_iota(jnp.int32, (rows, pair), 1)
    lane_r = lax.broadcasted_iota(jnp.int32, (rows, lanes), 1)
    pieces = []
    for p in range(heads // 2):
        cut = slice(p * pair, (p + 1) * pair)
        key_pair = jnp.concatenate([keys[:, cut], ropes], axis=1)
        value_pair = values[:, cut]
        outs = []
        for i in range(2):
            h = 2 * p + i
            in_head = (lane >= i * NOPE) & (lane < (i + 1) * NOPE)
            in_rope = (lane_r >= h * ROPE) & (lane_r < (h + 1) * ROPE)
            query = jnp.concatenate(
                [
                    jnp.where(in_head, q_nope[:, cut].astype(f32), 0.0).astype(bf16),
                    jnp.where(in_rope, q_rope.astype(f32), 0.0).astype(bf16),
                ],
                axis=1,
            )
            scores = dot_t(query, key_pair) * factor
            peak = jnp.max(scores, axis=1, keepdims=True)
            weights = jnp.exp(scores - peak)
            total = jnp.sum(weights, axis=1, keepdims=True)
            outs.append(dot(weights.astype(bf16), value_pair) / total)
        pieces.append(jnp.where(lane < NOPE, outs[0], outs[1]).astype(bf16))
    y_attn = jnp.concatenate(pieces, axis=1)
    for j in range(n):
        acc[j] = dot(y_attn, woa[j])

    def take(m):
        copy_to(part.at[0, m], got.at[m], s_p.at[0, m], r_p.at[m], s, near).wait_recv()
        own[m] = own[m] + got[m].astype(f32)

    take(2)
    take(0)

    def summed(i):
        return (row_scale * own[i]).astype(bf16).astype(f32)

    gated = (summed(2) * summed(0)).astype(bf16)
    gate[...] = gated
    edge = before.shape[0]
    up = copy_to(gate.at[pl.ds(rows - edge, edge)], before, s_h.at[0], r_h.at[0], s + 1, t)
    down = copy_to(gate.at[pl.ds(0, edge)], after, s_h.at[1], r_h.at[1], s - 1, t)

    @pl.when(s < n - 1)
    def _():
        up.start()

    @pl.when(s > 0)
    def _():
        down.start()

    take(1)
    conv_outer = summed(1)
    middle = gated.astype(f32)
    kernel = [taps[i : i + 1, :].astype(f32) for i in range(3)]
    row = lax.broadcasted_iota(jnp.int32, middle.shape, 0)
    previous = pltpu.roll(middle, 1, 0)
    following = pltpu.roll(middle, rows - 1, 0)

    @pl.when(s > 0)
    def _():
        up.wait_recv()

    @pl.when(s == 0)
    def _():
        before[...] = jnp.zeros_like(before)

    @pl.when(s < n - 1)
    def _():
        down.wait_recv()

    @pl.when(s == n - 1)
    def _():
        after[...] = jnp.zeros_like(after)

    first = before[...].astype(f32)[edge - 1 : edge, :]
    last = after[...].astype(f32)[0:1, :]
    previous = jnp.where(row == 0, first, previous)
    following = jnp.where(row == rows - 1, last, following)
    conv_out = previous * kernel[0] + middle * kernel[1] + following * kernel[2]
    y_conv = (conv_outer * conv_out).astype(bf16)

    def share(j):
        return acc[j] + dot(y_conv, woc[j])

    put_near[0] = share(diag).astype(bf16)
    o_diag = copy_to(put_near.at[0], got_near.at[0], s_o.at[0], r_o.at[0], s, near)
    o_diag.start()
    far_share = share(far).astype(bf16).astype(f32)
    o_diag.wait_recv()
    put_far[...] = (far_share + got_near[0].astype(f32)).astype(bf16)
    o_far = copy_to(put_far, got_far, s_o.at[1], r_o.at[1], s, far)
    o_far.start()
    put_near[1] = share(near).astype(bf16)
    o_near = copy_to(put_near.at[1], got_near.at[1], s_o.at[2], r_o.at[2], s, near)
    o_near.start()
    my_share = share(t).astype(bf16).astype(f32)
    o_near.wait_recv()
    my_share = my_share + got_near[1].astype(f32)

    tok_far.wait_send()
    tok_near.wait_send()
    tok_fwd.wait_send()

    z_own.wait_send()
    for copy in kv_sends + q_sends + kz_sends + kf_sends + w_sends + y_sends:
        copy.wait_send()

    @pl.when(is_hub)
    def _():
        for copy in p_sends + x_sends:
            copy.wait_send()

    @pl.when(s < n - 1)
    def _():
        up.wait_send()

    @pl.when(s > 0)
    def _():
        down.wait_send()

    o_diag.wait_send()
    o_near.wait_send()
    o_far.wait()
    out_ref[...] = (my_share + got_far[...].astype(f32)).astype(bf16)


def fits(grp, sp, tp, tokens, mix_gain, w_conv_value, *others):
    rows, width = tokens.shape
    if grp != 2 or sp != 4 or tp != 4 or rows * sp > width * tp:
        return False
    return width % 128 == 0 and rows % 64 == 0 and w_conv_value.shape[0] % 64 == 0


def fused(
    sp,
    tp,
    tokens,
    mix_gain,
    w_conv_value,
    w_conv_outer,
    w_conv_inner,
    conv_kernel,
    w_q_down,
    w_kv_down,
    w_rope_key,
    q_gain,
    kv_gain,
    w_q_nope,
    w_q_rope,
    w_k_nope,
    w_value,
    w_out_conv,
    w_out_attn,
):
    f32, bf16 = jnp.float32, jnp.bfloat16
    n = tp
    rows, width = tokens.shape
    heads = w_q_nope.shape[1] // NOPE
    inverse = np.float32(THETA) ** (-np.arange(0, ROPE, 2, dtype=np.float32) / np.float32(ROPE))
    phase = np.arange(sp * rows, dtype=np.float32)[:, None] * inverse[None, :].astype(np.float32)
    phase = np.tile(phase, (1, 2 * heads)).reshape(sp, rows, heads * ROPE)
    cosine, sine = np.cos(phase).astype(np.float32), np.sin(phase).astype(np.float32)
    operands = (
        tokens,
        mix_gain,
        w_conv_value,
        w_conv_outer,
        w_conv_inner,
        conv_kernel,
        w_q_down.reshape(n, width, -1),
        w_kv_down.T,
        w_rope_key.T,
        q_gain,
        kv_gain,
        w_q_nope,
        w_q_rope,
        w_k_nope,
        w_value,
        w_out_conv,
        w_out_attn,
        jnp.asarray(cosine),
        jnp.asarray(sine),
    )
    vm = pltpu.VMEM
    cw = w_conv_value.shape[1]
    lat = kv_gain.shape[0]
    lanes = heads * ROPE
    scratch = [vm((n, rows, width), bf16)]
    scratch += [vm(x.shape, x.dtype) for x in operands[1:15]]
    scratch += [vm((n, w_out_conv.shape[0], width), bf16)] * 2
    scratch += [vm((rows, lanes), f32)] * 2
    scratch += [
        vm((3,) + w_conv_value.shape, bf16),
        vm((2, 2, rows, width), bf16),
        vm((2, 3, rows, cw), bf16),
        vm((3, rows, cw), bf16),
        vm((3, rows, cw), f32),
        vm((n, rows, w_q_down.shape[1]), bf16),
        vm((n, rows, 2 * w_kv_down.shape[1]), bf16),
        vm((n, rows, lat + lanes), bf16),
        vm((rows, cw), bf16),
        vm((16, cw), bf16),
        vm((16, cw), bf16),
        vm((n, rows, width), f32),
        vm((2, rows, width), bf16),
        vm((2, rows, width), bf16),
        vm((rows, width), bf16),
        vm((rows, width), bf16),
    ]
    dma = pltpu.SemaphoreType.DMA
    scratch += [dma((17 + 2 * n,)), dma((3,)), dma((3,)), dma, dma((2,))]
    scratch += [dma((2,))] * 2
    scratch += [dma((6,))] * 4
    scratch += [dma((n - 1,))] * 6
    scratch += [dma((n - 1, n - 1))] * 2
    scratch += [dma((2, 3)), dma((3,))]
    scratch += [dma((2,)), dma((2,)), dma((3,)), dma((3,))]
    return pl.pallas_call(
        functools.partial(mixer_kernel, n),
        out_shape=jax.ShapeDtypeStruct((rows, width), bf16),
        in_specs=[pl.BlockSpec(memory_space=pl.ANY)] * len(operands),
        out_specs=pl.BlockSpec(memory_space=pltpu.VMEM),
        scratch_shapes=scratch,
        compiler_params=pltpu.CompilerParams(collective_id=0, has_side_effects=True),
    )(*operands)


def solution(mesh):
    placed = (
        P(("grp", "sp"), "tp"),
        P(),
        P("sp", "tp"),
        P("sp", "tp"),
        P("sp", "tp"),
        P(None, "tp"),
        P(None, "tp"),
        P(None, "tp"),
        P(),
        P(),
        P(),
        P(None, "tp"),
        P(None, "tp"),
        P(None, "tp"),
        P(None, "tp"),
        P("tp", None),
        P("tp", None),
    )
    grp, sp, tp = mesh.shape["grp"], mesh.shape["sp"], mesh.shape["tp"]

    def per_device(*args):
        if fits(grp, sp, tp, *args):
            return fused(sp, tp, *args)
        return gathered_weights(*args)

    return jax.shard_map(
        per_device, mesh=mesh, in_specs=placed, out_specs=P(("grp", "sp"), "tp"), check_vma=False
    )
```

```python
import functools

import jax
import jax.numpy as jnp
import numpy as np
from jax import lax
from jax.experimental import pallas as pl
from jax.experimental.pallas import tpu as pltpu
from jax.sharding import PartitionSpec as P

MESH = pl.DeviceIdType.MESH

D = 2048
NOPE = 64
ROPE = 32
VALUE = 64


EPS = 1e-06
THETA = 10000.0


def with_halo(x, sides, width):
    for axis, dim in sides:
        size, length = (lax.axis_size(axis), x.shape[dim])
        up = [(i, (i + 1) % size) for i in range(size - 1)]
        down = [(j, i) for i, j in up]
        last = lax.slice_in_dim(x, length - width, length, axis=dim)
        first = lax.slice_in_dim(x, 0, width, axis=dim)
        before = lax.ppermute(last, axis, up)
        after = lax.ppermute(first, axis, down)
        x = jnp.concatenate([before, x, after], axis=dim)
    return x


def rms_scale(values):
    return lax.rsqrt(jnp.mean(values * values, axis=-1, keepdims=True) + EPS)


def angles(positions, width):
    inverse = THETA ** (-jnp.arange(0, width, 2, dtype=jnp.float32) / width)
    phase = positions[:, None] * inverse[None, :]
    phase = jnp.concatenate([phase, phase], axis=-1)
    return (jnp.cos(phase), jnp.sin(phase))


def turned(values, cosine, sine):
    half = values.shape[-1] // 2
    first = values[..., :half]
    second = values[..., half:]
    return values * cosine + jnp.concatenate([-second, first], axis=-1) * sine


def block_rows(count):
    for candidate in range(min(count, 1024), 0, -1):
        if count % candidate == 0 and candidate % 128 == 0:
            return candidate
    for candidate in range(min(count, 1024), 0, -1):
        if count % candidate == 0:
            return candidate
    return count


def gathered_weights(
    tokens,
    mix_gain,
    w_conv_value,
    w_conv_outer,
    w_conv_inner,
    conv_kernel,
    w_q_down,
    w_kv_down,
    w_rope_key,
    q_gain,
    kv_gain,
    w_q_nope,
    w_q_rope,
    w_k_nope,
    w_value,
    w_out_conv,
    w_out_attn,
):
    f32 = jnp.float32
    bf16 = jnp.bfloat16
    rows = tokens.shape[0]
    conv_value_w, conv_outer_w, conv_inner_w = (
        lax.all_gather(w_conv_value, "sp", axis=0, tiled=True),
        lax.all_gather(w_conv_outer, "sp", axis=0, tiled=True),
        lax.all_gather(w_conv_inner, "sp", axis=0, tiled=True),
    )
    matrices = (conv_value_w, conv_outer_w, conv_inner_w, w_q_down, w_kv_down, w_rope_key)
    gain = mix_gain.astype(f32)
    piece_f = lax.all_gather(tokens, "tp", axis=1, tiled=True).astype(f32)
    scaled = (piece_f * gain).astype(bf16)
    updated = tuple((jnp.dot(scaled, matrix, preferred_element_type=f32) for matrix in matrices))
    squares = jnp.sum(piece_f * piece_f, axis=1)
    row_scale = lax.rsqrt(squares / D + EPS)[:, None]
    conv_value, conv_outer, conv_inner, q_part, kv_part, rope_raw = [
        (row_scale * total).astype(bf16) for total in updated
    ]
    gated = (conv_inner.astype(f32) * conv_value.astype(f32)).astype(bf16)
    padded = with_halo(gated, (("sp", 0),), 1).astype(f32)
    kernel = conv_kernel.astype(f32)
    conv_out = padded[:-2] * kernel[0] + padded[1:-1] * kernel[1] + padded[2:] * kernel[2]
    y_conv = (conv_outer.astype(f32) * conv_out).astype(bf16)
    q_latent, kv_latent = (
        lax.all_gather(q_part, "tp", axis=1, tiled=True),
        lax.all_gather(kv_part, "tp", axis=1, tiled=True),
    )
    q_float = q_latent.astype(f32)
    q_normed = (q_float * rms_scale(q_float) * q_gain.astype(f32)).astype(bf16)
    kv_float = kv_latent.astype(f32)
    kv_normed = (kv_float * rms_scale(kv_float) * kv_gain.astype(f32)).astype(bf16)
    heads = w_q_nope.shape[1] // NOPE
    positions = (lax.axis_index("sp") * rows + jnp.arange(rows, dtype=jnp.int32)).astype(f32)
    cosine, sine = angles(positions, ROPE)
    q_nope = (
        jnp.dot(q_normed, w_q_nope, preferred_element_type=f32)
        .astype(bf16)
        .reshape(rows, heads, NOPE)
    )
    q_rope_raw = jnp.dot(q_normed, w_q_rope, preferred_element_type=f32).reshape(rows, heads, ROPE)
    q_rope = turned(q_rope_raw, cosine[:, None, :], sine[:, None, :]).astype(bf16)
    k_rope = turned(rope_raw.astype(f32), cosine, sine).astype(bf16)
    factor = (NOPE + ROPE) ** (-0.5)

    def attend(state, key_block, value_block, rope_block):
        peak, total, summed = state
        count = key_block.shape[0]
        keys3 = key_block.reshape(count, heads, NOPE)
        values3 = value_block.reshape(count, heads, VALUE)
        scores = jnp.einsum("qhd,khd->qhk", q_nope, keys3, preferred_element_type=f32)
        scores = scores + jnp.einsum("qhr,kr->qhk", q_rope, rope_block, preferred_element_type=f32)
        scores = scores * factor
        new_peak = jnp.maximum(peak, jnp.max(scores, axis=-1))
        fade = jnp.exp(peak - new_peak)
        weights = jnp.exp(scores - new_peak[..., None])
        total = total * fade + jnp.sum(weights, axis=-1)
        summed = summed * fade[..., None] + jnp.einsum(
            "qhk,khd->qhd", weights.astype(bf16), values3, preferred_element_type=f32
        )
        return (new_peak, total, summed)

    start_state = (
        jnp.full((rows, heads), -jnp.inf, f32),
        jnp.zeros((rows, heads), f32),
        jnp.zeros((rows, heads, VALUE), f32),
    )
    latent = lax.all_gather(kv_normed, "sp", axis=0, tiled=True)
    rope_keys = lax.all_gather(k_rope, "sp", axis=0, tiled=True)
    size = block_rows(latent.shape[0])
    count = latent.shape[0] // size

    def one_block(carry, blocks):
        latent_block, rope_block = blocks
        key_block = jnp.dot(latent_block, w_k_nope, preferred_element_type=f32).astype(bf16)
        value_block = jnp.dot(latent_block, w_value, preferred_element_type=f32).astype(bf16)
        return (attend(carry, key_block, value_block, rope_block), None)

    carry, ignored = lax.scan(
        one_block,
        start_state,
        (
            latent.reshape(count, size, latent.shape[1]),
            rope_keys.reshape(count, size, rope_keys.shape[1]),
        ),
    )
    peak, total, summed = carry
    y_attn = (summed / total[..., None]).astype(bf16).reshape(rows, heads * VALUE)
    partial_sum = jnp.dot(y_conv, w_out_conv, preferred_element_type=f32) + jnp.dot(
        y_attn, w_out_attn, preferred_element_type=f32
    )
    return (
        lax.psum_scatter(partial_sum.astype(jnp.bfloat16), "tp", scatter_dimension=1, tiled=True)
        .astype(jnp.float32)
        .astype(bf16)
    )


def copy_to(src, dst, send, recv, sp, tp, **group):
    return pltpu.make_async_remote_copy(
        src_ref=src,
        dst_ref=dst,
        send_sem=send,
        recv_sem=recv,
        device_id={"sp": sp, "tp": tp, **group},
        device_id_type=MESH,
    )


def dot(a, b):
    return jnp.dot(a, b, preferred_element_type=jnp.float32)


def dot_t(a, b):
    return lax.dot_general(a, b, (((1,), (1,)), ((), ())), preferred_element_type=jnp.float32)


def mixer_kernel(
    n,
    tokens_h,
    gain_h,
    wcv_h,
    wco_h,
    wci_h,
    taps_h,
    wq_h,
    wkv_h,
    wr_h,
    qg_h,
    kvg_h,
    wqn_h,
    wqr_h,
    wkn_h,
    wva_h,
    woc_h,
    woa_h,
    cos_h,
    sin_h,
    out_ref,
    tok,
    gain,
    wcv,
    wco,
    wci,
    taps,
    wq,
    wkv,
    wr,
    qg,
    kvg,
    wqn,
    wqr,
    wkn,
    wva,
    woc,
    woa,
    cosine,
    sine,
    wx,
    xt,
    part,
    got,
    own,
    qp,
    kvp,
    kvr,
    gate,
    before,
    after,
    acc,
    put_near,
    got_near,
    put_far,
    got_far,
    load_sem,
    s_tok,
    r_tok,
    s_z,
    r_z,
    s_xf,
    r_xf,
    s_w,
    r_w,
    s_y,
    r_y,
    s_q,
    r_q,
    s_kv,
    r_kv,
    s_kz,
    r_kz,
    s_kf,
    r_kf,
    s_p,
    r_p,
    s_h,
    r_h,
    s_o,
    r_o,
):
    f32, bf16 = jnp.float32, jnp.bfloat16
    g, s, t = lax.axis_index("grp"), lax.axis_index("sp"), lax.axis_index("tp")
    core = lax.rem(t, 2)
    near = t + 1 - 2 * core
    far = lax.rem(t + 2, n)
    diag = lax.rem(near + 2, n)
    rows, width = tok.shape[1], tok.shape[2]
    cw = wcv.shape[1]
    tp_peers = (near, far, diag)
    upper = lax.div(s, n // 2)
    side = lax.div(t, 2)
    is_hub = (s == 1) | (s == n - 2)
    mate = s + 1 - 2 * lax.rem(s, 2)
    hub_over = n // 2 - upper
    end_over = (n - 1) * (1 - upper)

    loads = [
        (tokens_h, tok.at[t]),
        (gain_h, gain),
        (wq_h, wq),
        (wkv_h, wkv),
        (wr_h, wr),
        (wcv_h, wcv),
        (wco_h, wco),
        (wci_h, wci),
        (taps_h, taps),
        (qg_h, qg),
        (kvg_h, kvg),
        (wqn_h, wqn),
        (wqr_h, wqr),
        (wkn_h, wkn),
        (wva_h, wva),
        (cos_h.at[s], cosine),
        (sin_h.at[s], sine),
    ]
    for j in range(n):
        columns = pl.ds(j * width, width)
        loads.append((woa_h.at[:, columns], woa.at[j]))
        loads.append((woc_h.at[:, columns], woc.at[j]))
    loads = [pltpu.make_async_copy(a, b, load_sem.at[i]) for i, (a, b) in enumerate(loads)]
    for load in loads:
        load.start()

    barrier = pltpu.get_barrier_semaphore()
    for peer in tp_peers:
        pl.semaphore_signal(barrier, inc=1, device_id={"sp": s, "tp": peer}, device_id_type=MESH)
    for k in range(1, n):
        pl.semaphore_signal(
            barrier, inc=1, device_id={"sp": lax.rem(s + k, n), "tp": t}, device_id_type=MESH
        )
    pl.semaphore_signal(
        barrier, inc=1, device_id={"grp": 1 - g, "sp": s, "tp": t}, device_id_type=MESH
    )
    loads[0].wait()
    pl.semaphore_wait(barrier, 2 * (n - 1) + 1)

    tok_far = copy_to(tok.at[t], tok.at[t], s_tok.at[0], r_tok.at[0], s, far)
    tok_near = copy_to(tok.at[t], tok.at[t], s_tok.at[1], r_tok.at[1], s, near)
    tok_fwd = copy_to(tok.at[far], tok.at[far], s_tok.at[2], r_tok.at[2], s, near)
    z_slot = xt.at[jnp.where(is_hub, 1, 0), core]
    z_recv = r_z.at[jnp.where(is_hub, 1, 0)]
    z_own = copy_to(tok.at[t], z_slot, s_z, z_recv, hub_over, t)
    z_far = copy_to(tok.at[far], z_slot, s_z, z_recv, hub_over, t)
    own_first = side != upper
    tok_far.start()
    tok_near.start()
    weights = (wcv, wco, wci)
    order = (2, 0, 1)
    pieces_per = 4
    chunk = wcv.shape[0] // (2 * pieces_per)
    chunks = [(m, c) for m in order for c in range(pieces_per)]

    def chunk_rows(half, c):
        return pl.ds(pl.multiple_of((pieces_per * half + c) * chunk, chunk), chunk)

    w_sends, y_sends = [], []
    for k, (m, c) in enumerate(chunks):
        w_sends.append(
            copy_to(
                weights[m].at[chunk_rows(g, c)],
                wx.at[m, chunk_rows(g, c)],
                s_w.at[k],
                r_w.at[k],
                mate,
                t,
            )
        )
        block = wx.at[m, chunk_rows(g, c)]
        y_sends.append(copy_to(block, block, s_y.at[k], r_y.at[k], s, t, grp=1 - g))

    def relay(k):
        w_sends[k].wait_recv()
        y_sends[k].start()

    for load in loads[5:8]:
        load.wait()
    for copy in w_sends[:4]:
        copy.start()

    @pl.when(own_first)
    def _():
        z_own.start()

    for copy in w_sends[4:6]:
        copy.start()
    for load in loads[1:5] + loads[8:]:
        load.wait()
    copy_to(tok.at[far], tok.at[far], s_tok.at[0], r_tok.at[0], s, far).wait_recv()
    tok_fwd.start()

    @pl.when(jnp.logical_not(own_first))
    def _():
        z_far.start()

    for copy in w_sends[6:]:
        copy.start()
    copy_to(tok.at[near], tok.at[near], s_tok.at[1], r_tok.at[1], s, near).wait_recv()
    copy_to(tok.at[diag], tok.at[diag], s_tok.at[2], r_tok.at[2], s, near).wait_recv()

    squares = jnp.zeros((rows, 1), f32)
    q_sum = jnp.zeros((rows, wq.shape[2]), f32)
    kv_sum = jnp.zeros((rows, wkv.shape[0]), f32)
    r_sum = jnp.zeros((rows, wr.shape[0]), f32)
    for j in range(n):
        piece = tok[j].astype(f32)
        squares = squares + jnp.sum(piece * piece, axis=1, keepdims=True)
        scaled = (piece * gain[j * width : (j + 1) * width][None, :].astype(f32)).astype(bf16)
        kv_sum = kv_sum + dot_t(scaled, wkv[:, j * width : (j + 1) * width])
        r_sum = r_sum + dot_t(scaled, wr[:, j * width : (j + 1) * width])
        q_sum = q_sum + dot(scaled, wq[j])
    row_scale = lax.rsqrt(squares / (n * width) + EPS)
    kw = wkv.shape[0]
    place = (
        lax.broadcasted_iota(jnp.int32, (kw, 2 * kw), 1)
        == lax.broadcasted_iota(jnp.int32, (kw, 2 * kw), 0) + kw * core
    )
    place = jnp.where(place, 1.0, 0.0).astype(bf16)
    kvp[t] = dot((row_scale * kv_sum).astype(bf16), place).astype(bf16)
    kv_sends = [
        copy_to(kvp.at[t], kvp.at[t], s_kv.at[i], r_kv.at[i], s, p) for i, p in enumerate(tp_peers)
    ]
    for copy in (kv_sends[1], kv_sends[2], kv_sends[0]):
        copy.start()
    qp[t] = (row_scale * q_sum).astype(bf16)
    q_sends = [
        copy_to(qp.at[t], qp.at[t], s_q.at[i], r_q.at[i], s, p) for i, p in enumerate(tp_peers)
    ]
    for copy in (q_sends[1], q_sends[2], q_sends[0]):
        copy.start()

    def scaled_slice(block, f):
        gain_f = gain[pl.ds(pl.multiple_of(f * width, width), width)][None, :].astype(f32)
        return (block.astype(f32) * gain_f).astype(bf16)

    mine_scaled = scaled_slice(tok[s], s)
    for m in order:
        own[m] = dot(mine_scaled, weights[m][...])
    for k in range(4):
        relay(k)

    p_sends = []
    for i in range(2):
        for m in range(3):
            target = hub_over if i else end_over
            p_sends.append(
                copy_to(part.at[i, m], got.at[m], s_p.at[i, m], r_p.at[m], target, t)
            )
    x_sends = []
    for i in range(2):
        slot = xt.at[i, core]
        x_sends.append(copy_to(slot, slot, s_xf.at[i], r_xf.at[i], s, near))

    def conv_block(j):
        m = order[j]
        for k in range(pieces_per * j, pieces_per * (j + 1)):
            y_sends[k].wait_recv()

        @pl.when(is_hub)
        def _():
            first = jnp.concatenate([xt[i, lax.rem(s, 2)] for i in range(2)], axis=0)
            second = jnp.concatenate([xt[i, lax.rem(mate, 2)] for i in range(2)], axis=0)
            total = dot(scaled_slice(first, s), weights[m][...]) + dot(
                scaled_slice(second, mate), wx[m]
            )
            for i in range(2):
                part[i, m] = total[i * rows : (i + 1) * rows].astype(bf16)
                p_sends[3 * i + m].start()

        own[m] = own[m] + dot(scaled_slice(tok[mate], mate), wx[m])

    cos_v, sin_v = cosine[...], sine[...]
    lanes = cos_v.shape[1]
    turn_r = lax.broadcasted_iota(jnp.int32, (lanes, lanes), 0)
    turn_c = lax.broadcasted_iota(jnp.int32, (lanes, lanes), 1)
    half = ROPE // 2
    low = lax.rem(turn_c, ROPE) < half
    turn = jnp.where(
        low & (turn_r == turn_c + half), -1.0, jnp.where((~low) & (turn_r == turn_c - half), 1.0, 0.0)
    ).astype(bf16)
    spread_r = lax.broadcasted_iota(jnp.int32, (ROPE, lanes), 0)
    spread_c = lax.broadcasted_iota(jnp.int32, (ROPE, lanes), 1)
    spread = jnp.where(lax.rem(spread_c, ROPE) == spread_r, 1.0, 0.0).astype(bf16)
    rope_raw = dot((row_scale * r_sum).astype(bf16), spread).astype(bf16)
    k_rope = (rope_raw.astype(f32) * cos_v + dot(rope_raw, turn) * sin_v).astype(bf16)
    for i, p in enumerate(tp_peers):
        copy_to(kvp.at[p], kvp.at[p], s_kv.at[i], r_kv.at[i], s, p).wait_recv()
    kv_float = jnp.concatenate(
        [kvp[j].astype(f32) + kvp[j + 1].astype(f32) for j in range(0, n, 2)], axis=1
    )
    kv_scale = lax.rsqrt(jnp.mean(kv_float * kv_float, axis=1, keepdims=True) + EPS)
    lat = kv_float.shape[1]
    kvr[s, :, :lat] = (kv_float * kv_scale * kvg[...][None, :].astype(f32)).astype(bf16)
    kvr[s, :, lat:] = k_rope
    def quarter(index):
        return pl.ds(pl.multiple_of(index * (rows // n), rows // n), rows // n)

    mine = quarter(t)
    kz_sends = []
    for k in (2, 1, 3):
        z = lax.rem(s + k, n)
        copy = copy_to(
            kvr.at[s, mine], kvr.at[s, mine], s_kz.at[k - 1], r_kz.at[k - 1], z, t
        )
        copy.start()
        kz_sends.append(copy)

    for k in range(4, 7):
        relay(k)

    @pl.when(is_hub)
    def _():
        for i in range(2):
            slot = xt.at[i, core]
            copy_to(slot, slot, s_z, r_z.at[i], s, near).wait_recv()
            x_sends[i].start()
        for copy in x_sends:
            copy.wait_recv()

    conv_block(0)
    for k in range(7, 10):
        relay(k)

    for i, p in enumerate(tp_peers):
        copy_to(qp.at[p], qp.at[p], s_q.at[i], r_q.at[i], s, p).wait_recv()
    q_float = [qp[j].astype(f32) for j in range(n)]
    qw = q_float[0].shape[1]
    q_square = sum(jnp.sum(q * q, axis=1, keepdims=True) for q in q_float)
    q_scale = lax.rsqrt(q_square / (n * qw) + EPS)
    q_normed = jnp.concatenate(
        [(q * q_scale * qg[j * qw : (j + 1) * qw][None, :].astype(f32)).astype(bf16) for j, q in enumerate(q_float)], axis=1
    )
    q_nope = dot(q_normed, wqn[...]).astype(bf16)
    q_raw = dot(q_normed, wqr[...])
    w_turned = dot(wqr[...], turn).astype(bf16)
    q_rope = (q_raw * cos_v + dot(q_normed, w_turned) * sin_v).astype(bf16)

    for k in range(10, 12):
        relay(k)
    kf_sends = []
    for k in (2, 1, 3):
        z = lax.rem(s + n - k, n)
        copy_to(
            kvr.at[z, mine], kvr.at[z, mine], s_kz.at[k - 1], r_kz.at[k - 1], z, t
        ).wait_recv()
        for i, p in enumerate(tp_peers):
            copy = copy_to(
                kvr.at[z, mine], kvr.at[z, mine], s_kf.at[k - 1, i], r_kf.at[k - 1, i], s, p
            )
            copy.start()
            kf_sends.append(copy)
    conv_block(1)
    conv_block(2)
    for k in (2, 1, 3):
        z = lax.rem(s + n - k, n)
        for i, p in enumerate(tp_peers):
            rest = kvr.at[z, quarter(p)]
            copy_to(rest, rest, s_kf.at[k - 1, i], r_kf.at[k - 1, i], s, p).wait_recv()

    latent = jnp.concatenate([kvr[j, :, :lat] for j in range(n)], axis=0)
    ropes = jnp.concatenate([kvr[j, :, lat:] for j in range(n)], axis=0)
    keys = dot(latent, wkn[...]).astype(bf16)
    values = dot(latent, wva[...]).astype(bf16)
    heads = wqn.shape[1] // NOPE
    factor = (NOPE + ROPE) ** (-0.5)
    pair = 2 * NOPE
    lane = lax.broadcasted_iota(jnp.int32, (rows, pair), 1)
    lane_r = lax.broadcasted_iota(jnp.int32, (rows, lanes), 1)
    pieces = []
    for p in range(heads // 2):
        cut = slice(p * pair, (p + 1) * pair)
        key_pair = jnp.concatenate([keys[:, cut], ropes], axis=1)
        value_pair = values[:, cut]
        outs = []
        for i in range(2):
            h = 2 * p + i
            in_head = (lane >= i * NOPE) & (lane < (i + 1) * NOPE)
            in_rope = (lane_r >= h * ROPE) & (lane_r < (h + 1) * ROPE)
            query = jnp.concatenate(
                [
                    jnp.where(in_head, q_nope[:, cut].astype(f32), 0.0).astype(bf16),
                    jnp.where(in_rope, q_rope.astype(f32), 0.0).astype(bf16),
                ],
                axis=1,
            )
            scores = dot_t(query, key_pair) * factor
            peak = jnp.max(scores, axis=1, keepdims=True)
            weights = jnp.exp(scores - peak)
            total = jnp.sum(weights, axis=1, keepdims=True)
            outs.append(dot(weights.astype(bf16), value_pair) / total)
        pieces.append(jnp.where(lane < NOPE, outs[0], outs[1]).astype(bf16))
    y_attn = jnp.concatenate(pieces, axis=1)
    for j in range(n):
        acc[j] = dot(y_attn, woa[j])

    def take(m):
        copy_to(part.at[0, m], got.at[m], s_p.at[0, m], r_p.at[m], s, near).wait_recv()
        own[m] = own[m] + got[m].astype(f32)

    take(2)
    take(0)

    def summed(i):
        return (row_scale * own[i]).astype(bf16).astype(f32)

    gated = (summed(2) * summed(0)).astype(bf16)
    gate[...] = gated
    edge = before.shape[0]
    up = copy_to(gate.at[pl.ds(rows - edge, edge)], before, s_h.at[0], r_h.at[0], s + 1, t)
    down = copy_to(gate.at[pl.ds(0, edge)], after, s_h.at[1], r_h.at[1], s - 1, t)

    @pl.when(s < n - 1)
    def _():
        up.start()

    @pl.when(s > 0)
    def _():
        down.start()

    take(1)
    conv_outer = summed(1)
    middle = gated.astype(f32)
    kernel = [taps[i : i + 1, :].astype(f32) for i in range(3)]
    row = lax.broadcasted_iota(jnp.int32, middle.shape, 0)
    previous = pltpu.roll(middle, 1, 0)
    following = pltpu.roll(middle, rows - 1, 0)

    @pl.when(s > 0)
    def _():
        up.wait_recv()

    @pl.when(s == 0)
    def _():
        before[...] = jnp.zeros_like(before)

    @pl.when(s < n - 1)
    def _():
        down.wait_recv()

    @pl.when(s == n - 1)
    def _():
        after[...] = jnp.zeros_like(after)

    first = before[...].astype(f32)[edge - 1 : edge, :]
    last = after[...].astype(f32)[0:1, :]
    previous = jnp.where(row == 0, first, previous)
    following = jnp.where(row == rows - 1, last, following)
    conv_out = previous * kernel[0] + middle * kernel[1] + following * kernel[2]
    y_conv = (conv_outer * conv_out).astype(bf16)

    def share(j):
        return acc[j] + dot(y_conv, woc[j])

    put_near[0] = share(diag).astype(bf16)
    o_diag = copy_to(put_near.at[0], got_near.at[0], s_o.at[0], r_o.at[0], s, near)
    o_diag.start()
    far_share = share(far).astype(bf16).astype(f32)
    o_diag.wait_recv()
    put_far[...] = (far_share + got_near[0].astype(f32)).astype(bf16)
    o_far = copy_to(put_far, got_far, s_o.at[1], r_o.at[1], s, far)
    o_far.start()
    put_near[1] = share(near).astype(bf16)
    o_near = copy_to(put_near.at[1], got_near.at[1], s_o.at[2], r_o.at[2], s, near)
    o_near.start()
    my_share = share(t).astype(bf16).astype(f32)
    o_near.wait_recv()
    my_share = my_share + got_near[1].astype(f32)

    tok_far.wait_send()
    tok_near.wait_send()
    tok_fwd.wait_send()

    z_own.wait_send()
    for copy in kv_sends + q_sends + kz_sends + kf_sends + w_sends + y_sends:
        copy.wait_send()

    @pl.when(is_hub)
    def _():
        for copy in p_sends + x_sends:
            copy.wait_send()

    @pl.when(s < n - 1)
    def _():
        up.wait_send()

    @pl.when(s > 0)
    def _():
        down.wait_send()

    o_diag.wait_send()
    o_near.wait_send()
    o_far.wait()
    out_ref[...] = (my_share + got_far[...].astype(f32)).astype(bf16)


def fits(grp, sp, tp, tokens, mix_gain, w_conv_value, *others):
    rows, width = tokens.shape
    if grp != 2 or sp != 4 or tp != 4 or rows * sp > width * tp:
        return False
    return width % 128 == 0 and rows % 64 == 0 and w_conv_value.shape[0] % 64 == 0


def fused(
    sp,
    tp,
    tokens,
    mix_gain,
    w_conv_value,
    w_conv_outer,
    w_conv_inner,
    conv_kernel,
    w_q_down,
    w_kv_down,
    w_rope_key,
    q_gain,
    kv_gain,
    w_q_nope,
    w_q_rope,
    w_k_nope,
    w_value,
    w_out_conv,
    w_out_attn,
):
    f32, bf16 = jnp.float32, jnp.bfloat16
    n = tp
    rows, width = tokens.shape
    heads = w_q_nope.shape[1] // NOPE
    inverse = np.float32(THETA) ** (-np.arange(0, ROPE, 2, dtype=np.float32) / np.float32(ROPE))
    phase = np.arange(sp * rows, dtype=np.float32)[:, None] * inverse[None, :].astype(np.float32)
    phase = np.tile(phase, (1, 2 * heads)).reshape(sp, rows, heads * ROPE)
    cosine, sine = np.cos(phase).astype(np.float32), np.sin(phase).astype(np.float32)
    operands = (
        tokens,
        mix_gain,
        w_conv_value,
        w_conv_outer,
        w_conv_inner,
        conv_kernel,
        w_q_down.reshape(n, width, -1),
        w_kv_down.T,
        w_rope_key.T,
        q_gain,
        kv_gain,
        w_q_nope,
        w_q_rope,
        w_k_nope,
        w_value,
        w_out_conv,
        w_out_attn,
        jnp.asarray(cosine),
        jnp.asarray(sine),
    )
    vm = pltpu.VMEM
    cw = w_conv_value.shape[1]
    lat = kv_gain.shape[0]
    lanes = heads * ROPE
    scratch = [vm((n, rows, width), bf16)]
    scratch += [vm(x.shape, x.dtype) for x in operands[1:15]]
    scratch += [vm((n, w_out_conv.shape[0], width), bf16)] * 2
    scratch += [vm((rows, lanes), f32)] * 2
    scratch += [
        vm((3,) + w_conv_value.shape, bf16),
        vm((2, 2, rows, width), bf16),
        vm((2, 3, rows, cw), bf16),
        vm((3, rows, cw), bf16),
        vm((3, rows, cw), f32),
        vm((n, rows, w_q_down.shape[1]), bf16),
        vm((n, rows, 2 * w_kv_down.shape[1]), bf16),
        vm((n, rows, lat + lanes), bf16),
        vm((rows, cw), bf16),
        vm((16, cw), bf16),
        vm((16, cw), bf16),
        vm((n, rows, width), f32),
        vm((2, rows, width), bf16),
        vm((2, rows, width), bf16),
        vm((rows, width), bf16),
        vm((rows, width), bf16),
    ]
    dma = pltpu.SemaphoreType.DMA
    scratch += [dma((17 + 2 * n,)), dma((3,)), dma((3,)), dma, dma((2,))]
    scratch += [dma((2,))] * 2
    scratch += [dma((12,))] * 4
    scratch += [dma((n - 1,))] * 6
    scratch += [dma((n - 1, n - 1))] * 2
    scratch += [dma((2, 3)), dma((3,))]
    scratch += [dma((2,)), dma((2,)), dma((3,)), dma((3,))]
    return pl.pallas_call(
        functools.partial(mixer_kernel, n),
        out_shape=pltpu.VMEM((rows, width), bf16),
        in_specs=[pl.BlockSpec(memory_space=pl.ANY)] * len(operands),
        out_specs=pl.BlockSpec(memory_space=pltpu.VMEM),
        scratch_shapes=scratch,
        compiler_params=pltpu.CompilerParams(collective_id=0, has_side_effects=True),
    )(*operands)


def solution(mesh):
    placed = (
        P(("grp", "sp"), "tp"),
        P(),
        P("sp", "tp"),
        P("sp", "tp"),
        P("sp", "tp"),
        P(None, "tp"),
        P(None, "tp"),
        P(None, "tp"),
        P(),
        P(),
        P(),
        P(None, "tp"),
        P(None, "tp"),
        P(None, "tp"),
        P(None, "tp"),
        P("tp", None),
        P("tp", None),
    )
    grp, sp, tp = mesh.shape["grp"], mesh.shape["sp"], mesh.shape["tp"]

    def per_device(*args):
        if fits(grp, sp, tp, *args):
            return fused(sp, tp, *args)
        return gathered_weights(*args)

    return jax.shard_map(
        per_device, mesh=mesh, in_specs=placed, out_specs=P(("grp", "sp"), "tp"), check_vma=False
    )
```

```python
import functools

import jax
import jax.numpy as jnp
import numpy as np
from jax import lax
from jax.experimental import pallas as pl
from jax.experimental.pallas import tpu as pltpu
from jax.sharding import PartitionSpec as P

MESH = pl.DeviceIdType.MESH

D = 2048
NOPE = 64
ROPE = 32
VALUE = 64


EPS = 1e-06
THETA = 10000.0


def with_halo(x, sides, width):
    for axis, dim in sides:
        size, length = (lax.axis_size(axis), x.shape[dim])
        up = [(i, (i + 1) % size) for i in range(size - 1)]
        down = [(j, i) for i, j in up]
        last = lax.slice_in_dim(x, length - width, length, axis=dim)
        first = lax.slice_in_dim(x, 0, width, axis=dim)
        before = lax.ppermute(last, axis, up)
        after = lax.ppermute(first, axis, down)
        x = jnp.concatenate([before, x, after], axis=dim)
    return x


def rms_scale(values):
    return lax.rsqrt(jnp.mean(values * values, axis=-1, keepdims=True) + EPS)


def angles(positions, width):
    inverse = THETA ** (-jnp.arange(0, width, 2, dtype=jnp.float32) / width)
    phase = positions[:, None] * inverse[None, :]
    phase = jnp.concatenate([phase, phase], axis=-1)
    return (jnp.cos(phase), jnp.sin(phase))


def turned(values, cosine, sine):
    half = values.shape[-1] // 2
    first = values[..., :half]
    second = values[..., half:]
    return values * cosine + jnp.concatenate([-second, first], axis=-1) * sine


def block_rows(count):
    for candidate in range(min(count, 1024), 0, -1):
        if count % candidate == 0 and candidate % 128 == 0:
            return candidate
    for candidate in range(min(count, 1024), 0, -1):
        if count % candidate == 0:
            return candidate
    return count


def gathered_weights(
    tokens,
    mix_gain,
    w_conv_value,
    w_conv_outer,
    w_conv_inner,
    conv_kernel,
    w_q_down,
    w_kv_down,
    w_rope_key,
    q_gain,
    kv_gain,
    w_q_nope,
    w_q_rope,
    w_k_nope,
    w_value,
    w_out_conv,
    w_out_attn,
):
    f32 = jnp.float32
    bf16 = jnp.bfloat16
    rows = tokens.shape[0]
    conv_value_w, conv_outer_w, conv_inner_w = (
        lax.all_gather(w_conv_value, "sp", axis=0, tiled=True),
        lax.all_gather(w_conv_outer, "sp", axis=0, tiled=True),
        lax.all_gather(w_conv_inner, "sp", axis=0, tiled=True),
    )
    matrices = (conv_value_w, conv_outer_w, conv_inner_w, w_q_down, w_kv_down, w_rope_key)
    gain = mix_gain.astype(f32)
    piece_f = lax.all_gather(tokens, "tp", axis=1, tiled=True).astype(f32)
    scaled = (piece_f * gain).astype(bf16)
    updated = tuple((jnp.dot(scaled, matrix, preferred_element_type=f32) for matrix in matrices))
    squares = jnp.sum(piece_f * piece_f, axis=1)
    row_scale = lax.rsqrt(squares / D + EPS)[:, None]
    conv_value, conv_outer, conv_inner, q_part, kv_part, rope_raw = [
        (row_scale * total).astype(bf16) for total in updated
    ]
    gated = (conv_inner.astype(f32) * conv_value.astype(f32)).astype(bf16)
    padded = with_halo(gated, (("sp", 0),), 1).astype(f32)
    kernel = conv_kernel.astype(f32)
    conv_out = padded[:-2] * kernel[0] + padded[1:-1] * kernel[1] + padded[2:] * kernel[2]
    y_conv = (conv_outer.astype(f32) * conv_out).astype(bf16)
    q_latent, kv_latent = (
        lax.all_gather(q_part, "tp", axis=1, tiled=True),
        lax.all_gather(kv_part, "tp", axis=1, tiled=True),
    )
    q_float = q_latent.astype(f32)
    q_normed = (q_float * rms_scale(q_float) * q_gain.astype(f32)).astype(bf16)
    kv_float = kv_latent.astype(f32)
    kv_normed = (kv_float * rms_scale(kv_float) * kv_gain.astype(f32)).astype(bf16)
    heads = w_q_nope.shape[1] // NOPE
    positions = (lax.axis_index("sp") * rows + jnp.arange(rows, dtype=jnp.int32)).astype(f32)
    cosine, sine = angles(positions, ROPE)
    q_nope = (
        jnp.dot(q_normed, w_q_nope, preferred_element_type=f32)
        .astype(bf16)
        .reshape(rows, heads, NOPE)
    )
    q_rope_raw = jnp.dot(q_normed, w_q_rope, preferred_element_type=f32).reshape(rows, heads, ROPE)
    q_rope = turned(q_rope_raw, cosine[:, None, :], sine[:, None, :]).astype(bf16)
    k_rope = turned(rope_raw.astype(f32), cosine, sine).astype(bf16)
    factor = (NOPE + ROPE) ** (-0.5)

    def attend(state, key_block, value_block, rope_block):
        peak, total, summed = state
        count = key_block.shape[0]
        keys3 = key_block.reshape(count, heads, NOPE)
        values3 = value_block.reshape(count, heads, VALUE)
        scores = jnp.einsum("qhd,khd->qhk", q_nope, keys3, preferred_element_type=f32)
        scores = scores + jnp.einsum("qhr,kr->qhk", q_rope, rope_block, preferred_element_type=f32)
        scores = scores * factor
        new_peak = jnp.maximum(peak, jnp.max(scores, axis=-1))
        fade = jnp.exp(peak - new_peak)
        weights = jnp.exp(scores - new_peak[..., None])
        total = total * fade + jnp.sum(weights, axis=-1)
        summed = summed * fade[..., None] + jnp.einsum(
            "qhk,khd->qhd", weights.astype(bf16), values3, preferred_element_type=f32
        )
        return (new_peak, total, summed)

    start_state = (
        jnp.full((rows, heads), -jnp.inf, f32),
        jnp.zeros((rows, heads), f32),
        jnp.zeros((rows, heads, VALUE), f32),
    )
    latent = lax.all_gather(kv_normed, "sp", axis=0, tiled=True)
    rope_keys = lax.all_gather(k_rope, "sp", axis=0, tiled=True)
    size = block_rows(latent.shape[0])
    count = latent.shape[0] // size

    def one_block(carry, blocks):
        latent_block, rope_block = blocks
        key_block = jnp.dot(latent_block, w_k_nope, preferred_element_type=f32).astype(bf16)
        value_block = jnp.dot(latent_block, w_value, preferred_element_type=f32).astype(bf16)
        return (attend(carry, key_block, value_block, rope_block), None)

    carry, ignored = lax.scan(
        one_block,
        start_state,
        (
            latent.reshape(count, size, latent.shape[1]),
            rope_keys.reshape(count, size, rope_keys.shape[1]),
        ),
    )
    peak, total, summed = carry
    y_attn = (summed / total[..., None]).astype(bf16).reshape(rows, heads * VALUE)
    partial_sum = jnp.dot(y_conv, w_out_conv, preferred_element_type=f32) + jnp.dot(
        y_attn, w_out_attn, preferred_element_type=f32
    )
    return (
        lax.psum_scatter(partial_sum.astype(jnp.bfloat16), "tp", scatter_dimension=1, tiled=True)
        .astype(jnp.float32)
        .astype(bf16)
    )


def copy_to(src, dst, send, recv, sp, tp, **group):
    return pltpu.make_async_remote_copy(
        src_ref=src,
        dst_ref=dst,
        send_sem=send,
        recv_sem=recv,
        device_id={"sp": sp, "tp": tp, **group},
        device_id_type=MESH,
    )


def dot(a, b):
    return jnp.dot(a, b, preferred_element_type=jnp.float32)


def dot_t(a, b):
    return lax.dot_general(a, b, (((1,), (1,)), ((), ())), preferred_element_type=jnp.float32)


def mixer_kernel(
    n,
    tokens_h,
    gain_h,
    wcv_h,
    wco_h,
    wci_h,
    taps_h,
    wq_h,
    wkv_h,
    wr_h,
    qg_h,
    kvg_h,
    wqn_h,
    wqr_h,
    wkn_h,
    wva_h,
    woc_h,
    woa_h,
    cos_h,
    sin_h,
    out_ref,
    tok,
    gain,
    wcv,
    wco,
    wci,
    taps,
    wq,
    wkv,
    wr,
    qg,
    kvg,
    wqn,
    wqr,
    wkn,
    wva,
    woc,
    woa,
    cosine,
    sine,
    wx,
    xt,
    part,
    got,
    own,
    qp,
    kvp,
    kvr,
    gate,
    before,
    after,
    acc,
    put_near,
    got_near,
    put_far,
    got_far,
    load_sem,
    sent,
    r_tok,
    r_z,
    r_xf,
    r_w,
    r_y,
    r_q,
    r_kv,
    r_kz,
    r_kf,
    r_p,
    r_h,
    r_o,
):
    f32, bf16 = jnp.float32, jnp.bfloat16
    g, s, t = lax.axis_index("grp"), lax.axis_index("sp"), lax.axis_index("tp")
    core = lax.rem(t, 2)
    near = t + 1 - 2 * core
    far = lax.rem(t + 2, n)
    diag = lax.rem(near + 2, n)
    rows, width = tok.shape[1], tok.shape[2]
    cw = wcv.shape[1]
    tp_peers = (near, far, diag)
    upper = lax.div(s, n // 2)
    side = lax.div(t, 2)
    is_hub = (s == 1) | (s == n - 2)
    mate = s + 1 - 2 * lax.rem(s, 2)
    hub_over = n // 2 - upper
    end_over = (n - 1) * (1 - upper)

    loads = [
        (tokens_h, tok.at[t]),
        (gain_h, gain),
        (wq_h, wq),
        (wkv_h, wkv),
        (wr_h, wr),
        (wcv_h, wcv),
        (wco_h, wco),
        (wci_h, wci),
        (taps_h, taps),
        (qg_h, qg),
        (kvg_h, kvg),
        (wqn_h, wqn),
        (wqr_h, wqr),
        (wkn_h, wkn),
        (wva_h, wva),
        (cos_h.at[s], cosine),
        (sin_h.at[s], sine),
    ]
    for j in range(n):
        columns = pl.ds(j * width, width)
        loads.append((woa_h.at[:, columns], woa.at[j]))
        loads.append((woc_h.at[:, columns], woc.at[j]))
    groups = [0] + [2] * 4 + [1] * 3 + [3] * (len(loads) - 8)
    loads = [pltpu.make_async_copy(a, b, load_sem.at[i]) for (a, b), i in zip(loads, groups)]
    for load in loads:
        load.start()

    barrier = pltpu.get_barrier_semaphore()
    for peer in tp_peers:
        pl.semaphore_signal(barrier, inc=1, device_id={"sp": s, "tp": peer}, device_id_type=MESH)
    for k in range(1, n):
        pl.semaphore_signal(
            barrier, inc=1, device_id={"sp": lax.rem(s + k, n), "tp": t}, device_id_type=MESH
        )
    pl.semaphore_signal(
        barrier, inc=1, device_id={"grp": 1 - g, "sp": s, "tp": t}, device_id_type=MESH
    )
    loads[0].wait()
    pl.semaphore_wait(barrier, 2 * (n - 1) + 1)

    tok_far = copy_to(tok.at[t], tok.at[t], sent, r_tok.at[0], s, far)
    tok_near = copy_to(tok.at[t], tok.at[t], sent, r_tok.at[1], s, near)
    tok_fwd = copy_to(tok.at[far], tok.at[far], sent, r_tok.at[2], s, near)
    z_slot = xt.at[jnp.where(is_hub, 1, 0), core]
    z_recv = r_z.at[jnp.where(is_hub, 1, 0)]
    z_own = copy_to(tok.at[t], z_slot, sent, z_recv, hub_over, t)
    z_far = copy_to(tok.at[far], z_slot, sent, z_recv, hub_over, t)
    own_first = side != upper
    tok_far.start()
    tok_near.start()
    weights = (wcv, wco, wci)
    order = (2, 0, 1)
    pieces_per = 4
    chunk = wcv.shape[0] // (2 * pieces_per)
    chunks = [(m, c) for m in order for c in range(pieces_per)]

    def chunk_rows(half, c):
        return pl.ds(pl.multiple_of((pieces_per * half + c) * chunk, chunk), chunk)

    w_sends, y_sends = [], []
    for k, (m, c) in enumerate(chunks):
        w_sends.append(
            copy_to(
                weights[m].at[chunk_rows(g, c)],
                wx.at[m, chunk_rows(g, c)],
                sent,
                r_w.at[k],
                mate,
                t,
            )
        )
        block = wx.at[m, chunk_rows(g, c)]
        y_sends.append(copy_to(block, block, sent, r_y.at[m], s, t, grp=1 - g))

    def arrived(ref, sem):
        copy_to(ref, ref, sent, sem, s, near).wait_recv()

    def relay(k):
        w_sends[k].wait_recv()
        y_sends[k].start()

    for load in loads[5:8]:
        load.wait()
    for copy in w_sends[:4]:
        copy.start()

    @pl.when(own_first)
    def _():
        z_own.start()

    for copy in w_sends[4:6]:
        copy.start()
    for load in loads[1:5] + loads[8:]:
        load.wait()
    copy_to(tok.at[far], tok.at[far], sent, r_tok.at[0], s, far).wait_recv()
    tok_fwd.start()

    @pl.when(jnp.logical_not(own_first))
    def _():
        z_far.start()

    for copy in w_sends[6:]:
        copy.start()
    copy_to(tok.at[near], tok.at[near], sent, r_tok.at[1], s, near).wait_recv()
    copy_to(tok.at[diag], tok.at[diag], sent, r_tok.at[2], s, near).wait_recv()

    squares = jnp.zeros((rows, 1), f32)
    q_sum = jnp.zeros((rows, wq.shape[2]), f32)
    kv_sum = jnp.zeros((rows, wkv.shape[0]), f32)
    r_sum = jnp.zeros((rows, wr.shape[0]), f32)
    for j in range(n):
        piece = tok[j].astype(f32)
        squares = squares + jnp.sum(piece * piece, axis=1, keepdims=True)
        scaled = (piece * gain[j * width : (j + 1) * width][None, :].astype(f32)).astype(bf16)
        kv_sum = kv_sum + dot_t(scaled, wkv[:, j * width : (j + 1) * width])
        r_sum = r_sum + dot_t(scaled, wr[:, j * width : (j + 1) * width])
        q_sum = q_sum + dot(scaled, wq[j])
    row_scale = lax.rsqrt(squares / (n * width) + EPS)
    kw = wkv.shape[0]
    place = (
        lax.broadcasted_iota(jnp.int32, (kw, 2 * kw), 1)
        == lax.broadcasted_iota(jnp.int32, (kw, 2 * kw), 0) + kw * core
    )
    place = jnp.where(place, 1.0, 0.0).astype(bf16)
    kvp[t] = dot((row_scale * kv_sum).astype(bf16), place).astype(bf16)
    kv_sends = [
        copy_to(kvp.at[t], kvp.at[t], sent, r_kv, s, p) for i, p in enumerate(tp_peers)
    ]
    for copy in (kv_sends[1], kv_sends[2], kv_sends[0]):
        copy.start()
    qp[t] = (row_scale * q_sum).astype(bf16)
    q_sends = [
        copy_to(qp.at[t], qp.at[t], sent, r_q, s, p) for i, p in enumerate(tp_peers)
    ]
    for copy in (q_sends[1], q_sends[2], q_sends[0]):
        copy.start()

    def scaled_slice(block, f):
        gain_f = gain[pl.ds(pl.multiple_of(f * width, width), width)][None, :].astype(f32)
        return (block.astype(f32) * gain_f).astype(bf16)

    mine_scaled = scaled_slice(tok[s], s)
    for m in order:
        own[m] = dot(mine_scaled, weights[m][...])
    for k in range(4):
        relay(k)

    edge = before.shape[0]
    up = copy_to(gate.at[pl.ds(rows - edge, edge)], before, sent, r_h.at[0], s + 1, t)
    down = copy_to(gate.at[pl.ds(0, edge)], after, sent, r_h.at[1], s - 1, t)

    def take(m):
        arrived(got.at[m], r_p.at[m])
        own[m] = own[m] + got[m].astype(f32)

    def summed(i):
        return (row_scale * own[i]).astype(bf16).astype(f32)

    def gate_part():
        take(2)
        take(0)
        gate[...] = (summed(2) * summed(0)).astype(bf16)

        @pl.when(s < n - 1)
        def _():
            up.start()

        @pl.when(s > 0)
        def _():
            down.start()

    p_sends = []
    for i in range(2):
        for m in range(3):
            target = hub_over if i else end_over
            p_sends.append(
                copy_to(part.at[i, m], got.at[m], sent, r_p.at[m], target, t)
            )
    x_sends = []
    for i in range(2):
        slot = xt.at[i, core]
        x_sends.append(copy_to(slot, slot, sent, r_xf, s, near))

    def conv_block(j):
        m = order[j]
        arrived(wx.at[m, pl.ds(0, wx.shape[1] // 2)], r_y.at[m])

        @pl.when(is_hub)
        def _():
            first = jnp.concatenate([xt[i, lax.rem(s, 2)] for i in range(2)], axis=0)
            second = jnp.concatenate([xt[i, lax.rem(mate, 2)] for i in range(2)], axis=0)
            total = dot(scaled_slice(first, s), weights[m][...]) + dot(
                scaled_slice(second, mate), wx[m]
            )
            for i in range(2):
                part[i, m] = total[i * rows : (i + 1) * rows].astype(bf16)
                p_sends[3 * i + m].start()

        own[m] = own[m] + dot(scaled_slice(tok[mate], mate), wx[m])

    cos_v, sin_v = cosine[...], sine[...]
    lanes = cos_v.shape[1]
    turn_r = lax.broadcasted_iota(jnp.int32, (lanes, lanes), 0)
    turn_c = lax.broadcasted_iota(jnp.int32, (lanes, lanes), 1)
    half = ROPE // 2
    low = lax.rem(turn_c, ROPE) < half
    turn = jnp.where(
        low & (turn_r == turn_c + half), -1.0, jnp.where((~low) & (turn_r == turn_c - half), 1.0, 0.0)
    ).astype(bf16)
    spread_r = lax.broadcasted_iota(jnp.int32, (ROPE, lanes), 0)
    spread_c = lax.broadcasted_iota(jnp.int32, (ROPE, lanes), 1)
    spread = jnp.where(lax.rem(spread_c, ROPE) == spread_r, 1.0, 0.0).astype(bf16)
    rope_raw = dot((row_scale * r_sum).astype(bf16), spread).astype(bf16)
    k_rope = (rope_raw.astype(f32) * cos_v + dot(rope_raw, turn) * sin_v).astype(bf16)
    arrived(kvp.at[pl.ds(0, n - 1)], r_kv)
    kv_float = jnp.concatenate(
        [kvp[j].astype(f32) + kvp[j + 1].astype(f32) for j in range(0, n, 2)], axis=1
    )
    kv_scale = lax.rsqrt(jnp.mean(kv_float * kv_float, axis=1, keepdims=True) + EPS)
    lat = kv_float.shape[1]
    kvr[s, :, :lat] = (kv_float * kv_scale * kvg[...][None, :].astype(f32)).astype(bf16)
    kvr[s, :, lat:] = k_rope
    def quarter(index):
        return pl.ds(pl.multiple_of(index * (rows // n), rows // n), rows // n)

    mine = quarter(t)
    kz_sends = []
    for k in (2, 1, 3):
        z = lax.rem(s + k, n)
        copy = copy_to(
            kvr.at[s, mine], kvr.at[s, mine], sent, r_kz.at[k - 1], z, t
        )
        copy.start()
        kz_sends.append(copy)

    for k in range(4, 7):
        relay(k)

    @pl.when(is_hub)
    def _():
        for i in range(2):
            slot = xt.at[i, core]
            copy_to(slot, slot, sent, r_z.at[i], s, near).wait_recv()
            x_sends[i].start()
        arrived(xt.at[:, core], r_xf)

    conv_block(0)
    for k in range(7, 10):
        relay(k)

    arrived(qp.at[pl.ds(0, n - 1)], r_q)
    q_float = [qp[j].astype(f32) for j in range(n)]
    qw = q_float[0].shape[1]
    q_square = sum(jnp.sum(q * q, axis=1, keepdims=True) for q in q_float)
    q_scale = lax.rsqrt(q_square / (n * qw) + EPS)
    q_normed = jnp.concatenate(
        [(q * q_scale * qg[j * qw : (j + 1) * qw][None, :].astype(f32)).astype(bf16) for j, q in enumerate(q_float)], axis=1
    )
    q_nope = dot(q_normed, wqn[...]).astype(bf16)
    q_raw = dot(q_normed, wqr[...])
    w_turned = dot(wqr[...], turn).astype(bf16)
    q_rope = (q_raw * cos_v + dot(q_normed, w_turned) * sin_v).astype(bf16)

    for k in range(10, 12):
        relay(k)
    kf_sends = []
    for k in (2, 1, 3):
        z = lax.rem(s + n - k, n)
        copy_to(
            kvr.at[z, mine], kvr.at[z, mine], sent, r_kz.at[k - 1], z, t
        ).wait_recv()
        for i, p in enumerate(tp_peers):
            copy = copy_to(
                kvr.at[z, mine], kvr.at[z, mine], sent, r_kf, s, p
            )
            copy.start()
            kf_sends.append(copy)
    conv_block(1)
    conv_block(2)
    arrived(kvr.at[pl.ds(0, n - 1), pl.ds(0, (n - 1) * (rows // n))], r_kf)

    @pl.when(is_hub)
    def _():
        gate_part()

    latent = jnp.concatenate([kvr[j, :, :lat] for j in range(n)], axis=0)
    ropes = jnp.concatenate([kvr[j, :, lat:] for j in range(n)], axis=0)
    keys = dot(latent, wkn[...]).astype(bf16)
    values = dot(latent, wva[...]).astype(bf16)
    heads = wqn.shape[1] // NOPE
    factor = (NOPE + ROPE) ** (-0.5)
    pair = 2 * NOPE
    lane = lax.broadcasted_iota(jnp.int32, (rows, pair), 1)
    lane_r = lax.broadcasted_iota(jnp.int32, (rows, lanes), 1)
    pieces = []
    for p in range(heads // 2):
        cut = slice(p * pair, (p + 1) * pair)
        key_pair = jnp.concatenate([keys[:, cut], ropes], axis=1)
        value_pair = values[:, cut]
        outs = []
        for i in range(2):
            h = 2 * p + i
            in_head = (lane >= i * NOPE) & (lane < (i + 1) * NOPE)
            in_rope = (lane_r >= h * ROPE) & (lane_r < (h + 1) * ROPE)
            query = jnp.concatenate(
                [
                    jnp.where(in_head, q_nope[:, cut].astype(f32), 0.0).astype(bf16),
                    jnp.where(in_rope, q_rope.astype(f32), 0.0).astype(bf16),
                ],
                axis=1,
            )
            scores = dot_t(query, key_pair) * factor
            peak = jnp.max(scores, axis=1, keepdims=True)
            weights = jnp.exp(scores - peak)
            total = jnp.sum(weights, axis=1, keepdims=True)
            outs.append(dot(weights.astype(bf16), value_pair) / total)
        pieces.append(jnp.where(lane < NOPE, outs[0], outs[1]).astype(bf16))
    y_attn = jnp.concatenate(pieces, axis=1)
    for j in range(n):
        acc[j] = dot(y_attn, woa[j])

    @pl.when(jnp.logical_not(is_hub))
    def _():
        gate_part()

    take(1)
    conv_outer = summed(1)
    middle = gate[...].astype(f32)
    kernel = [taps[i : i + 1, :].astype(f32) for i in range(3)]
    row = lax.broadcasted_iota(jnp.int32, middle.shape, 0)
    previous = pltpu.roll(middle, 1, 0)
    following = pltpu.roll(middle, rows - 1, 0)

    @pl.when(s > 0)
    def _():
        up.wait_recv()

    @pl.when(s == 0)
    def _():
        before[...] = jnp.zeros_like(before)

    @pl.when(s < n - 1)
    def _():
        down.wait_recv()

    @pl.when(s == n - 1)
    def _():
        after[...] = jnp.zeros_like(after)

    first = before[...].astype(f32)[edge - 1 : edge, :]
    last = after[...].astype(f32)[0:1, :]
    previous = jnp.where(row == 0, first, previous)
    following = jnp.where(row == rows - 1, last, following)
    conv_out = previous * kernel[0] + middle * kernel[1] + following * kernel[2]
    y_conv = (conv_outer * conv_out).astype(bf16)

    def share(j):
        return acc[j] + dot(y_conv, woc[j])

    put_near[0] = share(diag).astype(bf16)
    o_diag = copy_to(put_near.at[0], got_near.at[0], sent, r_o.at[0], s, near)
    o_diag.start()
    far_share = share(far).astype(bf16).astype(f32)
    o_diag.wait_recv()
    put_far[...] = (far_share + got_near[0].astype(f32)).astype(bf16)
    o_far = copy_to(put_far, got_far, sent, r_o.at[1], s, far)
    o_far.start()
    put_near[1] = share(near).astype(bf16)
    o_near = copy_to(put_near.at[1], got_near.at[1], sent, r_o.at[2], s, near)
    o_near.start()
    my_share = share(t).astype(bf16).astype(f32)
    o_near.wait_recv()
    my_share = my_share + got_near[1].astype(f32)

    tok_far.wait_send()
    tok_near.wait_send()
    tok_fwd.wait_send()

    z_own.wait_send()
    for copy in kv_sends + q_sends + kz_sends + kf_sends + w_sends + y_sends:
        copy.wait_send()

    @pl.when(is_hub)
    def _():
        for copy in p_sends + x_sends:
            copy.wait_send()

    @pl.when(s < n - 1)
    def _():
        up.wait_send()

    @pl.when(s > 0)
    def _():
        down.wait_send()

    o_diag.wait_send()
    o_near.wait_send()
    o_far.wait()
    out_ref[...] = (my_share + got_far[...].astype(f32)).astype(bf16)


def fits(grp, sp, tp, tokens, mix_gain, w_conv_value, *others):
    rows, width = tokens.shape
    if grp != 2 or sp != 4 or tp != 4 or rows * sp > width * tp:
        return False
    return width % 128 == 0 and rows % 64 == 0 and w_conv_value.shape[0] % 64 == 0


def fused(
    sp,
    tp,
    tokens,
    mix_gain,
    w_conv_value,
    w_conv_outer,
    w_conv_inner,
    conv_kernel,
    w_q_down,
    w_kv_down,
    w_rope_key,
    q_gain,
    kv_gain,
    w_q_nope,
    w_q_rope,
    w_k_nope,
    w_value,
    w_out_conv,
    w_out_attn,
):
    f32, bf16 = jnp.float32, jnp.bfloat16
    n = tp
    rows, width = tokens.shape
    heads = w_q_nope.shape[1] // NOPE
    inverse = np.float32(THETA) ** (-np.arange(0, ROPE, 2, dtype=np.float32) / np.float32(ROPE))
    phase = np.arange(sp * rows, dtype=np.float32)[:, None] * inverse[None, :].astype(np.float32)
    phase = np.tile(phase, (1, 2 * heads)).reshape(sp, rows, heads * ROPE)
    cosine, sine = np.cos(phase).astype(np.float32), np.sin(phase).astype(np.float32)
    operands = (
        tokens,
        mix_gain,
        w_conv_value,
        w_conv_outer,
        w_conv_inner,
        conv_kernel,
        w_q_down.reshape(n, width, -1),
        w_kv_down.T,
        w_rope_key.T,
        q_gain,
        kv_gain,
        w_q_nope,
        w_q_rope,
        w_k_nope,
        w_value,
        w_out_conv,
        w_out_attn,
        jnp.asarray(cosine),
        jnp.asarray(sine),
    )
    vm = pltpu.VMEM
    cw = w_conv_value.shape[1]
    lat = kv_gain.shape[0]
    lanes = heads * ROPE
    scratch = [vm((n, rows, width), bf16)]
    scratch += [vm(x.shape, x.dtype) for x in operands[1:15]]
    scratch += [vm((n, w_out_conv.shape[0], width), bf16)] * 2
    scratch += [vm((rows, lanes), f32)] * 2
    scratch += [
        vm((3,) + w_conv_value.shape, bf16),
        vm((2, 2, rows, width), bf16),
        vm((2, 3, rows, cw), bf16),
        vm((3, rows, cw), bf16),
        vm((3, rows, cw), f32),
        vm((n, rows, w_q_down.shape[1]), bf16),
        vm((n, rows, 2 * w_kv_down.shape[1]), bf16),
        vm((n, rows, lat + lanes), bf16),
        vm((rows, cw), bf16),
        vm((16, cw), bf16),
        vm((16, cw), bf16),
        vm((n, rows, width), f32),
        vm((2, rows, width), bf16),
        vm((2, rows, width), bf16),
        vm((rows, width), bf16),
        vm((rows, width), bf16),
    ]
    dma = pltpu.SemaphoreType.DMA
    scratch += [dma((4,)), dma, dma((3,)), dma((2,)), dma, dma((12,)), dma((3,)), dma, dma]
    scratch += [dma((n - 1,)), dma, dma((3,)), dma((2,)), dma((3,))]
    return pl.pallas_call(
        functools.partial(mixer_kernel, n),
        out_shape=pltpu.VMEM((rows, width), bf16),
        in_specs=[pl.BlockSpec(memory_space=pl.ANY)] * len(operands),
        out_specs=pl.BlockSpec(memory_space=pltpu.VMEM),
        scratch_shapes=scratch,
        compiler_params=pltpu.CompilerParams(collective_id=0, has_side_effects=True),
    )(*operands)


def solution(mesh):
    placed = (
        P(("grp", "sp"), "tp"),
        P(),
        P("sp", "tp"),
        P("sp", "tp"),
        P("sp", "tp"),
        P(None, "tp"),
        P(None, "tp"),
        P(None, "tp"),
        P(),
        P(),
        P(),
        P(None, "tp"),
        P(None, "tp"),
        P(None, "tp"),
        P(None, "tp"),
        P("tp", None),
        P("tp", None),
    )
    grp, sp, tp = mesh.shape["grp"], mesh.shape["sp"], mesh.shape["tp"]

    def per_device(*args):
        if fits(grp, sp, tp, *args):
            return fused(sp, tp, *args)
        return gathered_weights(*args)

    return jax.shard_map(
        per_device, mesh=mesh, in_specs=placed, out_specs=P(("grp", "sp"), "tp"), check_vma=False
    )
```

```python
import functools

import jax
import jax.numpy as jnp
import numpy as np
from jax import lax
from jax.experimental import pallas as pl
from jax.experimental.pallas import tpu as pltpu
from jax.sharding import PartitionSpec as P

MESH = pl.DeviceIdType.MESH

D = 2048
NOPE = 64
ROPE = 32
VALUE = 64


EPS = 1e-06
THETA = 10000.0


def with_halo(x, sides, width):
    for axis, dim in sides:
        size, length = (lax.axis_size(axis), x.shape[dim])
        up = [(i, (i + 1) % size) for i in range(size - 1)]
        down = [(j, i) for i, j in up]
        last = lax.slice_in_dim(x, length - width, length, axis=dim)
        first = lax.slice_in_dim(x, 0, width, axis=dim)
        before = lax.ppermute(last, axis, up)
        after = lax.ppermute(first, axis, down)
        x = jnp.concatenate([before, x, after], axis=dim)
    return x


def rms_scale(values):
    return lax.rsqrt(jnp.mean(values * values, axis=-1, keepdims=True) + EPS)


def angles(positions, width):
    inverse = THETA ** (-jnp.arange(0, width, 2, dtype=jnp.float32) / width)
    phase = positions[:, None] * inverse[None, :]
    phase = jnp.concatenate([phase, phase], axis=-1)
    return (jnp.cos(phase), jnp.sin(phase))


def turned(values, cosine, sine):
    half = values.shape[-1] // 2
    first = values[..., :half]
    second = values[..., half:]
    return values * cosine + jnp.concatenate([-second, first], axis=-1) * sine


def block_rows(count):
    for candidate in range(min(count, 1024), 0, -1):
        if count % candidate == 0 and candidate % 128 == 0:
            return candidate
    for candidate in range(min(count, 1024), 0, -1):
        if count % candidate == 0:
            return candidate
    return count


def gathered_weights(
    tokens,
    mix_gain,
    w_conv_value,
    w_conv_outer,
    w_conv_inner,
    conv_kernel,
    w_q_down,
    w_kv_down,
    w_rope_key,
    q_gain,
    kv_gain,
    w_q_nope,
    w_q_rope,
    w_k_nope,
    w_value,
    w_out_conv,
    w_out_attn,
):
    f32 = jnp.float32
    bf16 = jnp.bfloat16
    rows = tokens.shape[0]
    conv_value_w, conv_outer_w, conv_inner_w = (
        lax.all_gather(w_conv_value, "sp", axis=0, tiled=True),
        lax.all_gather(w_conv_outer, "sp", axis=0, tiled=True),
        lax.all_gather(w_conv_inner, "sp", axis=0, tiled=True),
    )
    matrices = (conv_value_w, conv_outer_w, conv_inner_w, w_q_down, w_kv_down, w_rope_key)
    gain = mix_gain.astype(f32)
    piece_f = lax.all_gather(tokens, "tp", axis=1, tiled=True).astype(f32)
    scaled = (piece_f * gain).astype(bf16)
    updated = tuple((jnp.dot(scaled, matrix, preferred_element_type=f32) for matrix in matrices))
    squares = jnp.sum(piece_f * piece_f, axis=1)
    row_scale = lax.rsqrt(squares / D + EPS)[:, None]
    conv_value, conv_outer, conv_inner, q_part, kv_part, rope_raw = [
        (row_scale * total).astype(bf16) for total in updated
    ]
    gated = (conv_inner.astype(f32) * conv_value.astype(f32)).astype(bf16)
    padded = with_halo(gated, (("sp", 0),), 1).astype(f32)
    kernel = conv_kernel.astype(f32)
    conv_out = padded[:-2] * kernel[0] + padded[1:-1] * kernel[1] + padded[2:] * kernel[2]
    y_conv = (conv_outer.astype(f32) * conv_out).astype(bf16)
    q_latent, kv_latent = (
        lax.all_gather(q_part, "tp", axis=1, tiled=True),
        lax.all_gather(kv_part, "tp", axis=1, tiled=True),
    )
    q_float = q_latent.astype(f32)
    q_normed = (q_float * rms_scale(q_float) * q_gain.astype(f32)).astype(bf16)
    kv_float = kv_latent.astype(f32)
    kv_normed = (kv_float * rms_scale(kv_float) * kv_gain.astype(f32)).astype(bf16)
    heads = w_q_nope.shape[1] // NOPE
    positions = (lax.axis_index("sp") * rows + jnp.arange(rows, dtype=jnp.int32)).astype(f32)
    cosine, sine = angles(positions, ROPE)
    q_nope = (
        jnp.dot(q_normed, w_q_nope, preferred_element_type=f32)
        .astype(bf16)
        .reshape(rows, heads, NOPE)
    )
    q_rope_raw = jnp.dot(q_normed, w_q_rope, preferred_element_type=f32).reshape(rows, heads, ROPE)
    q_rope = turned(q_rope_raw, cosine[:, None, :], sine[:, None, :]).astype(bf16)
    k_rope = turned(rope_raw.astype(f32), cosine, sine).astype(bf16)
    factor = (NOPE + ROPE) ** (-0.5)

    def attend(state, key_block, value_block, rope_block):
        peak, total, summed = state
        count = key_block.shape[0]
        keys3 = key_block.reshape(count, heads, NOPE)
        values3 = value_block.reshape(count, heads, VALUE)
        scores = jnp.einsum("qhd,khd->qhk", q_nope, keys3, preferred_element_type=f32)
        scores = scores + jnp.einsum("qhr,kr->qhk", q_rope, rope_block, preferred_element_type=f32)
        scores = scores * factor
        new_peak = jnp.maximum(peak, jnp.max(scores, axis=-1))
        fade = jnp.exp(peak - new_peak)
        weights = jnp.exp(scores - new_peak[..., None])
        total = total * fade + jnp.sum(weights, axis=-1)
        summed = summed * fade[..., None] + jnp.einsum(
            "qhk,khd->qhd", weights.astype(bf16), values3, preferred_element_type=f32
        )
        return (new_peak, total, summed)

    start_state = (
        jnp.full((rows, heads), -jnp.inf, f32),
        jnp.zeros((rows, heads), f32),
        jnp.zeros((rows, heads, VALUE), f32),
    )
    latent = lax.all_gather(kv_normed, "sp", axis=0, tiled=True)
    rope_keys = lax.all_gather(k_rope, "sp", axis=0, tiled=True)
    size = block_rows(latent.shape[0])
    count = latent.shape[0] // size

    def one_block(carry, blocks):
        latent_block, rope_block = blocks
        key_block = jnp.dot(latent_block, w_k_nope, preferred_element_type=f32).astype(bf16)
        value_block = jnp.dot(latent_block, w_value, preferred_element_type=f32).astype(bf16)
        return (attend(carry, key_block, value_block, rope_block), None)

    carry, ignored = lax.scan(
        one_block,
        start_state,
        (
            latent.reshape(count, size, latent.shape[1]),
            rope_keys.reshape(count, size, rope_keys.shape[1]),
        ),
    )
    peak, total, summed = carry
    y_attn = (summed / total[..., None]).astype(bf16).reshape(rows, heads * VALUE)
    partial_sum = jnp.dot(y_conv, w_out_conv, preferred_element_type=f32) + jnp.dot(
        y_attn, w_out_attn, preferred_element_type=f32
    )
    return (
        lax.psum_scatter(partial_sum.astype(jnp.bfloat16), "tp", scatter_dimension=1, tiled=True)
        .astype(jnp.float32)
        .astype(bf16)
    )


def copy_to(src, dst, send, recv, sp, tp, **group):
    return pltpu.make_async_remote_copy(
        src_ref=src,
        dst_ref=dst,
        send_sem=send,
        recv_sem=recv,
        device_id={"sp": sp, "tp": tp, **group},
        device_id_type=MESH,
    )


def dot(a, b):
    return jnp.dot(a, b, preferred_element_type=jnp.float32)


def dot_t(a, b):
    return lax.dot_general(a, b, (((1,), (1,)), ((), ())), preferred_element_type=jnp.float32)


def mixer_kernel(
    n,
    tokens_h,
    gain_h,
    wcv_h,
    wco_h,
    wci_h,
    taps_h,
    wq_h,
    wkv_h,
    wr_h,
    qg_h,
    kvg_h,
    wqn_h,
    wqr_h,
    wkn_h,
    wva_h,
    woc_h,
    woa_h,
    cos_h,
    sin_h,
    out_ref,
    tok,
    gain,
    wcv,
    wco,
    wci,
    taps,
    wq,
    wkv,
    wr,
    qg,
    kvg,
    wqn,
    wqr,
    wkn,
    wva,
    woc,
    woa,
    cosine,
    sine,
    wx,
    xt,
    part,
    got,
    own,
    qp,
    kvp,
    kvr,
    rk,
    gate,
    before,
    after,
    acc,
    put_near,
    got_near,
    put_far,
    got_far,
    load_sem,
    sent,
    r_tok,
    r_z,
    r_xf,
    r_w,
    r_y,
    r_q,
    r_kv,
    r_kz,
    r_kf,
    r_rk,
    r_p,
    r_h,
    r_o,
):
    f32, bf16 = jnp.float32, jnp.bfloat16
    g, s, t = lax.axis_index("grp"), lax.axis_index("sp"), lax.axis_index("tp")
    core = lax.rem(t, 2)
    near = t + 1 - 2 * core
    far = lax.rem(t + 2, n)
    diag = lax.rem(near + 2, n)
    rows, width = tok.shape[1], tok.shape[2]
    cw = wcv.shape[1]
    tp_peers = (near, far, diag)
    upper = lax.div(s, n // 2)
    side = lax.div(t, 2)
    is_hub = (s == 1) | (s == n - 2)
    mate = s + 1 - 2 * lax.rem(s, 2)
    hub_over = n // 2 - upper
    end_over = (n - 1) * (1 - upper)

    loads = [
        (tokens_h, tok.at[t]),
        (gain_h, gain),
        (wq_h, wq),
        (wkv_h, wkv),
        (wr_h, wr),
        (wcv_h, wcv),
        (wco_h, wco),
        (wci_h, wci),
        (taps_h, taps),
        (qg_h, qg),
        (kvg_h, kvg),
        (wqn_h, wqn),
        (wqr_h, wqr),
        (wkn_h, wkn),
        (wva_h, wva),
        (cos_h.at[s], cosine),
        (sin_h.at[s], sine),
    ]
    for j in range(n):
        columns = pl.ds(j * width, width)
        loads.append((woa_h.at[:, columns], woa.at[j]))
        loads.append((woc_h.at[:, columns], woc.at[j]))
    groups = [0] + [2] * 4 + [1] * 3 + [3] * (len(loads) - 8)
    loads = [pltpu.make_async_copy(a, b, load_sem.at[i]) for (a, b), i in zip(loads, groups)]
    for load in loads:
        load.start()

    barrier = pltpu.get_barrier_semaphore()
    for peer in tp_peers:
        pl.semaphore_signal(barrier, inc=1, device_id={"sp": s, "tp": peer}, device_id_type=MESH)
    for k in range(1, n):
        pl.semaphore_signal(
            barrier, inc=1, device_id={"sp": lax.rem(s + k, n), "tp": t}, device_id_type=MESH
        )
    pl.semaphore_signal(
        barrier, inc=1, device_id={"grp": 1 - g, "sp": s, "tp": t}, device_id_type=MESH
    )
    loads[0].wait()
    pl.semaphore_wait(barrier, 2 * (n - 1) + 1)

    tok_far = copy_to(tok.at[t], tok.at[t], sent, r_tok.at[0], s, far)
    tok_near = copy_to(tok.at[t], tok.at[t], sent, r_tok.at[1], s, near)
    tok_fwd = copy_to(tok.at[far], tok.at[far], sent, r_tok.at[2], s, near)
    z_slot = xt.at[jnp.where(is_hub, 1, 0), core]
    z_recv = r_z.at[jnp.where(is_hub, 1, 0)]
    z_own = copy_to(tok.at[t], z_slot, sent, z_recv, hub_over, t)
    z_far = copy_to(tok.at[far], z_slot, sent, z_recv, hub_over, t)
    own_first = side != upper
    tok_far.start()
    tok_near.start()
    weights = (wcv, wco, wci)
    order = (2, 0, 1)
    pieces_per = 4
    chunk = wcv.shape[0] // (2 * pieces_per)
    chunks = [(m, c) for m in order for c in range(pieces_per)]

    def chunk_rows(half, c):
        return pl.ds(pl.multiple_of((pieces_per * half + c) * chunk, chunk), chunk)

    w_sends, y_sends = [], []
    for k, (m, c) in enumerate(chunks):
        w_sends.append(
            copy_to(
                weights[m].at[chunk_rows(g, c)],
                wx.at[m, chunk_rows(g, c)],
                sent,
                r_w.at[k],
                mate,
                t,
            )
        )
        block = wx.at[m, chunk_rows(g, c)]
        y_sends.append(copy_to(block, block, sent, r_y.at[m], s, t, grp=1 - g))

    def arrived(ref, sem):
        copy_to(ref, ref, sent, sem, s, near).wait_recv()

    def relay(k):
        w_sends[k].wait_recv()
        y_sends[k].start()

    for load in loads[5:8]:
        load.wait()
    for copy in w_sends[:4]:
        copy.start()

    @pl.when(own_first)
    def _():
        z_own.start()

    for copy in w_sends[4:6]:
        copy.start()
    for load in loads[1:5] + loads[8:]:
        load.wait()
    def scaled_slice(block, f):
        gain_f = gain[pl.ds(pl.multiple_of(f * width, width), width)][None, :].astype(f32)
        return (block.astype(f32) * gain_f).astype(bf16)

    def features(f):
        return pl.ds(pl.multiple_of(f * width, width), width)

    def square_sum(f):
        piece = tok[f].astype(f32)
        return jnp.sum(piece * piece, axis=1, keepdims=True)

    def kv_product(scaled, f):
        return dot_t(scaled, wkv[:, features(f)])

    def r_product(scaled, f):
        return dot_t(scaled, wr[:, features(f)])

    def project(f):
        scaled = scaled_slice(tok[f], f)
        sums = (kv_product(scaled, f), r_product(scaled, f), dot(scaled, wq[f]))
        return (square_sum(f),) + sums

    squares, kv_sum, r_sum, q_sum = project(t)
    copy_to(tok.at[near], tok.at[near], sent, r_tok.at[1], s, near).wait_recv()
    more = project(near)
    squares, kv_sum = squares + more[0], kv_sum + more[1]
    r_sum, q_sum = r_sum + more[2], q_sum + more[3]
    copy_to(tok.at[far], tok.at[far], sent, r_tok.at[0], s, far).wait_recv()
    tok_fwd.start()

    @pl.when(jnp.logical_not(own_first))
    def _():
        z_far.start()

    for copy in w_sends[6:9]:
        copy.start()
    more = project(far)
    squares, kv_sum = squares + more[0], kv_sum + more[1]
    r_sum, q_sum = r_sum + more[2], q_sum + more[3]
    copy_to(tok.at[diag], tok.at[diag], sent, r_tok.at[2], s, near).wait_recv()
    last = scaled_slice(tok[diag], diag)
    squares = squares + square_sum(diag)
    kv_sum = kv_sum + kv_product(last, diag)
    row_scale = lax.rsqrt(squares / (n * width) + EPS)
    kw = wkv.shape[0]
    place = (
        lax.broadcasted_iota(jnp.int32, (kw, 2 * kw), 1)
        == lax.broadcasted_iota(jnp.int32, (kw, 2 * kw), 0) + kw * core
    )
    place = jnp.where(place, 1.0, 0.0).astype(bf16)
    kvp[t] = dot((row_scale * kv_sum).astype(bf16), place).astype(bf16)
    kv_sends = [
        copy_to(kvp.at[t], kvp.at[t], sent, r_kv, s, p) for i, p in enumerate(tp_peers)
    ]
    for copy in (kv_sends[1], kv_sends[2], kv_sends[0]):
        copy.start()
    q_sum = q_sum + dot(last, wq[diag])
    r_sum = r_sum + r_product(last, diag)
    qp[t] = (row_scale * q_sum).astype(bf16)
    q_sends = [
        copy_to(qp.at[t], qp.at[t], sent, r_q, s, p) for i, p in enumerate(tp_peers)
    ]
    for copy in (q_sends[1], q_sends[2], q_sends[0]):
        copy.start()

    cos_v, sin_v = cosine[...], sine[...]
    lanes = cos_v.shape[1]
    turn_r = lax.broadcasted_iota(jnp.int32, (lanes, lanes), 0)
    turn_c = lax.broadcasted_iota(jnp.int32, (lanes, lanes), 1)
    half = ROPE // 2
    low = lax.rem(turn_c, ROPE) < half
    turn = jnp.where(
        low & (turn_r == turn_c + half), -1.0, jnp.where((~low) & (turn_r == turn_c - half), 1.0, 0.0)
    ).astype(bf16)
    spread_r = lax.broadcasted_iota(jnp.int32, (ROPE, lanes), 0)
    spread_c = lax.broadcasted_iota(jnp.int32, (ROPE, lanes), 1)
    spread = jnp.where(lax.rem(spread_c, ROPE) == spread_r, 1.0, 0.0).astype(bf16)
    rope_raw = dot((row_scale * r_sum).astype(bf16), spread).astype(bf16)
    k_rope = (rope_raw.astype(f32) * cos_v + dot(rope_raw, turn) * sin_v).astype(bf16)
    groups = lanes // ROPE
    slab = rows // groups
    slab_lane = lax.div(lax.broadcasted_iota(jnp.int32, (slab, lanes), 1), ROPE)
    packed = jnp.zeros((slab, lanes), f32)
    for i in range(groups):
        packed = jnp.where(slab_lane == i, k_rope[i * slab : (i + 1) * slab].astype(f32), packed)
    rk[s] = packed.astype(bf16)
    rk_sends = [
        copy_to(rk.at[s], rk.at[s], sent, r_rk, lax.rem(s + k, n), t) for k in range(1, n)
    ]
    for copy in (rk_sends[1], rk_sends[0], rk_sends[2]):
        copy.start()

    mine_scaled = scaled_slice(tok[s], s)
    for m in order:
        own[m] = dot(mine_scaled, weights[m][...])
    for k in range(4):
        relay(k)

    edge = before.shape[0]
    up = copy_to(gate.at[pl.ds(rows - edge, edge)], before, sent, r_h.at[0], s + 1, t)
    down = copy_to(gate.at[pl.ds(0, edge)], after, sent, r_h.at[1], s - 1, t)

    def take(m):
        arrived(got.at[m], r_p.at[m])
        own[m] = own[m] + got[m].astype(f32)

    def summed(i):
        return (row_scale * own[i]).astype(bf16).astype(f32)

    def gate_part():
        take(2)
        take(0)
        gate[...] = (summed(2) * summed(0)).astype(bf16)

        @pl.when(s < n - 1)
        def _():
            up.start()

        @pl.when(s > 0)
        def _():
            down.start()

    p_sends = []
    for i in range(2):
        for m in range(3):
            target = hub_over if i else end_over
            p_sends.append(
                copy_to(part.at[i, m], got.at[m], sent, r_p.at[m], target, t)
            )
    x_sends = []
    for i in range(2):
        slot = xt.at[i, core]
        x_sends.append(copy_to(slot, slot, sent, r_xf, s, near))

    def conv_block(j):
        m = order[j]
        arrived(wx.at[m, pl.ds(0, wx.shape[1] // 2)], r_y.at[m])

        @pl.when(is_hub)
        def _():
            first = jnp.concatenate([xt[i, lax.rem(s, 2)] for i in range(2)], axis=0)
            second = jnp.concatenate([xt[i, lax.rem(mate, 2)] for i in range(2)], axis=0)
            total = dot(scaled_slice(first, s), weights[m][...]) + dot(
                scaled_slice(second, mate), wx[m]
            )
            for i in range(2):
                part[i, m] = total[i * rows : (i + 1) * rows].astype(bf16)
                p_sends[3 * i + m].start()

        own[m] = own[m] + dot(scaled_slice(tok[mate], mate), wx[m])

    arrived(kvp.at[pl.ds(0, n - 1)], r_kv)
    kv_float = jnp.concatenate(
        [kvp[j].astype(f32) + kvp[j + 1].astype(f32) for j in range(0, n, 2)], axis=1
    )
    kv_scale = lax.rsqrt(jnp.mean(kv_float * kv_float, axis=1, keepdims=True) + EPS)
    kvr[s] = (kv_float * kv_scale * kvg[...][None, :].astype(f32)).astype(bf16)
    def quarter(index):
        return pl.ds(pl.multiple_of(index * (rows // n), rows // n), rows // n)

    mine = quarter(t)
    kz_sends = []
    for k in (2, 1, 3):
        z = lax.rem(s + k, n)
        copy = copy_to(
            kvr.at[s, mine], kvr.at[s, mine], sent, r_kz.at[k - 1], z, t
        )
        copy.start()
        kz_sends.append(copy)
    for copy in w_sends[9:]:
        copy.start()

    for k in range(4, 8):
        relay(k)

    @pl.when(is_hub)
    def _():
        for i in range(2):
            slot = xt.at[i, core]
            copy_to(slot, slot, sent, r_z.at[i], s, near).wait_recv()
            x_sends[i].start()
        arrived(xt.at[:, core], r_xf)

    conv_block(0)
    for k in range(8, 10):
        relay(k)

    arrived(qp.at[pl.ds(0, n - 1)], r_q)
    q_float = [qp[j].astype(f32) for j in range(n)]
    qw = q_float[0].shape[1]
    q_square = sum(jnp.sum(q * q, axis=1, keepdims=True) for q in q_float)
    q_scale = lax.rsqrt(q_square / (n * qw) + EPS)
    q_normed = jnp.concatenate(
        [(q * q_scale * qg[j * qw : (j + 1) * qw][None, :].astype(f32)).astype(bf16) for j, q in enumerate(q_float)], axis=1
    )
    q_nope = dot(q_normed, wqn[...]).astype(bf16)
    q_raw = dot(q_normed, wqr[...])
    w_turned = dot(wqr[...], turn).astype(bf16)
    q_rope = (q_raw * cos_v + dot(q_normed, w_turned) * sin_v).astype(bf16)

    for k in range(10, 12):
        relay(k)
    kf_sends = []
    for k in (2, 1, 3):
        z = lax.rem(s + n - k, n)
        copy_to(
            kvr.at[z, mine], kvr.at[z, mine], sent, r_kz.at[k - 1], z, t
        ).wait_recv()
        for i, p in enumerate(tp_peers):
            copy = copy_to(
                kvr.at[z, mine], kvr.at[z, mine], sent, r_kf, s, p
            )
            copy.start()
            kf_sends.append(copy)
    conv_block(1)
    conv_block(2)
    arrived(kvr.at[pl.ds(0, n - 1), pl.ds(0, (n - 1) * (rows // n))], r_kf)

    @pl.when(is_hub)
    def _():
        gate_part()

    latent = jnp.concatenate(
        [kvr[j, i * slab : (i + 1) * slab] for i in range(groups) for j in range(n)], axis=0
    )
    arrived(rk.at[pl.ds(0, n - 1)], r_rk)
    packs = jnp.concatenate([rk[j] for j in range(n)], axis=0)
    same = lax.rem(turn_r, ROPE) == lax.rem(turn_c, ROPE)
    ropes = jnp.concatenate(
        [
            dot(packs, jnp.where(same & (lax.div(turn_r, ROPE) == i), 1.0, 0.0).astype(bf16))
            for i in range(groups)
        ],
        axis=0,
    ).astype(bf16)
    keys = dot(latent, wkn[...]).astype(bf16)
    values = dot(latent, wva[...]).astype(bf16)
    heads = wqn.shape[1] // NOPE
    factor = (NOPE + ROPE) ** (-0.5)
    pair = 2 * NOPE
    lane = lax.broadcasted_iota(jnp.int32, (rows, pair), 1)
    lane_r = lax.broadcasted_iota(jnp.int32, (rows, lanes), 1)
    pieces = []
    for p in range(heads // 2):
        cut = slice(p * pair, (p + 1) * pair)
        key_pair = jnp.concatenate([keys[:, cut], ropes], axis=1)
        value_pair = values[:, cut]
        outs = []
        for i in range(2):
            h = 2 * p + i
            in_head = (lane >= i * NOPE) & (lane < (i + 1) * NOPE)
            in_rope = (lane_r >= h * ROPE) & (lane_r < (h + 1) * ROPE)
            query = jnp.concatenate(
                [
                    jnp.where(in_head, q_nope[:, cut].astype(f32), 0.0).astype(bf16),
                    jnp.where(in_rope, q_rope.astype(f32), 0.0).astype(bf16),
                ],
                axis=1,
            )
            scores = dot_t(query, key_pair) * factor
            peak = jnp.max(scores, axis=1, keepdims=True)
            weights = jnp.exp(scores - peak)
            total = jnp.sum(weights, axis=1, keepdims=True)
            outs.append(dot(weights.astype(bf16), value_pair) / total)
        pieces.append(jnp.where(lane < NOPE, outs[0], outs[1]).astype(bf16))
    y_attn = jnp.concatenate(pieces, axis=1)
    for j in range(n):
        acc[j] = dot(y_attn, woa[j])

    @pl.when(jnp.logical_not(is_hub))
    def _():
        gate_part()

    take(1)
    conv_outer = summed(1)
    middle = gate[...].astype(f32)
    kernel = [taps[i : i + 1, :].astype(f32) for i in range(3)]
    row = lax.broadcasted_iota(jnp.int32, middle.shape, 0)
    previous = pltpu.roll(middle, 1, 0)
    following = pltpu.roll(middle, rows - 1, 0)

    @pl.when(s > 0)
    def _():
        up.wait_recv()

    @pl.when(s == 0)
    def _():
        before[...] = jnp.zeros_like(before)

    @pl.when(s < n - 1)
    def _():
        down.wait_recv()

    @pl.when(s == n - 1)
    def _():
        after[...] = jnp.zeros_like(after)

    first = before[...].astype(f32)[edge - 1 : edge, :]
    last = after[...].astype(f32)[0:1, :]
    previous = jnp.where(row == 0, first, previous)
    following = jnp.where(row == rows - 1, last, following)
    conv_out = previous * kernel[0] + middle * kernel[1] + following * kernel[2]
    y_conv = (conv_outer * conv_out).astype(bf16)

    def share(j):
        return acc[j] + dot(y_conv, woc[j])

    put_near[0] = share(diag).astype(bf16)
    o_diag = copy_to(put_near.at[0], got_near.at[0], sent, r_o.at[0], s, near)
    o_diag.start()
    far_share = share(far).astype(bf16).astype(f32)
    o_diag.wait_recv()
    put_far[...] = (far_share + got_near[0].astype(f32)).astype(bf16)
    o_far = copy_to(put_far, got_far, sent, r_o.at[1], s, far)
    o_far.start()
    put_near[1] = share(near).astype(bf16)
    o_near = copy_to(put_near.at[1], got_near.at[1], sent, r_o.at[2], s, near)
    o_near.start()
    my_share = share(t).astype(bf16).astype(f32)
    o_near.wait_recv()
    my_share = my_share + got_near[1].astype(f32)

    tok_far.wait_send()
    tok_near.wait_send()
    tok_fwd.wait_send()

    z_own.wait_send()
    for copy in kv_sends + q_sends + rk_sends + kz_sends + kf_sends + w_sends + y_sends:
        copy.wait_send()

    @pl.when(is_hub)
    def _():
        for copy in p_sends + x_sends:
            copy.wait_send()

    @pl.when(s < n - 1)
    def _():
        up.wait_send()

    @pl.when(s > 0)
    def _():
        down.wait_send()

    o_diag.wait_send()
    o_near.wait_send()
    o_far.wait()
    out_ref[...] = (my_share + got_far[...].astype(f32)).astype(bf16)


def fits(grp, sp, tp, tokens, mix_gain, w_conv_value, *others):
    rows, width = tokens.shape
    if grp != 2 or sp != 4 or tp != 4 or rows * sp > width * tp:
        return False
    return width % 128 == 0 and rows % 64 == 0 and w_conv_value.shape[0] % 64 == 0


def fused(
    sp,
    tp,
    tokens,
    mix_gain,
    w_conv_value,
    w_conv_outer,
    w_conv_inner,
    conv_kernel,
    w_q_down,
    w_kv_down,
    w_rope_key,
    q_gain,
    kv_gain,
    w_q_nope,
    w_q_rope,
    w_k_nope,
    w_value,
    w_out_conv,
    w_out_attn,
):
    f32, bf16 = jnp.float32, jnp.bfloat16
    n = tp
    rows, width = tokens.shape
    heads = w_q_nope.shape[1] // NOPE
    inverse = np.float32(THETA) ** (-np.arange(0, ROPE, 2, dtype=np.float32) / np.float32(ROPE))
    phase = np.arange(sp * rows, dtype=np.float32)[:, None] * inverse[None, :].astype(np.float32)
    phase = np.tile(phase, (1, 2 * heads)).reshape(sp, rows, heads * ROPE)
    cosine, sine = np.cos(phase).astype(np.float32), np.sin(phase).astype(np.float32)
    operands = (
        tokens,
        mix_gain,
        w_conv_value,
        w_conv_outer,
        w_conv_inner,
        conv_kernel,
        w_q_down.reshape(n, width, -1),
        w_kv_down.T,
        w_rope_key.T,
        q_gain,
        kv_gain,
        w_q_nope,
        w_q_rope,
        w_k_nope,
        w_value,
        w_out_conv,
        w_out_attn,
        jnp.asarray(cosine),
        jnp.asarray(sine),
    )
    vm = pltpu.VMEM
    cw = w_conv_value.shape[1]
    lat = kv_gain.shape[0]
    lanes = heads * ROPE
    scratch = [vm((n, rows, width), bf16)]
    scratch += [vm(x.shape, x.dtype) for x in operands[1:15]]
    scratch += [vm((n, w_out_conv.shape[0], width), bf16)] * 2
    scratch += [vm((rows, lanes), f32)] * 2
    scratch += [
        vm((3,) + w_conv_value.shape, bf16),
        vm((2, 2, rows, width), bf16),
        vm((2, 3, rows, cw), bf16),
        vm((3, rows, cw), bf16),
        vm((3, rows, cw), f32),
        vm((n, rows, w_q_down.shape[1]), bf16),
        vm((n, rows, 2 * w_kv_down.shape[1]), bf16),
        vm((n, rows, lat), bf16),
        vm((n, rows // heads, lanes), bf16),
        vm((rows, cw), bf16),
        vm((16, cw), bf16),
        vm((16, cw), bf16),
        vm((n, rows, width), f32),
        vm((2, rows, width), bf16),
        vm((2, rows, width), bf16),
        vm((rows, width), bf16),
        vm((rows, width), bf16),
    ]
    dma = pltpu.SemaphoreType.DMA
    scratch += [dma((4,)), dma, dma((3,)), dma((2,)), dma, dma((12,)), dma((3,)), dma, dma]
    scratch += [dma((n - 1,)), dma, dma, dma((3,)), dma((2,)), dma((3,))]
    return pl.pallas_call(
        functools.partial(mixer_kernel, n),
        out_shape=pltpu.VMEM((rows, width), bf16),
        in_specs=[pl.BlockSpec(memory_space=pl.ANY)] * len(operands),
        out_specs=pl.BlockSpec(memory_space=pltpu.VMEM),
        scratch_shapes=scratch,
        compiler_params=pltpu.CompilerParams(collective_id=0, has_side_effects=True),
    )(*operands)


def solution(mesh):
    placed = (
        P(("grp", "sp"), "tp"),
        P(),
        P("sp", "tp"),
        P("sp", "tp"),
        P("sp", "tp"),
        P(None, "tp"),
        P(None, "tp"),
        P(None, "tp"),
        P(),
        P(),
        P(),
        P(None, "tp"),
        P(None, "tp"),
        P(None, "tp"),
        P(None, "tp"),
        P("tp", None),
        P("tp", None),
    )
    grp, sp, tp = mesh.shape["grp"], mesh.shape["sp"], mesh.shape["tp"]

    def per_device(*args):
        if fits(grp, sp, tp, *args):
            return fused(sp, tp, *args)
        return gathered_weights(*args)

    return jax.shard_map(
        per_device, mesh=mesh, in_specs=placed, out_specs=P(("grp", "sp"), "tp"), check_vma=False
    )
```

```python
import functools

import jax
import jax.numpy as jnp
import numpy as np
from jax import lax
from jax.experimental import pallas as pl
from jax.experimental.pallas import tpu as pltpu
from jax.sharding import PartitionSpec as P

MESH = pl.DeviceIdType.MESH

D = 2048
NOPE = 64
ROPE = 32
VALUE = 64


EPS = 1e-06
THETA = 10000.0


def with_halo(x, sides, width):
    for axis, dim in sides:
        size, length = (lax.axis_size(axis), x.shape[dim])
        up = [(i, (i + 1) % size) for i in range(size - 1)]
        down = [(j, i) for i, j in up]
        last = lax.slice_in_dim(x, length - width, length, axis=dim)
        first = lax.slice_in_dim(x, 0, width, axis=dim)
        before = lax.ppermute(last, axis, up)
        after = lax.ppermute(first, axis, down)
        x = jnp.concatenate([before, x, after], axis=dim)
    return x


def rms_scale(values):
    return lax.rsqrt(jnp.mean(values * values, axis=-1, keepdims=True) + EPS)


def angles(positions, width):
    inverse = THETA ** (-jnp.arange(0, width, 2, dtype=jnp.float32) / width)
    phase = positions[:, None] * inverse[None, :]
    phase = jnp.concatenate([phase, phase], axis=-1)
    return (jnp.cos(phase), jnp.sin(phase))


def turned(values, cosine, sine):
    half = values.shape[-1] // 2
    first = values[..., :half]
    second = values[..., half:]
    return values * cosine + jnp.concatenate([-second, first], axis=-1) * sine


def block_rows(count):
    for candidate in range(min(count, 1024), 0, -1):
        if count % candidate == 0 and candidate % 128 == 0:
            return candidate
    for candidate in range(min(count, 1024), 0, -1):
        if count % candidate == 0:
            return candidate
    return count


def gathered_weights(
    tokens,
    mix_gain,
    w_conv_value,
    w_conv_outer,
    w_conv_inner,
    conv_kernel,
    w_q_down,
    w_kv_down,
    w_rope_key,
    q_gain,
    kv_gain,
    w_q_nope,
    w_q_rope,
    w_k_nope,
    w_value,
    w_out_conv,
    w_out_attn,
):
    f32 = jnp.float32
    bf16 = jnp.bfloat16
    rows = tokens.shape[0]
    conv_value_w, conv_outer_w, conv_inner_w = (
        lax.all_gather(w_conv_value, "sp", axis=0, tiled=True),
        lax.all_gather(w_conv_outer, "sp", axis=0, tiled=True),
        lax.all_gather(w_conv_inner, "sp", axis=0, tiled=True),
    )
    matrices = (conv_value_w, conv_outer_w, conv_inner_w, w_q_down, w_kv_down, w_rope_key)
    gain = mix_gain.astype(f32)
    piece_f = lax.all_gather(tokens, "tp", axis=1, tiled=True).astype(f32)
    scaled = (piece_f * gain).astype(bf16)
    updated = tuple((jnp.dot(scaled, matrix, preferred_element_type=f32) for matrix in matrices))
    squares = jnp.sum(piece_f * piece_f, axis=1)
    row_scale = lax.rsqrt(squares / D + EPS)[:, None]
    conv_value, conv_outer, conv_inner, q_part, kv_part, rope_raw = [
        (row_scale * total).astype(bf16) for total in updated
    ]
    gated = (conv_inner.astype(f32) * conv_value.astype(f32)).astype(bf16)
    padded = with_halo(gated, (("sp", 0),), 1).astype(f32)
    kernel = conv_kernel.astype(f32)
    conv_out = padded[:-2] * kernel[0] + padded[1:-1] * kernel[1] + padded[2:] * kernel[2]
    y_conv = (conv_outer.astype(f32) * conv_out).astype(bf16)
    q_latent, kv_latent = (
        lax.all_gather(q_part, "tp", axis=1, tiled=True),
        lax.all_gather(kv_part, "tp", axis=1, tiled=True),
    )
    q_float = q_latent.astype(f32)
    q_normed = (q_float * rms_scale(q_float) * q_gain.astype(f32)).astype(bf16)
    kv_float = kv_latent.astype(f32)
    kv_normed = (kv_float * rms_scale(kv_float) * kv_gain.astype(f32)).astype(bf16)
    heads = w_q_nope.shape[1] // NOPE
    positions = (lax.axis_index("sp") * rows + jnp.arange(rows, dtype=jnp.int32)).astype(f32)
    cosine, sine = angles(positions, ROPE)
    q_nope = (
        jnp.dot(q_normed, w_q_nope, preferred_element_type=f32)
        .astype(bf16)
        .reshape(rows, heads, NOPE)
    )
    q_rope_raw = jnp.dot(q_normed, w_q_rope, preferred_element_type=f32).reshape(rows, heads, ROPE)
    q_rope = turned(q_rope_raw, cosine[:, None, :], sine[:, None, :]).astype(bf16)
    k_rope = turned(rope_raw.astype(f32), cosine, sine).astype(bf16)
    factor = (NOPE + ROPE) ** (-0.5)

    def attend(state, key_block, value_block, rope_block):
        peak, total, summed = state
        count = key_block.shape[0]
        keys3 = key_block.reshape(count, heads, NOPE)
        values3 = value_block.reshape(count, heads, VALUE)
        scores = jnp.einsum("qhd,khd->qhk", q_nope, keys3, preferred_element_type=f32)
        scores = scores + jnp.einsum("qhr,kr->qhk", q_rope, rope_block, preferred_element_type=f32)
        scores = scores * factor
        new_peak = jnp.maximum(peak, jnp.max(scores, axis=-1))
        fade = jnp.exp(peak - new_peak)
        weights = jnp.exp(scores - new_peak[..., None])
        total = total * fade + jnp.sum(weights, axis=-1)
        summed = summed * fade[..., None] + jnp.einsum(
            "qhk,khd->qhd", weights.astype(bf16), values3, preferred_element_type=f32
        )
        return (new_peak, total, summed)

    start_state = (
        jnp.full((rows, heads), -jnp.inf, f32),
        jnp.zeros((rows, heads), f32),
        jnp.zeros((rows, heads, VALUE), f32),
    )
    latent = lax.all_gather(kv_normed, "sp", axis=0, tiled=True)
    rope_keys = lax.all_gather(k_rope, "sp", axis=0, tiled=True)
    size = block_rows(latent.shape[0])
    count = latent.shape[0] // size

    def one_block(carry, blocks):
        latent_block, rope_block = blocks
        key_block = jnp.dot(latent_block, w_k_nope, preferred_element_type=f32).astype(bf16)
        value_block = jnp.dot(latent_block, w_value, preferred_element_type=f32).astype(bf16)
        return (attend(carry, key_block, value_block, rope_block), None)

    carry, ignored = lax.scan(
        one_block,
        start_state,
        (
            latent.reshape(count, size, latent.shape[1]),
            rope_keys.reshape(count, size, rope_keys.shape[1]),
        ),
    )
    peak, total, summed = carry
    y_attn = (summed / total[..., None]).astype(bf16).reshape(rows, heads * VALUE)
    partial_sum = jnp.dot(y_conv, w_out_conv, preferred_element_type=f32) + jnp.dot(
        y_attn, w_out_attn, preferred_element_type=f32
    )
    return (
        lax.psum_scatter(partial_sum.astype(jnp.bfloat16), "tp", scatter_dimension=1, tiled=True)
        .astype(jnp.float32)
        .astype(bf16)
    )


def copy_to(src, dst, send, recv, sp, tp, **group):
    return pltpu.make_async_remote_copy(
        src_ref=src,
        dst_ref=dst,
        send_sem=send,
        recv_sem=recv,
        device_id={"sp": sp, "tp": tp, **group},
        device_id_type=MESH,
    )


def dot(a, b):
    return jnp.dot(a, b, preferred_element_type=jnp.float32)


def dot_t(a, b):
    return lax.dot_general(a, b, (((1,), (1,)), ((), ())), preferred_element_type=jnp.float32)


def mixer_kernel(
    n,
    tokens_h,
    gain_h,
    wcv_h,
    wco_h,
    wci_h,
    taps_h,
    wq_h,
    wkv_h,
    wr_h,
    qg_h,
    kvg_h,
    wqn_h,
    wqr_h,
    wkn_h,
    wva_h,
    woc_h,
    woa_h,
    cos_h,
    sin_h,
    out_ref,
    tok,
    gain,
    wcv,
    wco,
    wci,
    taps,
    wq,
    wkv,
    wr,
    qg,
    kvg,
    wqn,
    wqr,
    wkn,
    wva,
    woc,
    woa,
    cosine,
    sine,
    wx,
    xt,
    xs,
    base,
    mine_other,
    part,
    got,
    own,
    qp,
    kvp,
    kvr,
    rk,
    gate,
    before,
    after,
    acc,
    put_near,
    got_near,
    put_far,
    got_far,
    got_early,
    load_sem,
    sent,
    r_tok,
    r_z,
    r_xf,
    r_w,
    r_y,
    r_q,
    r_kv,
    r_kz,
    r_kf,
    r_rk,
    r_p,
    r_h,
    r_o,
):
    f32, bf16 = jnp.float32, jnp.bfloat16
    g, s, t = lax.axis_index("grp"), lax.axis_index("sp"), lax.axis_index("tp")
    core = lax.rem(t, 2)
    near = t + 1 - 2 * core
    far = lax.rem(t + 2, n)
    diag = lax.rem(near + 2, n)
    rows, width = tok.shape[1], tok.shape[2]
    cw = wcv.shape[1]
    tp_peers = (near, far, diag)
    upper = lax.div(s, n // 2)
    side = lax.div(t, 2)
    is_hub = (s == 1) | (s == n - 2)
    mate = s + 1 - 2 * lax.rem(s, 2)
    hub_over = n // 2 - upper
    end_over = (n - 1) * (1 - upper)

    loads = [
        (tokens_h, tok.at[t]),
        (gain_h, gain),
        (wq_h, wq),
        (wkv_h, wkv),
        (wr_h, wr),
        (wcv_h, wcv),
        (wco_h, wco),
        (wci_h, wci),
        (taps_h, taps),
        (qg_h, qg),
        (kvg_h, kvg),
        (wqn_h, wqn),
        (wqr_h, wqr),
        (wkn_h, wkn),
        (wva_h, wva),
        (cos_h.at[s], cosine),
        (sin_h.at[s], sine),
    ]
    for j in range(n):
        columns = pl.ds(j * width, width)
        loads.append((woa_h.at[:, columns], woa.at[j]))
        loads.append((woc_h.at[:, columns], woc.at[j]))
    groups = [0] + [2] * 4 + [1] * 3 + [3] * (len(loads) - 8)
    loads = [pltpu.make_async_copy(a, b, load_sem.at[i]) for (a, b), i in zip(loads, groups)]
    for load in loads:
        load.start()

    barrier = pltpu.get_barrier_semaphore()
    for peer in tp_peers:
        pl.semaphore_signal(barrier, inc=1, device_id={"sp": s, "tp": peer}, device_id_type=MESH)
    for k in range(1, n):
        pl.semaphore_signal(
            barrier, inc=1, device_id={"sp": lax.rem(s + k, n), "tp": t}, device_id_type=MESH
        )
    pl.semaphore_signal(
        barrier, inc=1, device_id={"grp": 1 - g, "sp": s, "tp": t}, device_id_type=MESH
    )
    loads[0].wait()
    pl.semaphore_wait(barrier, 2 * (n - 1) + 1)

    tok_far = copy_to(tok.at[t], tok.at[t], sent, r_tok.at[0], s, far)
    tok_near = copy_to(tok.at[t], tok.at[t], sent, r_tok.at[1], s, near)
    tok_fwd = copy_to(tok.at[far], tok.at[far], sent, r_tok.at[2], s, near)
    z_slot = xt.at[jnp.where(is_hub, 1, 0), core]
    z_recv = r_z.at[jnp.where(is_hub, 1, 0)]
    z_own = copy_to(tok.at[t], z_slot, sent, z_recv, hub_over, t)
    z_far = copy_to(tok.at[far], z_slot, sent, z_recv, hub_over, t)
    own_first = side != upper
    tok_far.start()
    tok_near.start()
    weights = (wcv, wco, wci)
    order = (2, 0, 1)
    pieces_per = 4
    chunk = wcv.shape[0] // (2 * pieces_per)
    chunks = [(m, c) for m in order for c in range(pieces_per)]

    def chunk_rows(half, c):
        return pl.ds(pl.multiple_of((pieces_per * half + c) * chunk, chunk), chunk)

    w_sends, y_sends = [], []
    for k, (m, c) in enumerate(chunks):
        w_sends.append(
            copy_to(
                weights[m].at[chunk_rows(g, c)],
                wx.at[m, chunk_rows(g, c)],
                sent,
                r_w.at[k],
                mate,
                t,
            )
        )
        block = wx.at[m, chunk_rows(g, c)]
        y_sends.append(copy_to(block, block, sent, r_y.at[m], s, t, grp=1 - g))

    def arrived(ref, sem):
        copy_to(ref, ref, sent, sem, s, near).wait_recv()

    def relay(k):
        w_sends[k].wait_recv()
        y_sends[k].start()

    for load in loads[5:8]:
        load.wait()
    for copy in w_sends[:4]:
        copy.start()

    @pl.when(own_first)
    def _():
        z_own.start()

    for copy in w_sends[4:6]:
        copy.start()
    for load in loads[1:5] + loads[8:]:
        load.wait()
    def scaled_slice(block, f):
        gain_f = gain[pl.ds(pl.multiple_of(f * width, width), width)][None, :].astype(f32)
        return (block.astype(f32) * gain_f).astype(bf16)

    def features(f):
        return pl.ds(pl.multiple_of(f * width, width), width)

    def square_sum(f):
        piece = tok[f].astype(f32)
        return jnp.sum(piece * piece, axis=1, keepdims=True)

    def kv_product(scaled, f):
        return dot_t(scaled, wkv[:, features(f)])

    def r_product(scaled, f):
        return dot_t(scaled, wr[:, features(f)])

    def project(f):
        scaled = scaled_slice(tok[f], f)
        sums = (kv_product(scaled, f), r_product(scaled, f), dot(scaled, wq[f]))
        return (square_sum(f),) + sums

    squares, kv_sum, r_sum, q_sum = project(t)
    copy_to(tok.at[near], tok.at[near], sent, r_tok.at[1], s, near).wait_recv()
    more = project(near)
    squares, kv_sum = squares + more[0], kv_sum + more[1]
    r_sum, q_sum = r_sum + more[2], q_sum + more[3]
    copy_to(tok.at[far], tok.at[far], sent, r_tok.at[0], s, far).wait_recv()
    tok_fwd.start()

    @pl.when(jnp.logical_not(own_first))
    def _():
        z_far.start()

    for copy in w_sends[6:10]:
        copy.start()
    more = project(far)
    squares, kv_sum = squares + more[0], kv_sum + more[1]
    r_sum, q_sum = r_sum + more[2], q_sum + more[3]
    copy_to(tok.at[diag], tok.at[diag], sent, r_tok.at[2], s, near).wait_recv()
    last = scaled_slice(tok[diag], diag)
    squares = squares + square_sum(diag)
    kv_sum = kv_sum + kv_product(last, diag)
    row_scale = lax.rsqrt(squares / (n * width) + EPS)
    kw = wkv.shape[0]
    place = (
        lax.broadcasted_iota(jnp.int32, (kw, 2 * kw), 1)
        == lax.broadcasted_iota(jnp.int32, (kw, 2 * kw), 0) + kw * core
    )
    place = jnp.where(place, 1.0, 0.0).astype(bf16)
    kvp[t] = dot((row_scale * kv_sum).astype(bf16), place).astype(bf16)
    kv_sends = [
        copy_to(kvp.at[t], kvp.at[t], sent, r_kv, s, p) for i, p in enumerate(tp_peers)
    ]
    for copy in (kv_sends[1], kv_sends[2], kv_sends[0]):
        copy.start()
    q_sum = q_sum + dot(last, wq[diag])
    r_sum = r_sum + r_product(last, diag)
    qp[t] = (row_scale * q_sum).astype(bf16)
    q_sends = [
        copy_to(qp.at[t], qp.at[t], sent, r_q, s, p) for i, p in enumerate(tp_peers)
    ]
    for copy in (q_sends[1], q_sends[2], q_sends[0]):
        copy.start()

    cos_v, sin_v = cosine[...], sine[...]
    lanes = cos_v.shape[1]
    turn_r = lax.broadcasted_iota(jnp.int32, (lanes, lanes), 0)
    turn_c = lax.broadcasted_iota(jnp.int32, (lanes, lanes), 1)
    half = ROPE // 2
    low = lax.rem(turn_c, ROPE) < half
    turn = jnp.where(
        low & (turn_r == turn_c + half), -1.0, jnp.where((~low) & (turn_r == turn_c - half), 1.0, 0.0)
    ).astype(bf16)
    spread_r = lax.broadcasted_iota(jnp.int32, (ROPE, lanes), 0)
    spread_c = lax.broadcasted_iota(jnp.int32, (ROPE, lanes), 1)
    spread = jnp.where(lax.rem(spread_c, ROPE) == spread_r, 1.0, 0.0).astype(bf16)
    rope_raw = dot((row_scale * r_sum).astype(bf16), spread).astype(bf16)
    k_rope = (rope_raw.astype(f32) * cos_v + dot(rope_raw, turn) * sin_v).astype(bf16)
    groups = lanes // ROPE
    slab = rows // groups
    slab_lane = lax.div(lax.broadcasted_iota(jnp.int32, (slab, lanes), 1), ROPE)
    packed = jnp.zeros((slab, lanes), f32)
    for i in range(groups):
        packed = jnp.where(slab_lane == i, k_rope[i * slab : (i + 1) * slab].astype(f32), packed)
    rk[s] = packed.astype(bf16)
    rk_sends = [
        copy_to(rk.at[s], rk.at[s], sent, r_rk, lax.rem(s + k, n), t) for k in range(1, n)
    ]
    for copy in (rk_sends[1], rk_sends[0], rk_sends[2]):
        copy.start()

    mine_scaled = scaled_slice(tok[s], s)
    for m in order:
        own[m] = dot(mine_scaled, weights[m][...])
    for k in range(4):
        relay(k)

    edge = before.shape[0]
    up = copy_to(gate.at[pl.ds(rows - edge, edge)], before, sent, r_h.at[0], s + 1, t)
    down = copy_to(gate.at[pl.ds(0, edge)], after, sent, r_h.at[1], s - 1, t)

    def take(m):
        arrived(got.at[m], r_p.at[m])
        own[m] = own[m] + got[m].astype(f32)

    def summed(i):
        return (row_scale * own[i]).astype(bf16).astype(f32)

    def gate_part():
        take(2)
        take(0)
        gate[...] = (summed(2) * summed(0)).astype(bf16)

        @pl.when(s < n - 1)
        def _():
            up.start()

        @pl.when(s > 0)
        def _():
            down.start()

    p_sends = []
    for i in range(2):
        for m in range(3):
            target = hub_over if i else end_over
            p_sends.append(
                copy_to(part.at[i, m], got.at[m], sent, r_p.at[m], target, t)
            )
    x_sends = []
    for i in range(2):
        slot = xt.at[i, core]
        x_sends.append(copy_to(slot, slot, sent, r_xf, s, near))

    def conv_start():
        @pl.when(is_hub)
        def _():
            for i in range(2):
                piece_rows = pl.ds(i * rows, rows)
                xs[0, piece_rows] = scaled_slice(xt[i, lax.rem(s, 2)], s)
                xs[1, piece_rows] = scaled_slice(xt[i, lax.rem(mate, 2)], mate)
            base[order[0]] = dot(xs[0], weights[order[0]][...])

    def conv_ahead():
        @pl.when(is_hub)
        def _():
            for m in order[1:]:
                base[m] = dot(xs[0], weights[m][...])

        mine_other[...] = scaled_slice(tok[mate], mate)

    def conv_block(j):
        m = order[j]
        arrived(wx.at[m, pl.ds(0, wx.shape[1] // 2)], r_y.at[m])

        @pl.when(is_hub)
        def _():
            total = base[m] + dot(xs[1], wx[m])
            for i in (0, 1) if j == 2 else (1, 0):
                part[i, m] = total[i * rows : (i + 1) * rows].astype(bf16)
                p_sends[3 * i + m].start()

        own[m] = own[m] + dot(mine_other[...], wx[m])

    arrived(kvp.at[pl.ds(0, n - 1)], r_kv)
    kv_float = jnp.concatenate(
        [kvp[j].astype(f32) + kvp[j + 1].astype(f32) for j in range(0, n, 2)], axis=1
    )
    kv_scale = lax.rsqrt(jnp.mean(kv_float * kv_float, axis=1, keepdims=True) + EPS)
    kvr[s] = (kv_float * kv_scale * kvg[...][None, :].astype(f32)).astype(bf16)
    def quarter(index):
        return pl.ds(pl.multiple_of(index * (rows // n), rows // n), rows // n)

    mine = quarter(t)
    kz_sends = []
    for k in (2, 1, 3):
        z = lax.rem(s + k, n)
        copy = copy_to(
            kvr.at[s, mine], kvr.at[s, mine], sent, r_kz.at[k - 1], z, t
        )
        copy.start()
        kz_sends.append(copy)
    for copy in w_sends[10:]:
        copy.start()

    def pass_on(i):
        @pl.when(is_hub)
        def _():
            slot = xt.at[i, core]
            copy_to(slot, slot, sent, r_z.at[i], s, near).wait_recv()
            x_sends[i].start()

    relay(4)
    relay(5)
    pass_on(0)
    pass_on(1)
    relay(6)
    relay(7)

    @pl.when(is_hub)
    def _():
        arrived(xt.at[:, core], r_xf)

    conv_start()
    conv_ahead()
    conv_block(0)
    for k in range(8, 10):
        relay(k)

    arrived(qp.at[pl.ds(0, n - 1)], r_q)
    q_float = [qp[j].astype(f32) for j in range(n)]
    qw = q_float[0].shape[1]
    q_square = sum(jnp.sum(q * q, axis=1, keepdims=True) for q in q_float)
    q_scale = lax.rsqrt(q_square / (n * qw) + EPS)
    q_normed = jnp.concatenate(
        [(q * q_scale * qg[j * qw : (j + 1) * qw][None, :].astype(f32)).astype(bf16) for j, q in enumerate(q_float)], axis=1
    )
    q_nope = dot(q_normed, wqn[...]).astype(bf16)
    q_raw = dot(q_normed, wqr[...])
    w_turned = dot(wqr[...], turn).astype(bf16)
    q_rope = (q_raw * cos_v + dot(q_normed, w_turned) * sin_v).astype(bf16)

    for k in range(10, 12):
        relay(k)
    kf_sends = []
    for k in (2, 1, 3):
        z = lax.rem(s + n - k, n)
        copy_to(
            kvr.at[z, mine], kvr.at[z, mine], sent, r_kz.at[k - 1], z, t
        ).wait_recv()
        for i, p in enumerate(tp_peers):
            copy = copy_to(
                kvr.at[z, mine], kvr.at[z, mine], sent, r_kf, s, p
            )
            copy.start()
            kf_sends.append(copy)
    conv_block(1)
    conv_block(2)
    arrived(kvr.at[pl.ds(0, n - 1), pl.ds(0, (n - 1) * (rows // n))], r_kf)

    @pl.when(is_hub)
    def _():
        gate_part()

    latent = jnp.concatenate(
        [kvr[j, i * slab : (i + 1) * slab] for i in range(groups) for j in range(n)], axis=0
    )
    arrived(rk.at[pl.ds(0, n - 1)], r_rk)
    packs = jnp.concatenate([rk[j] for j in range(n)], axis=0)
    same = lax.rem(turn_r, ROPE) == lax.rem(turn_c, ROPE)
    ropes = jnp.concatenate(
        [
            dot(packs, jnp.where(same & (lax.div(turn_r, ROPE) == i), 1.0, 0.0).astype(bf16))
            for i in range(groups)
        ],
        axis=0,
    ).astype(bf16)
    keys = dot(latent, wkn[...]).astype(bf16)
    values = dot(latent, wva[...]).astype(bf16)
    heads = wqn.shape[1] // NOPE
    factor = (NOPE + ROPE) ** (-0.5)
    pair = 2 * NOPE
    lane = lax.broadcasted_iota(jnp.int32, (rows, pair), 1)
    lane_r = lax.broadcasted_iota(jnp.int32, (rows, lanes), 1)
    pieces = []
    for p in range(heads // 2):
        cut = slice(p * pair, (p + 1) * pair)
        key_pair = jnp.concatenate([keys[:, cut], ropes], axis=1)
        value_pair = values[:, cut]
        outs = []
        for i in range(2):
            h = 2 * p + i
            in_head = (lane >= i * NOPE) & (lane < (i + 1) * NOPE)
            in_rope = (lane_r >= h * ROPE) & (lane_r < (h + 1) * ROPE)
            query = jnp.concatenate(
                [
                    jnp.where(in_head, q_nope[:, cut].astype(f32), 0.0).astype(bf16),
                    jnp.where(in_rope, q_rope.astype(f32), 0.0).astype(bf16),
                ],
                axis=1,
            )
            scores = dot_t(query, key_pair) * factor
            peak = jnp.max(scores, axis=1, keepdims=True)
            weights = jnp.exp(scores - peak)
            total = jnp.sum(weights, axis=1, keepdims=True)
            outs.append(dot(weights.astype(bf16), value_pair) / total)
        pieces.append(jnp.where(lane < NOPE, outs[0], outs[1]).astype(bf16))
    y_attn = jnp.concatenate(pieces, axis=1)
    for j in range(n):
        acc[j] = dot(y_attn, woa[j])

    @pl.when(jnp.logical_not(is_hub))
    def _():
        gate_part()

    take(1)
    conv_outer = summed(1)
    middle = gate[...].astype(f32)
    kernel = [taps[i : i + 1, :].astype(f32) for i in range(3)]
    row = lax.broadcasted_iota(jnp.int32, middle.shape, 0)
    previous = pltpu.roll(middle, 1, 0)
    following = pltpu.roll(middle, rows - 1, 0)

    @pl.when(s > 0)
    def _():
        up.wait_recv()

    @pl.when(s == 0)
    def _():
        before[...] = jnp.zeros_like(before)

    @pl.when(s < n - 1)
    def _():
        down.wait_recv()

    @pl.when(s == n - 1)
    def _():
        after[...] = jnp.zeros_like(after)

    first = before[...].astype(f32)[edge - 1 : edge, :]
    last = after[...].astype(f32)[0:1, :]
    previous = jnp.where(row == 0, first, previous)
    following = jnp.where(row == rows - 1, last, following)
    conv_out = previous * kernel[0] + middle * kernel[1] + following * kernel[2]
    y_conv = (conv_outer * conv_out).astype(bf16)

    def share(j):
        return acc[j] + dot(y_conv, woc[j])

    early = got_early.shape[0]
    lead, rest = pl.ds(0, early), pl.ds(early, rows - early)
    put_near[0] = share(diag).astype(bf16)
    o_diag = copy_to(put_near.at[0, rest], got_near.at[0, rest], sent, r_o.at[0], s, near)
    o_diag.start()
    o_cross = copy_to(put_near.at[0, lead], got_early, sent, r_o.at[3], s, diag)
    o_cross.start()
    far_share = share(far).astype(bf16).astype(f32)
    put_far[lead] = far_share[:early].astype(bf16)
    o_lead = copy_to(put_far.at[lead], got_far.at[lead], sent, r_o.at[1], s, far)
    o_lead.start()
    o_diag.wait_recv()
    put_far[rest] = (far_share[early:] + got_near[0, rest].astype(f32)).astype(bf16)
    o_far = copy_to(put_far.at[rest], got_far.at[rest], sent, r_o.at[1], s, far)
    o_far.start()
    put_near[1] = share(near).astype(bf16)
    o_near = copy_to(put_near.at[1], got_near.at[1], sent, r_o.at[2], s, near)
    o_near.start()
    my_share = share(t).astype(bf16).astype(f32)
    o_near.wait_recv()
    my_share = my_share + got_near[1].astype(f32)

    tok_far.wait_send()
    tok_near.wait_send()
    tok_fwd.wait_send()

    z_own.wait_send()
    for copy in kv_sends + q_sends + rk_sends + kz_sends + kf_sends + w_sends + y_sends:
        copy.wait_send()

    @pl.when(is_hub)
    def _():
        for copy in p_sends + x_sends:
            copy.wait_send()

    @pl.when(s < n - 1)
    def _():
        up.wait_send()

    @pl.when(s > 0)
    def _():
        down.wait_send()

    for copy in (o_diag, o_cross, o_lead, o_near, o_far):
        copy.wait_send()
    arrived(got_early, r_o.at[3])
    arrived(got_far, r_o.at[1])
    my_share = my_share + got_far[...].astype(f32)
    out_ref[rest] = my_share[early:].astype(bf16)
    out_ref[lead] = (my_share[:early] + got_early[...].astype(f32)).astype(bf16)


def fits(grp, sp, tp, tokens, mix_gain, w_conv_value, *others):
    rows, width = tokens.shape
    if grp != 2 or sp != 4 or tp != 4 or rows * sp > width * tp:
        return False
    return width % 128 == 0 and rows % 64 == 0 and w_conv_value.shape[0] % 64 == 0


def fused(
    sp,
    tp,
    tokens,
    mix_gain,
    w_conv_value,
    w_conv_outer,
    w_conv_inner,
    conv_kernel,
    w_q_down,
    w_kv_down,
    w_rope_key,
    q_gain,
    kv_gain,
    w_q_nope,
    w_q_rope,
    w_k_nope,
    w_value,
    w_out_conv,
    w_out_attn,
):
    f32, bf16 = jnp.float32, jnp.bfloat16
    n = tp
    rows, width = tokens.shape
    heads = w_q_nope.shape[1] // NOPE
    inverse = np.float32(THETA) ** (-np.arange(0, ROPE, 2, dtype=np.float32) / np.float32(ROPE))
    phase = np.arange(sp * rows, dtype=np.float32)[:, None] * inverse[None, :].astype(np.float32)
    phase = np.tile(phase, (1, 2 * heads)).reshape(sp, rows, heads * ROPE)
    cosine, sine = np.cos(phase).astype(np.float32), np.sin(phase).astype(np.float32)
    operands = (
        tokens,
        mix_gain,
        w_conv_value,
        w_conv_outer,
        w_conv_inner,
        conv_kernel,
        w_q_down.reshape(n, width, -1),
        w_kv_down.T,
        w_rope_key.T,
        q_gain,
        kv_gain,
        w_q_nope,
        w_q_rope,
        w_k_nope,
        w_value,
        w_out_conv,
        w_out_attn,
        jnp.asarray(cosine),
        jnp.asarray(sine),
    )
    vm = pltpu.VMEM
    cw = w_conv_value.shape[1]
    lat = kv_gain.shape[0]
    lanes = heads * ROPE
    scratch = [vm((n, rows, width), bf16)]
    scratch += [vm(x.shape, x.dtype) for x in operands[1:15]]
    scratch += [vm((n, w_out_conv.shape[0], width), bf16)] * 2
    scratch += [vm((rows, lanes), f32)] * 2
    scratch += [
        vm((3,) + w_conv_value.shape, bf16),
        vm((2, 2, rows, width), bf16),
        vm((2, 2 * rows, width), bf16),
        vm((3, 2 * rows, cw), f32),
        vm((rows, width), bf16),
        vm((2, 3, rows, cw), bf16),
        vm((3, rows, cw), bf16),
        vm((3, rows, cw), f32),
        vm((n, rows, w_q_down.shape[1]), bf16),
        vm((n, rows, 2 * w_kv_down.shape[1]), bf16),
        vm((n, rows, lat), bf16),
        vm((n, rows // heads, lanes), bf16),
        vm((rows, cw), bf16),
        vm((16, cw), bf16),
        vm((16, cw), bf16),
        vm((n, rows, width), f32),
        vm((2, rows, width), bf16),
        vm((2, rows, width), bf16),
        vm((rows, width), bf16),
        vm((rows, width), bf16),
        vm((rows // 8, width), bf16),
    ]
    dma = pltpu.SemaphoreType.DMA
    scratch += [dma((4,)), dma, dma((3,)), dma((2,)), dma, dma((12,)), dma((3,)), dma, dma]
    scratch += [dma((n - 1,)), dma, dma, dma((3,)), dma((2,)), dma((4,))]
    return pl.pallas_call(
        functools.partial(mixer_kernel, n),
        out_shape=pltpu.VMEM((rows, width), bf16),
        in_specs=[pl.BlockSpec(memory_space=pl.ANY)] * len(operands),
        out_specs=pl.BlockSpec(memory_space=pltpu.VMEM),
        scratch_shapes=scratch,
        compiler_params=pltpu.CompilerParams(collective_id=0, has_side_effects=True),
    )(*operands)


def solution(mesh):
    placed = (
        P(("grp", "sp"), "tp"),
        P(),
        P("sp", "tp"),
        P("sp", "tp"),
        P("sp", "tp"),
        P(None, "tp"),
        P(None, "tp"),
        P(None, "tp"),
        P(),
        P(),
        P(),
        P(None, "tp"),
        P(None, "tp"),
        P(None, "tp"),
        P(None, "tp"),
        P("tp", None),
        P("tp", None),
    )
    grp, sp, tp = mesh.shape["grp"], mesh.shape["sp"], mesh.shape["tp"]

    def per_device(*args):
        if fits(grp, sp, tp, *args):
            return fused(sp, tp, *args)
        return gathered_weights(*args)

    return jax.shard_map(
        per_device, mesh=mesh, in_specs=placed, out_specs=P(("grp", "sp"), "tp"), check_vma=False
    )
```

```python
import functools

import jax
import jax.numpy as jnp
import numpy as np
from jax import lax
from jax.experimental import pallas as pl
from jax.experimental.pallas import tpu as pltpu
from jax.sharding import PartitionSpec as P

MESH = pl.DeviceIdType.MESH

D = 2048
NOPE = 64
ROPE = 32
VALUE = 64


EPS = 1e-06
THETA = 10000.0


def with_halo(x, sides, width):
    for axis, dim in sides:
        size, length = (lax.axis_size(axis), x.shape[dim])
        up = [(i, (i + 1) % size) for i in range(size - 1)]
        down = [(j, i) for i, j in up]
        last = lax.slice_in_dim(x, length - width, length, axis=dim)
        first = lax.slice_in_dim(x, 0, width, axis=dim)
        before = lax.ppermute(last, axis, up)
        after = lax.ppermute(first, axis, down)
        x = jnp.concatenate([before, x, after], axis=dim)
    return x


def rms_scale(values):
    return lax.rsqrt(jnp.mean(values * values, axis=-1, keepdims=True) + EPS)


def angles(positions, width):
    inverse = THETA ** (-jnp.arange(0, width, 2, dtype=jnp.float32) / width)
    phase = positions[:, None] * inverse[None, :]
    phase = jnp.concatenate([phase, phase], axis=-1)
    return (jnp.cos(phase), jnp.sin(phase))


def turned(values, cosine, sine):
    half = values.shape[-1] // 2
    first = values[..., :half]
    second = values[..., half:]
    return values * cosine + jnp.concatenate([-second, first], axis=-1) * sine


def block_rows(count):
    for candidate in range(min(count, 1024), 0, -1):
        if count % candidate == 0 and candidate % 128 == 0:
            return candidate
    for candidate in range(min(count, 1024), 0, -1):
        if count % candidate == 0:
            return candidate
    return count


def gathered_weights(
    tokens,
    mix_gain,
    w_conv_value,
    w_conv_outer,
    w_conv_inner,
    conv_kernel,
    w_q_down,
    w_kv_down,
    w_rope_key,
    q_gain,
    kv_gain,
    w_q_nope,
    w_q_rope,
    w_k_nope,
    w_value,
    w_out_conv,
    w_out_attn,
):
    f32 = jnp.float32
    bf16 = jnp.bfloat16
    rows = tokens.shape[0]
    conv_value_w, conv_outer_w, conv_inner_w = (
        lax.all_gather(w_conv_value, "sp", axis=0, tiled=True),
        lax.all_gather(w_conv_outer, "sp", axis=0, tiled=True),
        lax.all_gather(w_conv_inner, "sp", axis=0, tiled=True),
    )
    matrices = (conv_value_w, conv_outer_w, conv_inner_w, w_q_down, w_kv_down, w_rope_key)
    gain = mix_gain.astype(f32)
    piece_f = lax.all_gather(tokens, "tp", axis=1, tiled=True).astype(f32)
    scaled = (piece_f * gain).astype(bf16)
    updated = tuple((jnp.dot(scaled, matrix, preferred_element_type=f32) for matrix in matrices))
    squares = jnp.sum(piece_f * piece_f, axis=1)
    row_scale = lax.rsqrt(squares / D + EPS)[:, None]
    conv_value, conv_outer, conv_inner, q_part, kv_part, rope_raw = [
        (row_scale * total).astype(bf16) for total in updated
    ]
    gated = (conv_inner.astype(f32) * conv_value.astype(f32)).astype(bf16)
    padded = with_halo(gated, (("sp", 0),), 1).astype(f32)
    kernel = conv_kernel.astype(f32)
    conv_out = padded[:-2] * kernel[0] + padded[1:-1] * kernel[1] + padded[2:] * kernel[2]
    y_conv = (conv_outer.astype(f32) * conv_out).astype(bf16)
    q_latent, kv_latent = (
        lax.all_gather(q_part, "tp", axis=1, tiled=True),
        lax.all_gather(kv_part, "tp", axis=1, tiled=True),
    )
    q_float = q_latent.astype(f32)
    q_normed = (q_float * rms_scale(q_float) * q_gain.astype(f32)).astype(bf16)
    kv_float = kv_latent.astype(f32)
    kv_normed = (kv_float * rms_scale(kv_float) * kv_gain.astype(f32)).astype(bf16)
    heads = w_q_nope.shape[1] // NOPE
    positions = (lax.axis_index("sp") * rows + jnp.arange(rows, dtype=jnp.int32)).astype(f32)
    cosine, sine = angles(positions, ROPE)
    q_nope = (
        jnp.dot(q_normed, w_q_nope, preferred_element_type=f32)
        .astype(bf16)
        .reshape(rows, heads, NOPE)
    )
    q_rope_raw = jnp.dot(q_normed, w_q_rope, preferred_element_type=f32).reshape(rows, heads, ROPE)
    q_rope = turned(q_rope_raw, cosine[:, None, :], sine[:, None, :]).astype(bf16)
    k_rope = turned(rope_raw.astype(f32), cosine, sine).astype(bf16)
    factor = (NOPE + ROPE) ** (-0.5)

    def attend(state, key_block, value_block, rope_block):
        peak, total, summed = state
        count = key_block.shape[0]
        keys3 = key_block.reshape(count, heads, NOPE)
        values3 = value_block.reshape(count, heads, VALUE)
        scores = jnp.einsum("qhd,khd->qhk", q_nope, keys3, preferred_element_type=f32)
        scores = scores + jnp.einsum("qhr,kr->qhk", q_rope, rope_block, preferred_element_type=f32)
        scores = scores * factor
        new_peak = jnp.maximum(peak, jnp.max(scores, axis=-1))
        fade = jnp.exp(peak - new_peak)
        weights = jnp.exp(scores - new_peak[..., None])
        total = total * fade + jnp.sum(weights, axis=-1)
        summed = summed * fade[..., None] + jnp.einsum(
            "qhk,khd->qhd", weights.astype(bf16), values3, preferred_element_type=f32
        )
        return (new_peak, total, summed)

    start_state = (
        jnp.full((rows, heads), -jnp.inf, f32),
        jnp.zeros((rows, heads), f32),
        jnp.zeros((rows, heads, VALUE), f32),
    )
    latent = lax.all_gather(kv_normed, "sp", axis=0, tiled=True)
    rope_keys = lax.all_gather(k_rope, "sp", axis=0, tiled=True)
    size = block_rows(latent.shape[0])
    count = latent.shape[0] // size

    def one_block(carry, blocks):
        latent_block, rope_block = blocks
        key_block = jnp.dot(latent_block, w_k_nope, preferred_element_type=f32).astype(bf16)
        value_block = jnp.dot(latent_block, w_value, preferred_element_type=f32).astype(bf16)
        return (attend(carry, key_block, value_block, rope_block), None)

    carry, ignored = lax.scan(
        one_block,
        start_state,
        (
            latent.reshape(count, size, latent.shape[1]),
            rope_keys.reshape(count, size, rope_keys.shape[1]),
        ),
    )
    peak, total, summed = carry
    y_attn = (summed / total[..., None]).astype(bf16).reshape(rows, heads * VALUE)
    partial_sum = jnp.dot(y_conv, w_out_conv, preferred_element_type=f32) + jnp.dot(
        y_attn, w_out_attn, preferred_element_type=f32
    )
    return (
        lax.psum_scatter(partial_sum.astype(jnp.bfloat16), "tp", scatter_dimension=1, tiled=True)
        .astype(jnp.float32)
        .astype(bf16)
    )


def copy_to(src, dst, send, recv, sp, tp, **group):
    return pltpu.make_async_remote_copy(
        src_ref=src,
        dst_ref=dst,
        send_sem=send,
        recv_sem=recv,
        device_id={"sp": sp, "tp": tp, **group},
        device_id_type=MESH,
    )


def dot(a, b):
    return jnp.dot(a, b, preferred_element_type=jnp.float32)


def dot_t(a, b):
    return lax.dot_general(a, b, (((1,), (1,)), ((), ())), preferred_element_type=jnp.float32)


def mixer_kernel(
    n,
    tokens_h,
    gain_h,
    wcv_h,
    wco_h,
    wci_h,
    taps_h,
    wq_h,
    wkv_h,
    wr_h,
    qg_h,
    kvg_h,
    wqn_h,
    wqr_h,
    wkn_h,
    wva_h,
    woc_h,
    woa_h,
    cos_h,
    sin_h,
    out_ref,
    tok,
    gain,
    wcv,
    wco,
    wci,
    taps,
    wq,
    wkv,
    wr,
    qg,
    kvg,
    wqn,
    wqr,
    wkn,
    wva,
    woc,
    woa,
    cosine,
    sine,
    wx,
    xt,
    xs,
    base,
    mine_other,
    part,
    got,
    own,
    qp,
    kvp,
    kvr,
    rk,
    gate,
    before,
    after,
    acc,
    put_near,
    got_near,
    put_far,
    got_far,
    got_early,
    load_sem,
    sent,
    r_tok,
    r_z,
    r_xf,
    r_w,
    r_y,
    r_q,
    r_kv,
    r_kz,
    r_kf,
    r_rk,
    r_p,
    r_h,
    r_o,
):
    f32, bf16 = jnp.float32, jnp.bfloat16
    g, s, t = lax.axis_index("grp"), lax.axis_index("sp"), lax.axis_index("tp")
    core = lax.rem(t, 2)
    near = t + 1 - 2 * core
    far = lax.rem(t + 2, n)
    diag = lax.rem(near + 2, n)
    rows, width = tok.shape[1], tok.shape[2]
    cw = wcv.shape[1]
    tp_peers = (near, far, diag)
    upper = lax.div(s, n // 2)
    side = lax.div(t, 2)
    is_hub = (s == 1) | (s == n - 2)
    mate = s + 1 - 2 * lax.rem(s, 2)
    hub_over = n // 2 - upper
    end_over = (n - 1) * (1 - upper)

    loads = [
        (tokens_h, tok.at[t]),
        (gain_h, gain),
        (wq_h, wq),
        (wkv_h, wkv),
        (wr_h, wr),
        (wcv_h, wcv),
        (wco_h, wco),
        (wci_h, wci),
        (taps_h, taps),
        (qg_h, qg),
        (kvg_h, kvg),
        (wqn_h, wqn),
        (wqr_h, wqr),
        (wkn_h, wkn),
        (wva_h, wva),
        (cos_h.at[s], cosine),
        (sin_h.at[s], sine),
    ]
    for j in range(n):
        columns = pl.ds(j * width, width)
        loads.append((woa_h.at[:, columns], woa.at[j]))
        loads.append((woc_h.at[:, columns], woc.at[j]))
    groups = [0] + [2] * 4 + [1] * 3 + [3] * (len(loads) - 8)
    loads = [pltpu.make_async_copy(a, b, load_sem.at[i]) for (a, b), i in zip(loads, groups)]
    for load in loads:
        load.start()

    barrier = pltpu.get_barrier_semaphore()
    for peer in tp_peers:
        pl.semaphore_signal(barrier, inc=1, device_id={"sp": s, "tp": peer}, device_id_type=MESH)
    for k in range(1, n):
        pl.semaphore_signal(
            barrier, inc=1, device_id={"sp": lax.rem(s + k, n), "tp": t}, device_id_type=MESH
        )
    pl.semaphore_signal(
        barrier, inc=1, device_id={"grp": 1 - g, "sp": s, "tp": t}, device_id_type=MESH
    )
    loads[0].wait()
    pl.semaphore_wait(barrier, 2 * (n - 1) + 1)

    tok_far = copy_to(tok.at[t], tok.at[t], sent, r_tok.at[0], s, far)
    tok_near = copy_to(tok.at[t], tok.at[t], sent, r_tok.at[1], s, near)
    tok_fwd = copy_to(tok.at[far], tok.at[far], sent, r_tok.at[2], s, near)
    z_slot = xt.at[jnp.where(is_hub, 1, 0), core]
    z_recv = r_z.at[jnp.where(is_hub, 1, 0)]
    z_own = copy_to(tok.at[t], z_slot, sent, z_recv, hub_over, t)
    z_far = copy_to(tok.at[far], z_slot, sent, z_recv, hub_over, t)
    own_first = side != upper
    tok_far.start()
    tok_near.start()
    weights = (wcv, wco, wci)
    order = (2, 0, 1)
    pieces_per = 4
    chunk = wcv.shape[0] // (2 * pieces_per)
    chunks = [(m, c) for m in order for c in range(pieces_per)]

    def chunk_rows(half, c):
        return pl.ds(pl.multiple_of((pieces_per * half + c) * chunk, chunk), chunk)

    w_sends, y_sends = [], []
    for k, (m, c) in enumerate(chunks):
        w_sends.append(
            copy_to(
                weights[m].at[chunk_rows(g, c)],
                wx.at[m, chunk_rows(g, c)],
                sent,
                r_w.at[k],
                mate,
                t,
            )
        )
        block = wx.at[m, chunk_rows(g, c)]
        y_sends.append(copy_to(block, block, sent, r_y.at[m], s, t, grp=1 - g))

    def arrived(ref, sem):
        copy_to(ref, ref, sent, sem, s, near).wait_recv()

    def relay(k):
        w_sends[k].wait_recv()
        y_sends[k].start()

    for load in loads[5:8]:
        load.wait()
    for copy in w_sends[:4]:
        copy.start()

    @pl.when(own_first)
    def _():
        z_own.start()

    for copy in w_sends[4:7]:
        copy.start()
    for load in loads[1:5] + loads[8:]:
        load.wait()
    def scaled_slice(block, f):
        gain_f = gain[pl.ds(pl.multiple_of(f * width, width), width)][None, :].astype(f32)
        return (block.astype(f32) * gain_f).astype(bf16)

    def features(f):
        return pl.ds(pl.multiple_of(f * width, width), width)

    def square_sum(f):
        piece = tok[f].astype(f32)
        return jnp.sum(piece * piece, axis=1, keepdims=True)

    def kv_product(scaled, f):
        return dot_t(scaled, wkv[:, features(f)])

    def r_product(scaled, f):
        return dot_t(scaled, wr[:, features(f)])

    def project(f):
        scaled = scaled_slice(tok[f], f)
        sums = (kv_product(scaled, f), r_product(scaled, f), dot(scaled, wq[f]))
        return (square_sum(f),) + sums

    squares, kv_sum, r_sum, q_sum = project(t)
    copy_to(tok.at[near], tok.at[near], sent, r_tok.at[1], s, near).wait_recv()
    more = project(near)
    squares, kv_sum = squares + more[0], kv_sum + more[1]
    r_sum, q_sum = r_sum + more[2], q_sum + more[3]
    copy_to(tok.at[far], tok.at[far], sent, r_tok.at[0], s, far).wait_recv()
    tok_fwd.start()

    @pl.when(jnp.logical_not(own_first))
    def _():
        z_far.start()

    for copy in w_sends[7:10]:
        copy.start()
    more = project(far)
    squares, kv_sum = squares + more[0], kv_sum + more[1]
    r_sum, q_sum = r_sum + more[2], q_sum + more[3]
    copy_to(tok.at[diag], tok.at[diag], sent, r_tok.at[2], s, near).wait_recv()
    last = scaled_slice(tok[diag], diag)
    squares = squares + square_sum(diag)
    kv_sum = kv_sum + kv_product(last, diag)
    row_scale = lax.rsqrt(squares / (n * width) + EPS)
    kw = wkv.shape[0]
    place = (
        lax.broadcasted_iota(jnp.int32, (kw, 2 * kw), 1)
        == lax.broadcasted_iota(jnp.int32, (kw, 2 * kw), 0) + kw * core
    )
    place = jnp.where(place, 1.0, 0.0).astype(bf16)
    kvp[t] = dot((row_scale * kv_sum).astype(bf16), place).astype(bf16)
    kv_sends = [
        copy_to(kvp.at[t], kvp.at[t], sent, r_kv, s, p) for i, p in enumerate(tp_peers)
    ]
    for copy in (kv_sends[1], kv_sends[2], kv_sends[0]):
        copy.start()
    q_sum = q_sum + dot(last, wq[diag])
    r_sum = r_sum + r_product(last, diag)
    qp[t] = (row_scale * q_sum).astype(bf16)
    q_sends = [
        copy_to(qp.at[t], qp.at[t], sent, r_q, s, p) for i, p in enumerate(tp_peers)
    ]
    for copy in (q_sends[1], q_sends[2], q_sends[0]):
        copy.start()

    cos_v, sin_v = cosine[...], sine[...]
    lanes = cos_v.shape[1]
    turn_r = lax.broadcasted_iota(jnp.int32, (lanes, lanes), 0)
    turn_c = lax.broadcasted_iota(jnp.int32, (lanes, lanes), 1)
    half = ROPE // 2
    low = lax.rem(turn_c, ROPE) < half
    turn = jnp.where(
        low & (turn_r == turn_c + half), -1.0, jnp.where((~low) & (turn_r == turn_c - half), 1.0, 0.0)
    ).astype(bf16)
    spread_r = lax.broadcasted_iota(jnp.int32, (ROPE, lanes), 0)
    spread_c = lax.broadcasted_iota(jnp.int32, (ROPE, lanes), 1)
    spread = jnp.where(lax.rem(spread_c, ROPE) == spread_r, 1.0, 0.0).astype(bf16)
    rope_raw = dot((row_scale * r_sum).astype(bf16), spread).astype(bf16)
    k_rope = (rope_raw.astype(f32) * cos_v + dot(rope_raw, turn) * sin_v).astype(bf16)
    groups = lanes // ROPE
    slab = rows // groups
    slab_lane = lax.div(lax.broadcasted_iota(jnp.int32, (slab, lanes), 1), ROPE)
    packed = jnp.zeros((slab, lanes), f32)
    for i in range(groups):
        packed = jnp.where(slab_lane == i, k_rope[i * slab : (i + 1) * slab].astype(f32), packed)
    rk[s] = packed.astype(bf16)
    rk_sends = [
        copy_to(rk.at[s], rk.at[s], sent, r_rk, lax.rem(s + k, n), t) for k in range(1, n)
    ]
    for copy in (rk_sends[1], rk_sends[0], rk_sends[2]):
        copy.start()

    mine_scaled = scaled_slice(tok[s], s)
    for m in order:
        own[m] = dot(mine_scaled, weights[m][...])
    for k in range(4):
        relay(k)

    edge = before.shape[0]
    up = copy_to(gate.at[pl.ds(rows - edge, edge)], before, sent, r_h.at[0], s + 1, t)
    down = copy_to(gate.at[pl.ds(0, edge)], after, sent, r_h.at[1], s - 1, t)

    def take(m):
        arrived(got.at[m], r_p.at[m])
        own[m] = own[m] + got[m].astype(f32)

    def summed(i):
        return (row_scale * own[i]).astype(bf16).astype(f32)

    def gate_part():
        take(2)
        take(0)
        gate[...] = (summed(2) * summed(0)).astype(bf16)

        @pl.when(s < n - 1)
        def _():
            up.start()

        @pl.when(s > 0)
        def _():
            down.start()

    p_sends = []
    for i in range(2):
        for m in range(3):
            target = hub_over if i else end_over
            p_sends.append(
                copy_to(part.at[i, m], got.at[m], sent, r_p.at[m], target, t)
            )
    x_sends = []
    for i in range(2):
        slot = xt.at[i, core]
        x_sends.append(copy_to(slot, slot, sent, r_xf, s, near))

    def conv_start():
        @pl.when(is_hub)
        def _():
            for i in range(2):
                piece_rows = pl.ds(i * rows, rows)
                xs[0, piece_rows] = scaled_slice(xt[i, lax.rem(s, 2)], s)
                xs[1, piece_rows] = scaled_slice(xt[i, lax.rem(mate, 2)], mate)
            base[order[0]] = dot(xs[0], weights[order[0]][...])

    def conv_ahead():
        @pl.when(is_hub)
        def _():
            for m in order[1:]:
                base[m] = dot(xs[0], weights[m][...])

        mine_other[...] = scaled_slice(tok[mate], mate)

    def conv_block(j):
        m = order[j]
        arrived(wx.at[m, pl.ds(0, wx.shape[1] // 2)], r_y.at[m])

        @pl.when(is_hub)
        def _():
            if j == 2:
                for i in range(2):
                    block = pl.ds(i * rows, rows)
                    total = base[m, block] + dot(xs[1, block], wx[m])
                    part[i, m] = total.astype(bf16)
                    p_sends[3 * i + m].start()
            else:
                total = base[m] + dot(xs[1], wx[m])
                for i in (1, 0):
                    part[i, m] = total[i * rows : (i + 1) * rows].astype(bf16)
                    p_sends[3 * i + m].start()

        own[m] = own[m] + dot(mine_other[...], wx[m])

    arrived(kvp.at[pl.ds(0, n - 1)], r_kv)
    kv_float = jnp.concatenate(
        [kvp[j].astype(f32) + kvp[j + 1].astype(f32) for j in range(0, n, 2)], axis=1
    )
    kv_scale = lax.rsqrt(jnp.mean(kv_float * kv_float, axis=1, keepdims=True) + EPS)
    kvr[s] = (kv_float * kv_scale * kvg[...][None, :].astype(f32)).astype(bf16)
    def quarter(index):
        return pl.ds(pl.multiple_of(index * (rows // n), rows // n), rows // n)

    mine = quarter(t)
    kz_sends = []
    for k in (2, 1, 3):
        z = lax.rem(s + k, n)
        copy = copy_to(
            kvr.at[s, mine], kvr.at[s, mine], sent, r_kz.at[k - 1], z, t
        )
        copy.start()
        kz_sends.append(copy)
    for copy in w_sends[10:]:
        copy.start()

    def pass_on(i):
        @pl.when(is_hub)
        def _():
            slot = xt.at[i, core]
            copy_to(slot, slot, sent, r_z.at[i], s, near).wait_recv()
            x_sends[i].start()

    relay(4)
    relay(5)
    pass_on(0)
    pass_on(1)
    relay(6)
    relay(7)

    @pl.when(is_hub)
    def _():
        arrived(xt.at[:, core], r_xf)

    conv_start()
    conv_ahead()
    conv_block(0)
    for k in range(8, 10):
        relay(k)

    arrived(qp.at[pl.ds(0, n - 1)], r_q)
    q_float = [qp[j].astype(f32) for j in range(n)]
    qw = q_float[0].shape[1]
    q_square = sum(jnp.sum(q * q, axis=1, keepdims=True) for q in q_float)
    q_scale = lax.rsqrt(q_square / (n * qw) + EPS)
    q_normed = jnp.concatenate(
        [(q * q_scale * qg[j * qw : (j + 1) * qw][None, :].astype(f32)).astype(bf16) for j, q in enumerate(q_float)], axis=1
    )
    q_nope = dot(q_normed, wqn[...]).astype(bf16)
    q_raw = dot(q_normed, wqr[...])
    w_turned = dot(wqr[...], turn).astype(bf16)
    q_rope = (q_raw * cos_v + dot(q_normed, w_turned) * sin_v).astype(bf16)

    for k in range(10, 12):
        relay(k)
    kf_sends = []
    for k in (2, 1, 3):
        z = lax.rem(s + n - k, n)
        copy_to(
            kvr.at[z, mine], kvr.at[z, mine], sent, r_kz.at[k - 1], z, t
        ).wait_recv()
        for i, p in enumerate(tp_peers):
            copy = copy_to(
                kvr.at[z, mine], kvr.at[z, mine], sent, r_kf, s, p
            )
            copy.start()
            kf_sends.append(copy)
    conv_block(1)
    conv_block(2)
    arrived(kvr.at[pl.ds(0, n - 1), pl.ds(0, (n - 1) * (rows // n))], r_kf)

    @pl.when(is_hub)
    def _():
        gate_part()

    latent = jnp.concatenate(
        [kvr[j, i * slab : (i + 1) * slab] for i in range(groups) for j in range(n)], axis=0
    )
    arrived(rk.at[pl.ds(0, n - 1)], r_rk)
    packs = jnp.concatenate([rk[j] for j in range(n)], axis=0)
    same = lax.rem(turn_r, ROPE) == lax.rem(turn_c, ROPE)
    ropes = jnp.concatenate(
        [
            dot(packs, jnp.where(same & (lax.div(turn_r, ROPE) == i), 1.0, 0.0).astype(bf16))
            for i in range(groups)
        ],
        axis=0,
    ).astype(bf16)
    keys = dot(latent, wkn[...]).astype(bf16)
    values = dot(latent, wva[...]).astype(bf16)
    heads = wqn.shape[1] // NOPE
    factor = (NOPE + ROPE) ** (-0.5)
    pair = 2 * NOPE
    lane = lax.broadcasted_iota(jnp.int32, (rows, pair), 1)
    lane_r = lax.broadcasted_iota(jnp.int32, (rows, lanes), 1)
    pieces = []
    for p in range(heads // 2):
        cut = slice(p * pair, (p + 1) * pair)
        key_pair = jnp.concatenate([keys[:, cut], ropes], axis=1)
        value_pair = values[:, cut]
        outs = []
        for i in range(2):
            h = 2 * p + i
            in_head = (lane >= i * NOPE) & (lane < (i + 1) * NOPE)
            in_rope = (lane_r >= h * ROPE) & (lane_r < (h + 1) * ROPE)
            query = jnp.concatenate(
                [
                    jnp.where(in_head, q_nope[:, cut].astype(f32), 0.0).astype(bf16),
                    jnp.where(in_rope, q_rope.astype(f32), 0.0).astype(bf16),
                ],
                axis=1,
            )
            scores = dot_t(query, key_pair) * factor
            peak = jnp.max(scores, axis=1, keepdims=True)
            weights = jnp.exp(scores - peak)
            total = jnp.sum(weights, axis=1, keepdims=True)
            outs.append(dot(weights.astype(bf16), value_pair) / total)
        pieces.append(jnp.where(lane < NOPE, outs[0], outs[1]).astype(bf16))
    y_attn = jnp.concatenate(pieces, axis=1)
    for j in range(n):
        acc[j] = dot(y_attn, woa[j])

    @pl.when(jnp.logical_not(is_hub))
    def _():
        gate_part()

    take(1)
    conv_outer = summed(1)
    middle = gate[...].astype(f32)
    kernel = [taps[i : i + 1, :].astype(f32) for i in range(3)]
    row = lax.broadcasted_iota(jnp.int32, middle.shape, 0)
    previous = pltpu.roll(middle, 1, 0)
    following = pltpu.roll(middle, rows - 1, 0)

    @pl.when(s > 0)
    def _():
        up.wait_recv()

    @pl.when(s == 0)
    def _():
        before[...] = jnp.zeros_like(before)

    @pl.when(s < n - 1)
    def _():
        down.wait_recv()

    @pl.when(s == n - 1)
    def _():
        after[...] = jnp.zeros_like(after)

    first = before[...].astype(f32)[edge - 1 : edge, :]
    last = after[...].astype(f32)[0:1, :]
    previous = jnp.where(row == 0, first, previous)
    following = jnp.where(row == rows - 1, last, following)
    conv_out = previous * kernel[0] + middle * kernel[1] + following * kernel[2]
    y_conv = (conv_outer * conv_out).astype(bf16)

    def share(j):
        return acc[j] + dot(y_conv, woc[j])

    early = got_early.shape[0]
    lead, rest = pl.ds(0, early), pl.ds(early, rows - early)
    put_near[0] = share(diag).astype(bf16)
    o_diag = copy_to(put_near.at[0, rest], got_near.at[0, rest], sent, r_o.at[0], s, near)
    o_diag.start()
    o_cross = copy_to(put_near.at[0, lead], got_early, sent, r_o.at[3], s, diag)
    o_cross.start()
    far_share = share(far).astype(bf16).astype(f32)
    put_far[lead] = far_share[:early].astype(bf16)
    o_lead = copy_to(put_far.at[lead], got_far.at[lead], sent, r_o.at[1], s, far)
    o_lead.start()
    o_diag.wait_recv()
    put_far[rest] = (far_share[early:] + got_near[0, rest].astype(f32)).astype(bf16)
    o_far = copy_to(put_far.at[rest], got_far.at[rest], sent, r_o.at[1], s, far)
    o_far.start()
    put_near[1] = share(near).astype(bf16)
    o_near = copy_to(put_near.at[1], got_near.at[1], sent, r_o.at[2], s, near)
    o_near.start()
    my_share = share(t).astype(bf16).astype(f32)
    o_near.wait_recv()
    my_share = my_share + got_near[1].astype(f32)

    tok_far.wait_send()
    tok_near.wait_send()
    tok_fwd.wait_send()

    z_own.wait_send()
    for copy in kv_sends + q_sends + rk_sends + kz_sends + kf_sends + w_sends + y_sends:
        copy.wait_send()

    @pl.when(is_hub)
    def _():
        for copy in p_sends + x_sends:
            copy.wait_send()

    @pl.when(s < n - 1)
    def _():
        up.wait_send()

    @pl.when(s > 0)
    def _():
        down.wait_send()

    for copy in (o_diag, o_cross, o_lead, o_near, o_far):
        copy.wait_send()
    arrived(got_early, r_o.at[3])
    arrived(got_far, r_o.at[1])
    my_share = my_share + got_far[...].astype(f32)
    out_ref[rest] = my_share[early:].astype(bf16)
    out_ref[lead] = (my_share[:early] + got_early[...].astype(f32)).astype(bf16)


def fits(grp, sp, tp, tokens, mix_gain, w_conv_value, *others):
    rows, width = tokens.shape
    if grp != 2 or sp != 4 or tp != 4 or rows * sp > width * tp:
        return False
    return width % 128 == 0 and rows % 64 == 0 and w_conv_value.shape[0] % 64 == 0


def fused(
    sp,
    tp,
    tokens,
    mix_gain,
    w_conv_value,
    w_conv_outer,
    w_conv_inner,
    conv_kernel,
    w_q_down,
    w_kv_down,
    w_rope_key,
    q_gain,
    kv_gain,
    w_q_nope,
    w_q_rope,
    w_k_nope,
    w_value,
    w_out_conv,
    w_out_attn,
):
    f32, bf16 = jnp.float32, jnp.bfloat16
    n = tp
    rows, width = tokens.shape
    heads = w_q_nope.shape[1] // NOPE
    inverse = np.float32(THETA) ** (-np.arange(0, ROPE, 2, dtype=np.float32) / np.float32(ROPE))
    phase = np.arange(sp * rows, dtype=np.float32)[:, None] * inverse[None, :].astype(np.float32)
    phase = np.tile(phase, (1, 2 * heads)).reshape(sp, rows, heads * ROPE)
    cosine, sine = np.cos(phase).astype(np.float32), np.sin(phase).astype(np.float32)
    operands = (
        tokens,
        mix_gain,
        w_conv_value,
        w_conv_outer,
        w_conv_inner,
        conv_kernel,
        w_q_down.reshape(n, width, -1),
        w_kv_down.T,
        w_rope_key.T,
        q_gain,
        kv_gain,
        w_q_nope,
        w_q_rope,
        w_k_nope,
        w_value,
        w_out_conv,
        w_out_attn,
        jnp.asarray(cosine),
        jnp.asarray(sine),
    )
    vm = pltpu.VMEM
    cw = w_conv_value.shape[1]
    lat = kv_gain.shape[0]
    lanes = heads * ROPE
    scratch = [vm((n, rows, width), bf16)]
    scratch += [vm(x.shape, x.dtype) for x in operands[1:15]]
    scratch += [vm((n, w_out_conv.shape[0], width), bf16)] * 2
    scratch += [vm((rows, lanes), f32)] * 2
    scratch += [
        vm((3,) + w_conv_value.shape, bf16),
        vm((2, 2, rows, width), bf16),
        vm((2, 2 * rows, width), bf16),
        vm((3, 2 * rows, cw), f32),
        vm((rows, width), bf16),
        vm((2, 3, rows, cw), bf16),
        vm((3, rows, cw), bf16),
        vm((3, rows, cw), f32),
        vm((n, rows, w_q_down.shape[1]), bf16),
        vm((n, rows, 2 * w_kv_down.shape[1]), bf16),
        vm((n, rows, lat), bf16),
        vm((n, rows // heads, lanes), bf16),
        vm((rows, cw), bf16),
        vm((16, cw), bf16),
        vm((16, cw), bf16),
        vm((n, rows, width), f32),
        vm((2, rows, width), bf16),
        vm((2, rows, width), bf16),
        vm((rows, width), bf16),
        vm((rows, width), bf16),
        vm((rows // 8, width), bf16),
    ]
    dma = pltpu.SemaphoreType.DMA
    scratch += [dma((4,)), dma, dma((3,)), dma((2,)), dma, dma((12,)), dma((3,)), dma, dma]
    scratch += [dma((n - 1,)), dma, dma, dma((3,)), dma((2,)), dma((4,))]
    return pl.pallas_call(
        functools.partial(mixer_kernel, n),
        out_shape=pltpu.VMEM((rows, width), bf16),
        in_specs=[pl.BlockSpec(memory_space=pl.ANY)] * len(operands),
        out_specs=pl.BlockSpec(memory_space=pltpu.VMEM),
        scratch_shapes=scratch,
        compiler_params=pltpu.CompilerParams(collective_id=0, has_side_effects=True),
    )(*operands)


def solution(mesh):
    placed = (
        P(("grp", "sp"), "tp"),
        P(),
        P("sp", "tp"),
        P("sp", "tp"),
        P("sp", "tp"),
        P(None, "tp"),
        P(None, "tp"),
        P(None, "tp"),
        P(),
        P(),
        P(),
        P(None, "tp"),
        P(None, "tp"),
        P(None, "tp"),
        P(None, "tp"),
        P("tp", None),
        P("tp", None),
    )
    grp, sp, tp = mesh.shape["grp"], mesh.shape["sp"], mesh.shape["tp"]

    def per_device(*args):
        if fits(grp, sp, tp, *args):
            return fused(sp, tp, *args)
        return gathered_weights(*args)

    return jax.shard_map(
        per_device, mesh=mesh, in_specs=placed, out_specs=P(("grp", "sp"), "tp"), check_vma=False
    )
```

```python
import functools

import jax
import jax.numpy as jnp
import numpy as np
from jax import lax
from jax.experimental import pallas as pl
from jax.experimental.pallas import tpu as pltpu
from jax.sharding import PartitionSpec as P

MESH = pl.DeviceIdType.MESH

D = 2048
NOPE = 64
ROPE = 32
VALUE = 64


EPS = 1e-06
THETA = 10000.0


def with_halo(x, sides, width):
    for axis, dim in sides:
        size, length = (lax.axis_size(axis), x.shape[dim])
        up = [(i, (i + 1) % size) for i in range(size - 1)]
        down = [(j, i) for i, j in up]
        last = lax.slice_in_dim(x, length - width, length, axis=dim)
        first = lax.slice_in_dim(x, 0, width, axis=dim)
        before = lax.ppermute(last, axis, up)
        after = lax.ppermute(first, axis, down)
        x = jnp.concatenate([before, x, after], axis=dim)
    return x


def rms_scale(values):
    return lax.rsqrt(jnp.mean(values * values, axis=-1, keepdims=True) + EPS)


def angles(positions, width):
    inverse = THETA ** (-jnp.arange(0, width, 2, dtype=jnp.float32) / width)
    phase = positions[:, None] * inverse[None, :]
    phase = jnp.concatenate([phase, phase], axis=-1)
    return (jnp.cos(phase), jnp.sin(phase))


def turned(values, cosine, sine):
    half = values.shape[-1] // 2
    first = values[..., :half]
    second = values[..., half:]
    return values * cosine + jnp.concatenate([-second, first], axis=-1) * sine


def block_rows(count):
    for candidate in range(min(count, 1024), 0, -1):
        if count % candidate == 0 and candidate % 128 == 0:
            return candidate
    for candidate in range(min(count, 1024), 0, -1):
        if count % candidate == 0:
            return candidate
    return count


def gathered_weights(
    tokens,
    mix_gain,
    w_conv_value,
    w_conv_outer,
    w_conv_inner,
    conv_kernel,
    w_q_down,
    w_kv_down,
    w_rope_key,
    q_gain,
    kv_gain,
    w_q_nope,
    w_q_rope,
    w_k_nope,
    w_value,
    w_out_conv,
    w_out_attn,
):
    f32 = jnp.float32
    bf16 = jnp.bfloat16
    rows = tokens.shape[0]
    conv_value_w, conv_outer_w, conv_inner_w = (
        lax.all_gather(w_conv_value, "sp", axis=0, tiled=True),
        lax.all_gather(w_conv_outer, "sp", axis=0, tiled=True),
        lax.all_gather(w_conv_inner, "sp", axis=0, tiled=True),
    )
    matrices = (conv_value_w, conv_outer_w, conv_inner_w, w_q_down, w_kv_down, w_rope_key)
    gain = mix_gain.astype(f32)
    piece_f = lax.all_gather(tokens, "tp", axis=1, tiled=True).astype(f32)
    scaled = (piece_f * gain).astype(bf16)
    updated = tuple((jnp.dot(scaled, matrix, preferred_element_type=f32) for matrix in matrices))
    squares = jnp.sum(piece_f * piece_f, axis=1)
    row_scale = lax.rsqrt(squares / D + EPS)[:, None]
    conv_value, conv_outer, conv_inner, q_part, kv_part, rope_raw = [
        (row_scale * total).astype(bf16) for total in updated
    ]
    gated = (conv_inner.astype(f32) * conv_value.astype(f32)).astype(bf16)
    padded = with_halo(gated, (("sp", 0),), 1).astype(f32)
    kernel = conv_kernel.astype(f32)
    conv_out = padded[:-2] * kernel[0] + padded[1:-1] * kernel[1] + padded[2:] * kernel[2]
    y_conv = (conv_outer.astype(f32) * conv_out).astype(bf16)
    q_latent, kv_latent = (
        lax.all_gather(q_part, "tp", axis=1, tiled=True),
        lax.all_gather(kv_part, "tp", axis=1, tiled=True),
    )
    q_float = q_latent.astype(f32)
    q_normed = (q_float * rms_scale(q_float) * q_gain.astype(f32)).astype(bf16)
    kv_float = kv_latent.astype(f32)
    kv_normed = (kv_float * rms_scale(kv_float) * kv_gain.astype(f32)).astype(bf16)
    heads = w_q_nope.shape[1] // NOPE
    positions = (lax.axis_index("sp") * rows + jnp.arange(rows, dtype=jnp.int32)).astype(f32)
    cosine, sine = angles(positions, ROPE)
    q_nope = (
        jnp.dot(q_normed, w_q_nope, preferred_element_type=f32)
        .astype(bf16)
        .reshape(rows, heads, NOPE)
    )
    q_rope_raw = jnp.dot(q_normed, w_q_rope, preferred_element_type=f32).reshape(rows, heads, ROPE)
    q_rope = turned(q_rope_raw, cosine[:, None, :], sine[:, None, :]).astype(bf16)
    k_rope = turned(rope_raw.astype(f32), cosine, sine).astype(bf16)
    factor = (NOPE + ROPE) ** (-0.5)

    def attend(state, key_block, value_block, rope_block):
        peak, total, summed = state
        count = key_block.shape[0]
        keys3 = key_block.reshape(count, heads, NOPE)
        values3 = value_block.reshape(count, heads, VALUE)
        scores = jnp.einsum("qhd,khd->qhk", q_nope, keys3, preferred_element_type=f32)
        scores = scores + jnp.einsum("qhr,kr->qhk", q_rope, rope_block, preferred_element_type=f32)
        scores = scores * factor
        new_peak = jnp.maximum(peak, jnp.max(scores, axis=-1))
        fade = jnp.exp(peak - new_peak)
        weights = jnp.exp(scores - new_peak[..., None])
        total = total * fade + jnp.sum(weights, axis=-1)
        summed = summed * fade[..., None] + jnp.einsum(
            "qhk,khd->qhd", weights.astype(bf16), values3, preferred_element_type=f32
        )
        return (new_peak, total, summed)

    start_state = (
        jnp.full((rows, heads), -jnp.inf, f32),
        jnp.zeros((rows, heads), f32),
        jnp.zeros((rows, heads, VALUE), f32),
    )
    latent = lax.all_gather(kv_normed, "sp", axis=0, tiled=True)
    rope_keys = lax.all_gather(k_rope, "sp", axis=0, tiled=True)
    size = block_rows(latent.shape[0])
    count = latent.shape[0] // size

    def one_block(carry, blocks):
        latent_block, rope_block = blocks
        key_block = jnp.dot(latent_block, w_k_nope, preferred_element_type=f32).astype(bf16)
        value_block = jnp.dot(latent_block, w_value, preferred_element_type=f32).astype(bf16)
        return (attend(carry, key_block, value_block, rope_block), None)

    carry, ignored = lax.scan(
        one_block,
        start_state,
        (
            latent.reshape(count, size, latent.shape[1]),
            rope_keys.reshape(count, size, rope_keys.shape[1]),
        ),
    )
    peak, total, summed = carry
    y_attn = (summed / total[..., None]).astype(bf16).reshape(rows, heads * VALUE)
    partial_sum = jnp.dot(y_conv, w_out_conv, preferred_element_type=f32) + jnp.dot(
        y_attn, w_out_attn, preferred_element_type=f32
    )
    return (
        lax.psum_scatter(partial_sum.astype(jnp.bfloat16), "tp", scatter_dimension=1, tiled=True)
        .astype(jnp.float32)
        .astype(bf16)
    )


def copy_to(src, dst, send, recv, sp, tp, **group):
    return pltpu.make_async_remote_copy(
        src_ref=src,
        dst_ref=dst,
        send_sem=send,
        recv_sem=recv,
        device_id={"sp": sp, "tp": tp, **group},
        device_id_type=MESH,
    )


def dot(a, b):
    return jnp.dot(a, b, preferred_element_type=jnp.float32)


def dot_t(a, b):
    return lax.dot_general(a, b, (((1,), (1,)), ((), ())), preferred_element_type=jnp.float32)


def mixer_kernel(
    n,
    tokens_h,
    gain_h,
    wcv_h,
    wco_h,
    wci_h,
    taps_h,
    wq_h,
    wkv_h,
    wr_h,
    qg_h,
    kvg_h,
    wqn_h,
    wqr_h,
    wkn_h,
    wva_h,
    woc_h,
    woa_h,
    cos_h,
    sin_h,
    out_ref,
    tok,
    gain,
    wcv,
    wco,
    wci,
    taps,
    wq,
    wkv,
    wr,
    qg,
    kvg,
    wqn,
    wqr,
    wkn,
    wva,
    woc,
    woa,
    cosine,
    sine,
    wx,
    xt,
    xs,
    base,
    mine_other,
    part,
    got,
    own,
    qp,
    kvp,
    kvr,
    rk,
    gate,
    before,
    after,
    acc,
    put_near,
    got_near,
    put_far,
    got_far,
    got_early,
    load_sem,
    sent,
    r_tok,
    r_z,
    r_xf,
    r_w,
    r_y,
    r_q,
    r_kv,
    r_kz,
    r_kf,
    r_rk,
    r_p,
    r_h,
    r_o,
):
    f32, bf16 = jnp.float32, jnp.bfloat16
    g, s, t = lax.axis_index("grp"), lax.axis_index("sp"), lax.axis_index("tp")
    core = lax.rem(t, 2)
    near = t + 1 - 2 * core
    far = lax.rem(t + 2, n)
    diag = lax.rem(near + 2, n)
    rows, width = tok.shape[1], tok.shape[2]
    cw = wcv.shape[1]
    tp_peers = (near, far, diag)
    upper = lax.div(s, n // 2)
    side = lax.div(t, 2)
    is_hub = (s == 1) | (s == n - 2)
    mate = s + 1 - 2 * lax.rem(s, 2)
    hub_over = n // 2 - upper
    end_over = (n - 1) * (1 - upper)

    loads = [
        (tokens_h, tok.at[t]),
        (gain_h, gain),
        (wq_h, wq),
        (wkv_h, wkv),
        (wr_h, wr),
        (wcv_h, wcv),
        (wco_h, wco),
        (wci_h, wci),
        (taps_h, taps),
        (qg_h, qg),
        (kvg_h, kvg),
        (wqn_h, wqn),
        (wqr_h, wqr),
        (wkn_h, wkn),
        (wva_h, wva),
        (cos_h.at[s], cosine),
        (sin_h.at[s], sine),
    ]
    for j in range(n):
        columns = pl.ds(j * width, width)
        loads.append((woa_h.at[:, columns], woa.at[j]))
        loads.append((woc_h.at[:, columns], woc.at[j]))
    groups = [0] + [2] * 4 + [1] * 3 + [3] * (len(loads) - 8)
    loads = [pltpu.make_async_copy(a, b, load_sem.at[i]) for (a, b), i in zip(loads, groups)]
    for load in loads:
        load.start()

    barrier = pltpu.get_barrier_semaphore()
    for peer in tp_peers:
        pl.semaphore_signal(barrier, inc=1, device_id={"sp": s, "tp": peer}, device_id_type=MESH)
    for k in range(1, n):
        pl.semaphore_signal(
            barrier, inc=1, device_id={"sp": lax.rem(s + k, n), "tp": t}, device_id_type=MESH
        )
    pl.semaphore_signal(
        barrier, inc=1, device_id={"grp": 1 - g, "sp": s, "tp": t}, device_id_type=MESH
    )
    loads[0].wait()
    pl.semaphore_wait(barrier, 2 * (n - 1) + 1)

    tok_far = copy_to(tok.at[t], tok.at[t], sent, r_tok.at[0], s, far)
    tok_near = copy_to(tok.at[t], tok.at[t], sent, r_tok.at[1], s, near)
    tok_fwd = copy_to(tok.at[far], tok.at[far], sent, r_tok.at[2], s, near)
    z_slot = xt.at[jnp.where(is_hub, 1, 0), core]
    z_recv = r_z.at[jnp.where(is_hub, 1, 0)]
    z_own = copy_to(tok.at[t], z_slot, sent, z_recv, hub_over, t)
    z_far = copy_to(tok.at[far], z_slot, sent, z_recv, hub_over, t)
    own_first = side != upper
    tok_far.start()
    tok_near.start()
    weights = (wcv, wco, wci)
    order = (2, 0, 1)
    pieces_per = 4
    chunk = wcv.shape[0] // (2 * pieces_per)
    chunks = [(m, c) for m in order for c in range(pieces_per)]

    def chunk_rows(half, c):
        return pl.ds(pl.multiple_of((pieces_per * half + c) * chunk, chunk), chunk)

    w_sends, y_sends = [], []
    for k, (m, c) in enumerate(chunks):
        w_sends.append(
            copy_to(
                weights[m].at[chunk_rows(g, c)],
                wx.at[m, chunk_rows(g, c)],
                sent,
                r_w.at[k],
                mate,
                t,
            )
        )
        block = wx.at[m, chunk_rows(g, c)]
        y_sends.append(copy_to(block, block, sent, r_y.at[m], s, t, grp=1 - g))

    def arrived(ref, sem):
        copy_to(ref, ref, sent, sem, s, near).wait_recv()

    def relay(k):
        w_sends[k].wait_recv()
        y_sends[k].start()

    for load in loads[5:8]:
        load.wait()
    for copy in w_sends[:4]:
        copy.start()

    @pl.when(own_first)
    def _():
        z_own.start()

    for copy in w_sends[4:6]:
        copy.start()
    for load in loads[1:5] + loads[8:]:
        load.wait()
    def scaled_slice(block, f):
        gain_f = gain[pl.ds(pl.multiple_of(f * width, width), width)][None, :].astype(f32)
        return (block.astype(f32) * gain_f).astype(bf16)

    def features(f):
        return pl.ds(pl.multiple_of(f * width, width), width)

    def square_sum(f):
        piece = tok[f].astype(f32)
        return jnp.sum(piece * piece, axis=1, keepdims=True)

    def kv_product(scaled, f):
        return dot_t(scaled, wkv[:, features(f)])

    def r_product(scaled, f):
        return dot_t(scaled, wr[:, features(f)])

    def project(f):
        scaled = scaled_slice(tok[f], f)
        sums = (kv_product(scaled, f), r_product(scaled, f), dot(scaled, wq[f]))
        return (square_sum(f),) + sums

    squares, kv_sum, r_sum, q_sum = project(t)
    copy_to(tok.at[near], tok.at[near], sent, r_tok.at[1], s, near).wait_recv()
    more = project(near)
    squares, kv_sum = squares + more[0], kv_sum + more[1]
    r_sum, q_sum = r_sum + more[2], q_sum + more[3]
    copy_to(tok.at[far], tok.at[far], sent, r_tok.at[0], s, far).wait_recv()
    tok_fwd.start()

    @pl.when(jnp.logical_not(own_first))
    def _():
        z_far.start()

    first_part = (12, 10)
    for copy in w_sends[6 : min(first_part)]:
        copy.start()
    for c in range(2):

        @pl.when(core == c)
        def _():
            for copy in w_sends[min(first_part) : first_part[c]]:
                copy.start()

    more = project(far)
    squares, kv_sum = squares + more[0], kv_sum + more[1]
    r_sum, q_sum = r_sum + more[2], q_sum + more[3]
    copy_to(tok.at[diag], tok.at[diag], sent, r_tok.at[2], s, near).wait_recv()
    last = scaled_slice(tok[diag], diag)
    squares = squares + square_sum(diag)
    kv_sum = kv_sum + kv_product(last, diag)
    row_scale = lax.rsqrt(squares / (n * width) + EPS)
    kw = wkv.shape[0]
    place = (
        lax.broadcasted_iota(jnp.int32, (kw, 2 * kw), 1)
        == lax.broadcasted_iota(jnp.int32, (kw, 2 * kw), 0) + kw * core
    )
    place = jnp.where(place, 1.0, 0.0).astype(bf16)
    kvp[t] = dot((row_scale * kv_sum).astype(bf16), place).astype(bf16)
    kv_sends = [
        copy_to(kvp.at[t], kvp.at[t], sent, r_kv, s, p) for i, p in enumerate(tp_peers)
    ]
    for copy in (kv_sends[1], kv_sends[2], kv_sends[0]):
        copy.start()
    q_sum = q_sum + dot(last, wq[diag])
    r_sum = r_sum + r_product(last, diag)
    qp[t] = (row_scale * q_sum).astype(bf16)
    q_sends = [
        copy_to(qp.at[t], qp.at[t], sent, r_q, s, p) for i, p in enumerate(tp_peers)
    ]
    for copy in (q_sends[1], q_sends[2], q_sends[0]):
        copy.start()

    cos_v, sin_v = cosine[...], sine[...]
    lanes = cos_v.shape[1]
    turn_r = lax.broadcasted_iota(jnp.int32, (lanes, lanes), 0)
    turn_c = lax.broadcasted_iota(jnp.int32, (lanes, lanes), 1)
    half = ROPE // 2
    low = lax.rem(turn_c, ROPE) < half
    turn = jnp.where(
        low & (turn_r == turn_c + half), -1.0, jnp.where((~low) & (turn_r == turn_c - half), 1.0, 0.0)
    ).astype(bf16)
    spread_r = lax.broadcasted_iota(jnp.int32, (ROPE, lanes), 0)
    spread_c = lax.broadcasted_iota(jnp.int32, (ROPE, lanes), 1)
    spread = jnp.where(lax.rem(spread_c, ROPE) == spread_r, 1.0, 0.0).astype(bf16)
    rope_raw = dot((row_scale * r_sum).astype(bf16), spread).astype(bf16)
    k_rope = (rope_raw.astype(f32) * cos_v + dot(rope_raw, turn) * sin_v).astype(bf16)
    groups = lanes // ROPE
    slab = rows // groups
    slab_lane = lax.div(lax.broadcasted_iota(jnp.int32, (slab, lanes), 1), ROPE)
    packed = jnp.zeros((slab, lanes), f32)
    for i in range(groups):
        packed = jnp.where(slab_lane == i, k_rope[i * slab : (i + 1) * slab].astype(f32), packed)
    rk[s] = packed.astype(bf16)
    rk_sends = [
        copy_to(rk.at[s], rk.at[s], sent, r_rk, lax.rem(s + k, n), t) for k in range(1, n)
    ]
    for copy in (rk_sends[1], rk_sends[0], rk_sends[2]):
        copy.start()

    mine_scaled = scaled_slice(tok[s], s)
    for m in order:
        own[m] = dot(mine_scaled, weights[m][...])
    for k in range(4):
        relay(k)

    edge = before.shape[0]
    up = copy_to(gate.at[pl.ds(rows - edge, edge)], before, sent, r_h.at[0], s + 1, t)
    down = copy_to(gate.at[pl.ds(0, edge)], after, sent, r_h.at[1], s - 1, t)

    def take(m):
        arrived(got.at[m], r_p.at[m])
        own[m] = own[m] + got[m].astype(f32)

    def summed(i):
        return (row_scale * own[i]).astype(bf16).astype(f32)

    def gate_part():
        take(2)
        take(0)
        gate[...] = (summed(2) * summed(0)).astype(bf16)

        @pl.when(s < n - 1)
        def _():
            up.start()

        @pl.when(s > 0)
        def _():
            down.start()

    p_sends = []
    for i in range(2):
        for m in range(3):
            target = hub_over if i else end_over
            p_sends.append(
                copy_to(part.at[i, m], got.at[m], sent, r_p.at[m], target, t)
            )
    x_sends = []
    for i in range(2):
        slot = xt.at[i, core]
        x_sends.append(copy_to(slot, slot, sent, r_xf, s, near))

    def conv_start():
        @pl.when(is_hub)
        def _():
            for i in range(2):
                piece_rows = pl.ds(i * rows, rows)
                xs[0, piece_rows] = scaled_slice(xt[i, lax.rem(s, 2)], s)
                xs[1, piece_rows] = scaled_slice(xt[i, lax.rem(mate, 2)], mate)
            base[order[0]] = dot(xs[0], weights[order[0]][...])

    def conv_ahead():
        @pl.when(is_hub)
        def _():
            for m in order[1:]:
                base[m] = dot(xs[0], weights[m][...])

        mine_other[...] = scaled_slice(tok[mate], mate)

    def conv_block(j):
        m = order[j]
        arrived(wx.at[m, pl.ds(0, wx.shape[1] // 2)], r_y.at[m])

        @pl.when(is_hub)
        def _():
            if j == 2:
                for i in range(2):
                    block = pl.ds(i * rows, rows)
                    total = base[m, block] + dot(xs[1, block], wx[m])
                    part[i, m] = total.astype(bf16)
                    p_sends[3 * i + m].start()
            else:
                total = base[m] + dot(xs[1], wx[m])
                for i in (1, 0):
                    part[i, m] = total[i * rows : (i + 1) * rows].astype(bf16)
                    p_sends[3 * i + m].start()

        own[m] = own[m] + dot(mine_other[...], wx[m])

    arrived(kvp.at[pl.ds(0, n - 1)], r_kv)
    kv_float = jnp.concatenate(
        [kvp[j].astype(f32) + kvp[j + 1].astype(f32) for j in range(0, n, 2)], axis=1
    )
    kv_scale = lax.rsqrt(jnp.mean(kv_float * kv_float, axis=1, keepdims=True) + EPS)
    kvr[s] = (kv_float * kv_scale * kvg[...][None, :].astype(f32)).astype(bf16)
    def quarter(index):
        return pl.ds(pl.multiple_of(index * (rows // n), rows // n), rows // n)

    mine = quarter(t)
    kz_sends = []
    for k in (2, 1, 3):
        z = lax.rem(s + k, n)
        copy = copy_to(
            kvr.at[s, mine], kvr.at[s, mine], sent, r_kz.at[k - 1], z, t
        )
        copy.start()
        kz_sends.append(copy)
    for c in range(2):

        @pl.when(core == c)
        def _():
            for copy in w_sends[first_part[c] :]:
                copy.start()


    def pass_on(i):
        @pl.when(is_hub)
        def _():
            slot = xt.at[i, core]
            copy_to(slot, slot, sent, r_z.at[i], s, near).wait_recv()
            x_sends[i].start()

    relay(4)
    relay(5)
    pass_on(0)
    pass_on(1)
    relay(6)
    relay(7)

    @pl.when(is_hub)
    def _():
        arrived(xt.at[:, core], r_xf)

    conv_start()
    conv_ahead()
    conv_block(0)
    for k in range(8, 10):
        relay(k)

    arrived(qp.at[pl.ds(0, n - 1)], r_q)
    q_float = [qp[j].astype(f32) for j in range(n)]
    qw = q_float[0].shape[1]
    q_square = sum(jnp.sum(q * q, axis=1, keepdims=True) for q in q_float)
    q_scale = lax.rsqrt(q_square / (n * qw) + EPS)
    q_normed = jnp.concatenate(
        [(q * q_scale * qg[j * qw : (j + 1) * qw][None, :].astype(f32)).astype(bf16) for j, q in enumerate(q_float)], axis=1
    )
    q_nope = dot(q_normed, wqn[...]).astype(bf16)
    q_raw = dot(q_normed, wqr[...])
    w_turned = dot(wqr[...], turn).astype(bf16)
    q_rope = (q_raw * cos_v + dot(q_normed, w_turned) * sin_v).astype(bf16)

    for k in range(10, 12):
        relay(k)
    kf_sends = []
    for k in (2, 1, 3):
        z = lax.rem(s + n - k, n)
        copy_to(
            kvr.at[z, mine], kvr.at[z, mine], sent, r_kz.at[k - 1], z, t
        ).wait_recv()
        for i, p in enumerate(tp_peers):
            copy = copy_to(
                kvr.at[z, mine], kvr.at[z, mine], sent, r_kf, s, p
            )
            copy.start()
            kf_sends.append(copy)
    conv_block(1)
    conv_block(2)
    arrived(kvr.at[pl.ds(0, n - 1), pl.ds(0, (n - 1) * (rows // n))], r_kf)

    @pl.when(is_hub)
    def _():
        gate_part()

    latent = jnp.concatenate(
        [kvr[j, i * slab : (i + 1) * slab] for i in range(groups) for j in range(n)], axis=0
    )
    arrived(rk.at[pl.ds(0, n - 1)], r_rk)
    packs = jnp.concatenate([rk[j] for j in range(n)], axis=0)
    same = lax.rem(turn_r, ROPE) == lax.rem(turn_c, ROPE)
    ropes = jnp.concatenate(
        [
            dot(packs, jnp.where(same & (lax.div(turn_r, ROPE) == i), 1.0, 0.0).astype(bf16))
            for i in range(groups)
        ],
        axis=0,
    ).astype(bf16)
    keys = dot(latent, wkn[...]).astype(bf16)
    values = dot(latent, wva[...]).astype(bf16)
    heads = wqn.shape[1] // NOPE
    factor = (NOPE + ROPE) ** (-0.5)
    pair = 2 * NOPE
    lane = lax.broadcasted_iota(jnp.int32, (rows, pair), 1)
    lane_r = lax.broadcasted_iota(jnp.int32, (rows, lanes), 1)
    pieces = []
    for p in range(heads // 2):
        cut = slice(p * pair, (p + 1) * pair)
        key_pair = jnp.concatenate([keys[:, cut], ropes], axis=1)
        value_pair = values[:, cut]
        outs = []
        for i in range(2):
            h = 2 * p + i
            in_head = (lane >= i * NOPE) & (lane < (i + 1) * NOPE)
            in_rope = (lane_r >= h * ROPE) & (lane_r < (h + 1) * ROPE)
            query = jnp.concatenate(
                [
                    jnp.where(in_head, q_nope[:, cut].astype(f32), 0.0).astype(bf16),
                    jnp.where(in_rope, q_rope.astype(f32), 0.0).astype(bf16),
                ],
                axis=1,
            )
            scores = dot_t(query, key_pair) * factor
            peak = jnp.max(scores, axis=1, keepdims=True)
            weights = jnp.exp(scores - peak)
            total = jnp.sum(weights, axis=1, keepdims=True)
            outs.append(dot(weights.astype(bf16), value_pair) / total)
        pieces.append(jnp.where(lane < NOPE, outs[0], outs[1]).astype(bf16))
    y_attn = jnp.concatenate(pieces, axis=1)
    for j in range(n):
        acc[j] = dot(y_attn, woa[j])

    @pl.when(jnp.logical_not(is_hub))
    def _():
        gate_part()

    take(1)
    conv_outer = summed(1)
    middle = gate[...].astype(f32)
    kernel = [taps[i : i + 1, :].astype(f32) for i in range(3)]
    row = lax.broadcasted_iota(jnp.int32, middle.shape, 0)
    previous = pltpu.roll(middle, 1, 0)
    following = pltpu.roll(middle, rows - 1, 0)

    @pl.when(s > 0)
    def _():
        up.wait_recv()

    @pl.when(s == 0)
    def _():
        before[...] = jnp.zeros_like(before)

    @pl.when(s < n - 1)
    def _():
        down.wait_recv()

    @pl.when(s == n - 1)
    def _():
        after[...] = jnp.zeros_like(after)

    first = before[...].astype(f32)[edge - 1 : edge, :]
    last = after[...].astype(f32)[0:1, :]
    previous = jnp.where(row == 0, first, previous)
    following = jnp.where(row == rows - 1, last, following)
    conv_out = previous * kernel[0] + middle * kernel[1] + following * kernel[2]
    y_conv = (conv_outer * conv_out).astype(bf16)

    def share(j):
        return acc[j] + dot(y_conv, woc[j])

    early = got_early.shape[0]
    lead, rest = pl.ds(0, early), pl.ds(early, rows - early)
    put_near[0] = share(diag).astype(bf16)
    o_diag = copy_to(put_near.at[0, rest], got_near.at[0, rest], sent, r_o.at[0], s, near)
    o_diag.start()
    o_cross = copy_to(put_near.at[0, lead], got_early, sent, r_o.at[3], s, diag)
    o_cross.start()
    far_share = share(far).astype(bf16).astype(f32)
    put_far[lead] = far_share[:early].astype(bf16)
    o_lead = copy_to(put_far.at[lead], got_far.at[lead], sent, r_o.at[1], s, far)
    o_lead.start()
    o_diag.wait_recv()
    put_far[rest] = (far_share[early:] + got_near[0, rest].astype(f32)).astype(bf16)
    o_far = copy_to(put_far.at[rest], got_far.at[rest], sent, r_o.at[1], s, far)
    o_far.start()
    put_near[1] = share(near).astype(bf16)
    o_near = copy_to(put_near.at[1], got_near.at[1], sent, r_o.at[2], s, near)
    o_near.start()
    my_share = share(t).astype(bf16).astype(f32)
    o_near.wait_recv()
    my_share = my_share + got_near[1].astype(f32)

    tok_far.wait_send()
    tok_near.wait_send()
    tok_fwd.wait_send()

    z_own.wait_send()
    for copy in kv_sends + q_sends + rk_sends + kz_sends + kf_sends + w_sends + y_sends:
        copy.wait_send()

    @pl.when(is_hub)
    def _():
        for copy in p_sends + x_sends:
            copy.wait_send()

    @pl.when(s < n - 1)
    def _():
        up.wait_send()

    @pl.when(s > 0)
    def _():
        down.wait_send()

    for copy in (o_diag, o_cross, o_lead, o_near, o_far):
        copy.wait_send()
    arrived(got_early, r_o.at[3])
    arrived(got_far, r_o.at[1])
    my_share = my_share + got_far[...].astype(f32)
    out_ref[rest] = my_share[early:].astype(bf16)
    out_ref[lead] = (my_share[:early] + got_early[...].astype(f32)).astype(bf16)


def fits(grp, sp, tp, tokens, mix_gain, w_conv_value, *others):
    rows, width = tokens.shape
    if grp != 2 or sp != 4 or tp != 4 or rows * sp > width * tp:
        return False
    return width % 128 == 0 and rows % 64 == 0 and w_conv_value.shape[0] % 64 == 0


def fused(
    sp,
    tp,
    tokens,
    mix_gain,
    w_conv_value,
    w_conv_outer,
    w_conv_inner,
    conv_kernel,
    w_q_down,
    w_kv_down,
    w_rope_key,
    q_gain,
    kv_gain,
    w_q_nope,
    w_q_rope,
    w_k_nope,
    w_value,
    w_out_conv,
    w_out_attn,
):
    f32, bf16 = jnp.float32, jnp.bfloat16
    n = tp
    rows, width = tokens.shape
    heads = w_q_nope.shape[1] // NOPE
    inverse = np.float32(THETA) ** (-np.arange(0, ROPE, 2, dtype=np.float32) / np.float32(ROPE))
    phase = np.arange(sp * rows, dtype=np.float32)[:, None] * inverse[None, :].astype(np.float32)
    phase = np.tile(phase, (1, 2 * heads)).reshape(sp, rows, heads * ROPE)
    cosine, sine = np.cos(phase).astype(np.float32), np.sin(phase).astype(np.float32)
    operands = (
        tokens,
        mix_gain,
        w_conv_value,
        w_conv_outer,
        w_conv_inner,
        conv_kernel,
        w_q_down.reshape(n, width, -1),
        w_kv_down.T,
        w_rope_key.T,
        q_gain,
        kv_gain,
        w_q_nope,
        w_q_rope,
        w_k_nope,
        w_value,
        w_out_conv,
        w_out_attn,
        jnp.asarray(cosine),
        jnp.asarray(sine),
    )
    vm = pltpu.VMEM
    cw = w_conv_value.shape[1]
    lat = kv_gain.shape[0]
    lanes = heads * ROPE
    scratch = [vm((n, rows, width), bf16)]
    scratch += [vm(x.shape, x.dtype) for x in operands[1:15]]
    scratch += [vm((n, w_out_conv.shape[0], width), bf16)] * 2
    scratch += [vm((rows, lanes), f32)] * 2
    scratch += [
        vm((3,) + w_conv_value.shape, bf16),
        vm((2, 2, rows, width), bf16),
        vm((2, 2 * rows, width), bf16),
        vm((3, 2 * rows, cw), f32),
        vm((rows, width), bf16),
        vm((2, 3, rows, cw), bf16),
        vm((3, rows, cw), bf16),
        vm((3, rows, cw), f32),
        vm((n, rows, w_q_down.shape[1]), bf16),
        vm((n, rows, 2 * w_kv_down.shape[1]), bf16),
        vm((n, rows, lat), bf16),
        vm((n, rows // heads, lanes), bf16),
        vm((rows, cw), bf16),
        vm((16, cw), bf16),
        vm((16, cw), bf16),
        vm((n, rows, width), f32),
        vm((2, rows, width), bf16),
        vm((2, rows, width), bf16),
        vm((rows, width), bf16),
        vm((rows, width), bf16),
        vm((rows // 8, width), bf16),
    ]
    dma = pltpu.SemaphoreType.DMA
    scratch += [dma((4,)), dma, dma((3,)), dma((2,)), dma, dma((12,)), dma((3,)), dma, dma]
    scratch += [dma((n - 1,)), dma, dma, dma((3,)), dma((2,)), dma((4,))]
    return pl.pallas_call(
        functools.partial(mixer_kernel, n),
        out_shape=pltpu.VMEM((rows, width), bf16),
        in_specs=[pl.BlockSpec(memory_space=pl.ANY)] * len(operands),
        out_specs=pl.BlockSpec(memory_space=pltpu.VMEM),
        scratch_shapes=scratch,
        compiler_params=pltpu.CompilerParams(collective_id=0, has_side_effects=True),
    )(*operands)


def solution(mesh):
    placed = (
        P(("grp", "sp"), "tp"),
        P(),
        P("sp", "tp"),
        P("sp", "tp"),
        P("sp", "tp"),
        P(None, "tp"),
        P(None, "tp"),
        P(None, "tp"),
        P(),
        P(),
        P(),
        P(None, "tp"),
        P(None, "tp"),
        P(None, "tp"),
        P(None, "tp"),
        P("tp", None),
        P("tp", None),
    )
    grp, sp, tp = mesh.shape["grp"], mesh.shape["sp"], mesh.shape["tp"]

    def per_device(*args):
        if fits(grp, sp, tp, *args):
            return fused(sp, tp, *args)
        return gathered_weights(*args)

    return jax.shard_map(
        per_device, mesh=mesh, in_specs=placed, out_specs=P(("grp", "sp"), "tp"), check_vma=False
    )
```
